32 devices in a mesh: grp: 2 (over y), sp: 4 (over z), fs: 2 (over x), tp: 2 (over core).
Axes of the slice: x: 2, y: 2, z: 4, core: 2. Of those that a mesh axis runs over, the one named last changes fastest.
Arguments:
- tokens: bfloat16 [4, 512, 2048], P(('grp', 'fs'), 'sp', 'tp'), parts along dimension 0, may hold values from -120 to 120
- mix_gain: float32 [2048], replicated, may hold values from 0.1 to 1.9
- attn_query: bfloat16 [2048, 1024], P('fs', 'tp'), may hold values from -0.375 to 0.375
- attn_key: bfloat16 [2048, 1024], P('fs', 'tp'), may hold values from -0.125 to 0.125
- attn_value: bfloat16 [2048, 1024], P('fs', 'tp'), may hold values from -0.125 to 0.125
- rec_query: bfloat16 [2048, 1024], P('fs', 'tp'), may hold values from -0.125 to 0.125
- rec_forget: bfloat16 [2048, 1024], P('fs', 'tp'), may hold values from -0.125 to 0.125
- rec_input: bfloat16 [2048, 1024], P('fs', 'tp'), may hold values from -0.125 to 0.125
- break_offset: float32 [8], P('tp'), may hold values from -13.5 to -7
- forget_room: float32 [8, 128], P('tp'), may hold values from 0.0009765625 to 0.05
- out_gain: float32 [128], replicated, may hold values from 0.1 to 1.9
- out_attn: bfloat16 [1024, 2048], P('tp', 'fs'), may hold values from -0.125 to 0.125
- out_rec: bfloat16 [1024, 2048], P('tp', 'fs'), may hold values from -0.125 to 0.125
Outputs:
- mixed: bfloat16 [4, 512, 2048], P(('grp', 'fs'), ('sp', 'tp')), parts along dimension 0
The draws below stay inside these ranges and needn't reach their ends.
There are 2 independent parts, one for each index of `grp`. The reference program is written for one: setup_inputs(seed, part) draws one part's arguments, and reference() takes and returns one part's arrays. A program takes and returns all parts, laid end to end along the dimension named above; an argument that names none is the same for every part. Nothing has to cross between parts.
All inputs are finite; a program needn't handle non-finite values.
Results may differ from the reference program's by a relative error of at most 0.019.
Values may be sent and summed in bfloat16 or wider, within the bound.
A program may use at most 64 MiB of HBM per device.

```python
import math
import jax
import jax.numpy as jnp
from jax import lax

D = 2048
SB_HEADS = 8
HEAD = 128
REC_HEADS = 8
DK = 128
DV = 128
REC_BLOCK = 64
TOK_DEV = 128
SEQS = 2
LENGTH = 512
N_TP = 2


def draw_tokens(key, part):
    full_shape = (SEQS, LENGTH, D)
    subkeys = jax.random.split(key, 4)
    row_scale = jnp.exp(jax.random.uniform(subkeys[0], (SEQS, LENGTH, 1), jnp.float32, 0.0, math.log(10.0)))
    col_scale = jnp.exp(jax.random.uniform(subkeys[1], (1, 1, D), jnp.float32, 0.0, math.log(10.0)))
    regions = jax.random.normal(subkeys[2], (SEQS, LENGTH // TOK_DEV, 1, D), jnp.float32)
    regions = jnp.broadcast_to(regions, (SEQS, LENGTH // TOK_DEV, TOK_DEV, D)).reshape(full_shape)
    rough_part = jax.random.normal(subkeys[3], full_shape, jnp.float32)
    regions = 0.5 * regions
    drawn = (rough_part * col_scale / 3.0 + regions) * row_scale
    return jnp.clip(drawn, -120.0, 120.0).astype(jnp.bfloat16)


def block_scale(key, extent, shards, smallest, high):
    level, own = 1.0, jax.random.fold_in(key, 6)
    for position, blocks in shards:
        heights = jnp.exp(jax.random.uniform(jax.random.fold_in(own, position), (blocks,), jnp.float32, smallest / len(shards), high / len(shards)))
        level = level * jnp.repeat(heights, extent[position] // blocks).reshape([-1 if axis == position else 1 for axis in range(len(extent))])
    return level


def normal_values(stream_key, shape, width, bound, cuts=(), kind=jnp.bfloat16):
    entries = jax.random.normal(stream_key, shape, jnp.float32) * width
    if len(cuts) > 0:
        entries = block_scale(stream_key, shape, cuts, -0.22, 0.18) * entries
    return jnp.clip(entries, min=-bound, max=bound).astype(kind)


def setup_inputs(seed: int = 0, part: int = 0) -> dict:
    arg_keys = jax.random.split(jax.random.key(seed), 14)
    part_keys = jax.random.split(jax.random.fold_in(arg_keys[13], part), 14)
    tokens = draw_tokens(jax.random.fold_in(jax.random.fold_in(arg_keys[13], part), 71), part)
    mix_gain = jnp.clip(1.0 + 0.18 * jax.random.normal(arg_keys[1], (D,), jnp.float32), 0.1, 1.9)
    attn_query = normal_values(arg_keys[2], (D, SB_HEADS * HEAD), (D // 9) ** -0.5, 0.375, ((0, 2), (1, 2)))
    attn_key = normal_values(arg_keys[3], (D, SB_HEADS * HEAD), D ** -0.5, 0.125, ((0, 2), (1, 2)))
    attn_value = normal_values(arg_keys[4], (D, SB_HEADS * HEAD), D ** -0.5, 0.125, ((0, 2), (1, 2)))
    rec_query = normal_values(arg_keys[5], (D, REC_HEADS * DK), D ** -0.5, 0.125, ((0, 2), (1, 2)))
    rec_forget = normal_values(arg_keys[6], (D, REC_HEADS * DK), D ** -0.5, 0.125, ((0, 2), (1, 2)))
    rec_input = normal_values(arg_keys[7], (D, REC_HEADS * DV), D ** -0.5, 0.125, ((0, 2), (1, 2)))
    break_offset = jnp.clip(-13.5 + 6.5 * jax.random.uniform(arg_keys[8], (SB_HEADS,), jnp.float32) ** block_scale(arg_keys[8], (SB_HEADS,), ((0, 2),), -0.2, 0.2), -13.5, -7.0)
    forget_room = jnp.clip(jnp.exp(math.log(0.05) - 3.9357395 * jax.random.uniform(arg_keys[9], (REC_HEADS, DK), jnp.float32) ** block_scale(arg_keys[9], (REC_HEADS, DK), ((0, 2),), -0.2, 0.2)), 0.0009765625, 0.05)
    out_gain = jnp.clip(1.0 + 0.18 * jax.random.normal(arg_keys[10], (DV,), jnp.float32), 0.1, 1.9)
    out_attn = normal_values(arg_keys[11], (SB_HEADS * HEAD, D), (SB_HEADS * HEAD + REC_HEADS * DV) ** -0.5, 0.125, ((0, 2), (1, 2)))
    out_rec = normal_values(arg_keys[12], (REC_HEADS * DV, D), (SB_HEADS * HEAD + REC_HEADS * DV) ** -0.5, 0.125, ((0, 2), (1, 2)))
    return {"tokens": tokens, "mix_gain": mix_gain, "attn_query": attn_query, "attn_key": attn_key, "attn_value": attn_value, "rec_query": rec_query, "rec_forget": rec_forget, "rec_input": rec_input, "break_offset": break_offset, "forget_room": forget_room, "out_gain": out_gain, "out_attn": out_attn, "out_rec": out_rec}


norm_eps = 1e-06
highest = lax.Precision.HIGHEST

def block_step(states, inputs):
    queries, key_in, value_rows, log_forget = inputs
    block_len = queries.shape[-2]
    cum_log = jnp.cumsum(log_forget, axis=-2)
    last_log = cum_log[..., -1:, :]
    q_dec = queries * jnp.exp(cum_log)
    k_inv = key_in * jnp.exp(-cum_log)
    causal = lax.iota(jnp.int32, block_len)[:, None] >= lax.iota(jnp.int32, block_len)[None, :]
    carried_part = jnp.einsum('...tk,...kv->...tv', q_dec, states, precision=highest)
    scores = jnp.where(causal, jnp.einsum('...tk,...sk->...ts', q_dec, k_inv, precision=highest), 0.0)
    inner_part = jnp.einsum('...ts,...sv->...tv', scores, value_rows, precision=highest)
    fresh_state = jnp.einsum('...sk,...sv->...kv', key_in * jnp.exp(last_log - cum_log), value_rows, precision=highest)
    return (jnp.exp(jnp.swapaxes(last_log, -1, -2)) * states + fresh_state, carried_part + inner_part)

def stick_sequence(queries, key_rows, value_rows, offsets):
    head_count = queries.shape[1]
    head_width = queries.shape[2]
    factor = 1.0 / math.sqrt(head_width)
    blocks = LENGTH // TOK_DEV

    def per_block(block_idx):
        q_blk = lax.dynamic_slice_in_dim(queries, block_idx * TOK_DEV, TOK_DEV, 0).astype(jnp.float32)
        q_pos = block_idx * TOK_DEV + lax.iota(jnp.int32, TOK_DEV)

        def turn(step_idx, carried):
            sums_acc, running = carried
            source = block_idx - step_idx
            k_blk = lax.dynamic_slice_in_dim(key_rows, source * TOK_DEV, TOK_DEV, 0).astype(jnp.float32)
            v_blk = lax.dynamic_slice_in_dim(value_rows, source * TOK_DEV, TOK_DEV, 0).astype(jnp.float32)
            scores = jnp.einsum('qhe,khe->hqk', q_blk, k_blk) * factor + offsets[:, None, None]
            k_pos = source * TOK_DEV + lax.iota(jnp.int32, TOK_DEV)
            strict = k_pos[None, :] < q_pos[:, None]
            log_keep = jnp.where(strict, jax.nn.log_sigmoid(-scores), 0.0)
            inner_sum = lax.cumsum(log_keep, axis=2, reverse=True) - log_keep
            sticks = jnp.where(strict, jnp.exp(jax.nn.log_sigmoid(scores) + inner_sum), 0.0)
            sticks = lax.optimization_barrier(sticks.astype(jnp.bfloat16)).astype(jnp.float32)
            partial_value = jnp.einsum('hqk,khe->qhe', sticks, v_blk)
            sums_acc = sums_acc + partial_value * jnp.transpose(jnp.exp(running))[:, :, None]
            return (sums_acc, running + lax.optimization_barrier(jnp.sum(log_keep, axis=2)))
        start_state = (jnp.zeros((TOK_DEV, head_count, head_width), jnp.float32), jnp.zeros((head_count, TOK_DEV), jnp.float32))
        sums_acc, unused_run = lax.fori_loop(0, block_idx + 1, turn, start_state)
        return sums_acc.astype(jnp.bfloat16)
    result = lax.map(per_block, jnp.arange(blocks, dtype=jnp.int32))
    return result.reshape(LENGTH, head_count, head_width)

def recur_sequence(queries, gate_pre, inputs, rooms, gain):
    key_in = rooms * jax.nn.sigmoid(-gate_pre.astype(jnp.float32))
    log_forget = jnp.log1p(-key_in)
    head_count = queries.shape[1]
    blocks = LENGTH // REC_BLOCK

    def split_blocks(tensor):
        return jnp.transpose(tensor.reshape(blocks, REC_BLOCK, head_count, tensor.shape[2]), (0, 2, 1, 3))
    empty_state = jnp.zeros((head_count, DK, DV), jnp.float32)
    final_state, pieces = lax.scan(block_step, empty_state, (split_blocks(queries.astype(jnp.float32)), split_blocks(key_in), split_blocks(inputs.astype(jnp.float32)), split_blocks(log_forget)))
    raw_out = jnp.transpose(pieces, (0, 2, 1, 3)).reshape(LENGTH, head_count, DV)
    factor = lax.rsqrt(lax.optimization_barrier(jnp.mean(raw_out * raw_out, axis=2, keepdims=True)) + norm_eps)
    return (raw_out * factor * gain).astype(jnp.bfloat16)

def reference(tokens, mix_gain, attn_query, attn_key, attn_value, rec_query, rec_forget, rec_input, break_offset, forget_room, out_gain, out_attn, out_rec):
    rows32 = tokens.astype(jnp.float32)
    factor = lax.rsqrt(lax.optimization_barrier(jnp.mean(rows32 * rows32, axis=2, keepdims=True)) + norm_eps)
    normed = (rows32 * factor * mix_gain).astype(jnp.bfloat16).reshape(SEQS * LENGTH, D)

    def project(matrix, head_width):
        product = jnp.dot(normed, matrix, preferred_element_type=jnp.float32).astype(jnp.bfloat16)
        return product.reshape(SEQS, LENGTH, matrix.shape[1] // head_width, head_width)
    attn_q = project(attn_query, HEAD)
    attn_k = project(attn_key, HEAD)
    attn_v = project(attn_value, HEAD)
    rec_q = project(rec_query, DK)
    rec_f = project(rec_forget, DK)
    rec_i = project(rec_input, DV)
    attn_out = lax.map(lambda triple: stick_sequence(triple[0], triple[1], triple[2], break_offset), (attn_q, attn_k, attn_v))
    rec_out = lax.map(lambda triple: recur_sequence(triple[0], triple[1], triple[2], forget_room, out_gain), (rec_q, rec_f, rec_i))
    attn_flat = attn_out.reshape(SEQS * LENGTH, SB_HEADS * HEAD)
    rec_flat = rec_out.reshape(SEQS * LENGTH, REC_HEADS * DV)
    attn_part = SB_HEADS * HEAD // N_TP
    rec_part = REC_HEADS * DV // N_TP
    mixed = jnp.zeros((SEQS * LENGTH, D), jnp.float32)
    for group in range(N_TP):
        attn_slice = attn_flat[:, group * attn_part:(group + 1) * attn_part]
        rec_slice = rec_flat[:, group * rec_part:(group + 1) * rec_part]
        partial_value = jnp.dot(attn_slice, out_attn[group * attn_part:(group + 1) * attn_part], preferred_element_type=jnp.float32) + jnp.dot(rec_slice, out_rec[group * rec_part:(group + 1) * rec_part], preferred_element_type=jnp.float32)
        mixed = mixed + lax.optimization_barrier(partial_value.astype(jnp.bfloat16)).astype(jnp.float32)
    return mixed.astype(jnp.bfloat16).reshape(SEQS, LENGTH, D)
```

```python
import functools
import math

import jax
import jax.numpy as jnp
from jax import lax
from jax.experimental import pallas as pl
from jax.experimental.pallas import tpu as pltpu
from jax.sharding import PartitionSpec as P

LANES = 128
norm_eps = 1e-06
MESH = pl.DeviceIdType.MESH
F32 = jnp.float32
BF16 = jnp.bfloat16
N_PROJ = 6
GROUPS = 2
CHUNKS = 2


def dot_nn(a, b):
    return lax.dot_general(a, b, (((1,), (0,)), ((), ())), preferred_element_type=F32)


def dot_nt(a, b):
    return lax.dot_general(a, b, (((1,), (1,)), ((), ())), preferred_element_type=F32)


def dot_tn(a, b):
    return lax.dot_general(a, b, (((0,), (0,)), ((), ())), preferred_element_type=F32)


def halves(x):
    high = x.astype(BF16)
    return high, (x - high.astype(F32)).astype(BF16)


def kernel(
    n_sp, n_fs, n_tp,
    tok_hbm, gain_hbm, w_k, w_v, w_f, w_i, w_q, w_r, offs_hbm, room_hbm, out_gain_hbm, o_attn, o_rec,
    out,
    gain, offs, room, out_gain,
    tok, wbuf, obuf, xt, xg, ss, acc, psend, precv, kv, qbuf, qdec, ecum, kinv,
    att, run, loc, st_loc, dec, st_in, st_out, heads, hrecv, part_acc, part, precv2, mix, mrecv,
    t_sem, s_sem, w_sem, x_send, x_recv, f_send, ss_send, ss_recv, p_send, p_recv, kv_send, kv_recv,
    st_sem, h_send, h_recv, pp_send, pp_recv, m_send, m_recv,
):
    sp, fs, tp = lax.axis_index("sp"), lax.axis_index("fs"), lax.axis_index("tp")
    rows, feat_t = tok.shape
    feat_f = xt.shape[2]
    width = feat_t * n_tp
    cols = wbuf.shape[2]
    n_heads = cols // LANES
    share = rows // n_tp
    out_cols = obuf.shape[2]
    has_next = sp < n_sp - 1
    has_prev = sp > 0

    def fs_at(step):
        return lax.rem(fs + step, n_fs)

    def tp_at(step):
        return lax.rem(tp + step, n_tp)

    tok_copy = pltpu.make_async_copy(tok_hbm, tok, t_sem.at[0])
    tok_copy.start()
    small_copies = [
        pltpu.make_async_copy(source, target, s_sem.at[i])
        for i, (source, target) in enumerate(
            ((gain_hbm, gain), (offs_hbm, offs), (room_hbm, room), (out_gain_hbm, out_gain))
        )
    ]
    for copy in small_copies:
        copy.start()
    w_copies = [
        pltpu.make_async_copy(w, wbuf.at[i], w_sem.at[i])
        for i, w in enumerate((w_k, w_v, w_f, w_i, w_q, w_r))
    ]
    w_copies += [
        pltpu.make_async_copy(w, obuf.at[i], w_sem.at[N_PROJ + i])
        for i, w in enumerate((o_attn, o_rec))
    ]
    barrier = pltpu.get_barrier_semaphore()
    for df in range(n_fs):
        for dt in range(n_tp):
            if df or dt:
                pl.semaphore_signal(
                    barrier, inc=1, device_id={"fs": fs_at(df), "tp": tp_at(dt)}, device_id_type=MESH
                )

    @pl.when(has_next)
    def _():
        pl.semaphore_signal(barrier, inc=1, device_id={"sp": sp + 1}, device_id_type=MESH)

    @pl.when(has_prev)
    def _():
        pl.semaphore_signal(barrier, inc=1, device_id={"sp": sp - 1}, device_id_type=MESH)

    for copy in w_copies:
        copy.start()
    tok_copy.wait()

    next_count = jnp.where(has_next, 1, 0)
    prev_count = jnp.where(has_prev, 1, 0)
    pl.semaphore_wait(barrier, n_fs * n_tp - 1 + next_count + prev_count)

    def holder(f_index):
        return (f_index * feat_f) // feat_t

    def x_copy(df, dt):
        dest = fs_at(df)
        start = pl.multiple_of(lax.rem(dest * feat_f, feat_t), LANES)
        part_rows = rows if df == 0 else share
        first = 0 if df == 0 else pl.multiple_of(tp_at(dt) * share, share)
        piece = tp if df == 0 else tp_at(dt)
        return pltpu.make_async_remote_copy(
            src_ref=tok.at[pl.ds(first, part_rows), pl.ds(start, feat_f)],
            dst_ref=xt.at[fs, pl.ds(first, part_rows)],
            send_sem=x_send.at[df * n_tp + dt],
            recv_sem=x_recv.at[fs * n_tp + piece],
            device_id={"fs": dest, "tp": tp_at(dt)},
            device_id_type=MESH,
        )

    def f_copy(df, dt):
        slot = fs_at(df)
        first = pl.multiple_of(tp * share, share)
        return pltpu.make_async_remote_copy(
            src_ref=xt.at[slot, pl.ds(first, share)],
            dst_ref=xt.at[slot, pl.ds(first, share)],
            send_sem=f_send.at[df * n_tp + dt],
            recv_sem=x_recv.at[slot * n_tp + tp],
            device_id={"tp": tp_at(dt)},
            device_id_type=MESH,
        )

    x_order = [(df, dt) for df in list(range(1, n_fs)) + [0] for dt in range(n_tp) if df or dt]
    for df, dt in x_order:
        @pl.when(holder(fs_at(df)) == tp)
        def _(df=df, dt=dt):
            x_copy(df, dt).start()

    squares = jnp.zeros((rows, LANES), F32)
    for c in range(feat_t // LANES):
        piece = tok[:, c * LANES:(c + 1) * LANES].astype(F32)
        squares = squares + piece * piece
    ss[tp] = squares

    def ss_copy(dt):
        return pltpu.make_async_remote_copy(
            src_ref=ss.at[tp], dst_ref=ss.at[tp],
            send_sem=ss_send.at[dt - 1], recv_sem=ss_recv.at[tp],
            device_id={"tp": tp_at(dt)}, device_id_type=MESH,
        )

    for dt in range(1, n_tp):
        ss_copy(dt).start()

    own_holder = holder(fs) == tp
    for copy in small_copies:
        copy.wait()
    gain_f = gain[:, pl.ds(pl.multiple_of(fs * feat_f, LANES), feat_f)]

    @pl.when(own_holder)
    def _():
        start = pl.multiple_of(lax.rem(fs * feat_f, feat_t), LANES)
        xg[0] = (tok[:, pl.ds(start, feat_f)].astype(F32) * gain_f).astype(BF16)

    def x_wait(slot, piece, first, count):
        view = xt.at[slot, pl.ds(first, count)]
        pltpu.make_async_remote_copy(
            src_ref=view, dst_ref=view,
            send_sem=x_send.at[0], recv_sem=x_recv.at[slot * n_tp + piece],
            device_id={"tp": tp_at(1)}, device_id_type=MESH,
        ).wait_recv()

    g_cols = cols // GROUPS
    units = [(w, g * g_cols, g_cols) for g in range(GROUPS) for w in (0, 1)]
    units += [(w, 0, cols) for w in range(2, N_PROJ)]
    n_units = len(units)
    n_kv = 2 * GROUPS

    def p_copy(df, u):
        w, first, count = units[u]
        return pltpu.make_async_remote_copy(
            src_ref=psend.at[df - 1, w, :, pl.ds(first, count)],
            dst_ref=precv.at[df - 1, w, :, pl.ds(first, count)],
            send_sem=p_send.at[(df - 1) * n_units + u], recv_sem=p_recv.at[(df - 1) * n_units + u],
            device_id={"fs": fs_at(df)}, device_id_type=MESH,
        )

    def row_part(dt):
        return pl.ds(pl.multiple_of(tp_at(dt) * share, share), share)

    def first_copy(df, dt):
        index = (n_fs - 1) * n_units + (df - 1) * n_tp + dt
        return pltpu.make_async_remote_copy(
            src_ref=psend.at[df - 1, 0, row_part(dt), pl.ds(0, g_cols)],
            dst_ref=precv.at[df - 1, 0, row_part(dt), pl.ds(0, g_cols)],
            send_sem=p_send.at[index], recv_sem=p_recv.at[index],
            device_id={"fs": fs_at(df)}, device_id_type=MESH,
        )

    def first_part(df, dt):
        mine = row_part(dt)
        xg[df, mine, :] = (xt[fs_at(df), mine, :].astype(F32) * gain_f).astype(BF16)
        psend[df - 1, 0, mine, 0:g_cols] = dot_nn(xg[df, mine, :], wbuf[0, :, 0:g_cols]).astype(BF16)
        first_copy(df, dt).start()

    w_copies[0].wait()
    for df in range(1, n_fs):
        slot = fs_at(df)
        x_wait(slot, tp, pl.multiple_of(tp * share, share), share)
        for dt in range(1, n_tp):
            f_copy(df, dt).start()
        first_part(df, 0)
    for df in range(1, n_fs):
        slot = fs_at(df)
        for dt in range(1, n_tp):
            piece = tp_at(dt)
            x_wait(slot, piece, pl.multiple_of(piece * share, share), share)
            first_part(df, dt)
    for u, (w, first, count) in enumerate(units):
        if u == 0:
            continue
        if first == 0:
            w_copies[w].wait()
        cut = slice(first, first + count)
        for df in range(1, n_fs):
            psend[df - 1, w, :, cut] = dot_nn(xg[df], wbuf[w, :, cut]).astype(BF16)
            p_copy(df, u).start()

    @pl.when(jnp.logical_not(own_holder))
    def _():
        x_wait(fs, holder(fs), 0, rows)
        xg[0] = (xt[fs].astype(F32) * gain_f).astype(BF16)

    for w in range(N_PROJ):
        acc[w] = dot_nn(xg[0], wbuf[w])

    total = ss[tp]
    for dt in range(1, n_tp):
        other = tp_at(dt)
        pltpu.make_async_remote_copy(
            src_ref=ss.at[other], dst_ref=ss.at[other],
            send_sem=ss_send.at[dt - 1], recv_sem=ss_recv.at[other],
            device_id={"tp": other}, device_id_type=MESH,
        ).wait_recv()
        total = total + ss[other]
    factor = lax.rsqrt(jnp.sum(total, axis=1, keepdims=True) / width + norm_eps)

    def finish(u):
        w, first, count = units[u]
        cut = slice(first, first + count)
        value = acc[w, :, cut]
        for df in range(1, n_fs):
            if u == 0:
                for dt in range(n_tp):
                    first_copy(df, dt).wait_recv()
            else:
                p_copy(df, u).wait_recv()
            value = value + precv[df - 1, w, :, cut].astype(F32)
        return (value * factor).astype(BF16)

    def kv_copy(slot, c):
        return pltpu.make_async_remote_copy(
            src_ref=kv.at[slot, c], dst_ref=kv.at[slot, c],
            send_sem=kv_send.at[slot * n_kv + c], recv_sem=kv_recv.at[slot * n_kv + c],
            device_id={"sp": lax.rem(sp + 1, n_sp)}, device_id_type=MESH,
        )

    for c in range(n_kv):
        kv[sp, c] = finish(c)

        @pl.when(has_next)
        def _(c=c):
            kv_copy(sp, c).start()

    def hand_on(step, c):
        kv_copy(sp - step, c).wait_recv()

        @pl.when(has_next)
        def _():
            kv_copy(sp - step, c).start()

    def hand_on_if(step, c):
        if step < n_sp:
            pl.when(sp >= step)(functools.partial(hand_on, step, c))

    hand_on_if(1, 0)
    hand_on_if(1, 1)
    iota_r = lax.broadcasted_iota(jnp.int32, (rows, rows), 0)
    iota_c = lax.broadcasted_iota(jnp.int32, (rows, rows), 1)
    causal = iota_r >= iota_c
    strict = iota_c < iota_r

    def st_copy(h):
        return pltpu.make_async_remote_copy(
            src_ref=st_out.at[h], dst_ref=st_in.at[h],
            send_sem=st_sem.at[h], recv_sem=st_sem.at[n_heads + h],
            device_id={"sp": lax.rem(sp + 1, n_sp)}, device_id_type=MESH,
        )

    lower = jnp.where(causal, 1.0, 0.0).astype(BF16)
    forget_pre = finish(n_kv)
    for c in range(2, n_kv):
        hand_on_if(1, c)
    rec_i = finish(n_kv + 1)
    for h in range(n_heads):
        lanes = slice(h * LANES, (h + 1) * LANES)
        key_in = room[h:h + 1, :] * jax.nn.sigmoid(-forget_pre[:, lanes].astype(F32))
        high, low = halves(jnp.log1p(-key_in))
        cum = dot_nn(lower, high) + dot_nn(lower, low)
        last = cum[rows - 1:rows, :]
        ecum[:, lanes] = jnp.exp(cum)
        kinv[:, lanes] = (key_in * jnp.exp(-cum)).astype(BF16)
        fresh = (key_in * jnp.exp(last - cum)).astype(BF16)
        st_loc[h] = dot_tn(rec_i[:, lanes], fresh)
        dec[h] = jnp.broadcast_to(jnp.exp(last), dec.shape[1:])

        @pl.when(jnp.logical_and(sp == 0, has_next))
        def _(h=h):
            st_out[h] = st_loc[h].astype(BF16)
            st_copy(h).start()

    hand_on_if(2, 0)
    hand_on_if(2, 1)

    qbuf[...] = finish(n_kv + 2)
    later = jnp.where(iota_r > iota_c, 1.0, 0.0).astype(BF16)
    sums = jnp.concatenate([later, jnp.ones((rows, LANES), BF16)], axis=1)
    scale = 1.0 / math.sqrt(LANES)

    g_heads = n_heads // GROUPS

    def attend(slot, g, diagonal):
        for h in range(g * g_heads, (g + 1) * g_heads):
            lanes = slice(h * LANES, (h + 1) * LANES)
            inner = slice((h - g * g_heads) * LANES, (h - g * g_heads + 1) * LANES)
            z = dot_nt(qbuf[:, lanes], kv[slot, 2 * g, :, inner]) * scale + offs[0:1, h:h + 1]
            keep = -(jnp.maximum(z, 0.0) + jnp.log1p(jnp.exp(-jnp.abs(z))))
            log_stick = z + keep
            if diagonal:
                keep = jnp.where(strict, keep, 0.0)
            high, low = halves(keep)
            both = dot_nn(high, sums) + dot_nn(low, sums)
            stick = jnp.exp(log_stick + both[:, :rows])
            if diagonal:
                stick = jnp.where(strict, stick, 0.0)
            value = dot_nn(stick.astype(BF16), kv[slot, 2 * g + 1, :, inner])
            if diagonal:
                att[:, lanes] = value
                run[h] = both[:, rows:]
            else:
                past = run[h]
                att[:, lanes] += value * jnp.exp(past)
                run[h] = past + both[:, rows:]

    def attend_if(step):
        if step < n_sp:
            @pl.when(sp >= step)
            def _():
                for g in range(GROUPS):
                    attend(sp - step, g, False)

    for g in range(GROUPS):
        attend(sp, g, True)
    for c in range(2, n_kv):
        hand_on_if(2, c)
    attend_if(1)
    rec_q = finish(n_kv + 3)
    for h in range(n_heads):
        lanes = slice(h * LANES, (h + 1) * LANES)
        decayed = (rec_q[:, lanes].astype(F32) * ecum[:, lanes]).astype(BF16)
        qdec[:, lanes] = decayed
        scores = jnp.where(causal, dot_nt(decayed, kinv[:, lanes]), 0.0)
        loc[:, lanes] = dot_nn(scores.astype(BF16), rec_i[:, lanes])

    attend_if(2)

    def block(step, carry):
        for c in range(n_kv):
            hand_on(step, c)
        for g in range(GROUPS):
            attend(sp - step, g, False)
        return carry

    lax.fori_loop(3, sp, block, 0)

    n_head_units = GROUPS + n_heads

    def h_copy(df, c):
        index = (df - 1) * n_head_units + c
        if c < GROUPS:
            lanes = pl.ds(c * g_cols, g_cols)
            source, target = heads.at[0, :, lanes], hrecv.at[df - 1, 0, :, lanes]
        else:
            lanes = pl.ds((c - GROUPS) * LANES, LANES)
            source, target = heads.at[1, :, lanes], hrecv.at[df - 1, 1, :, lanes]
        return pltpu.make_async_remote_copy(
            src_ref=source, dst_ref=target, send_sem=h_send.at[index], recv_sem=h_recv.at[index],
            device_id={"fs": fs_at(df)}, device_id_type=MESH,
        )

    for g in range(GROUPS):
        @pl.when(sp >= 3)
        def _(g=g):
            for c in (2 * g, 2 * g + 1):
                hand_on(sp, c)
            attend(0, g, False)

        cut = slice(g * g_cols, (g + 1) * g_cols)
        heads[0, :, cut] = att[:, cut].astype(BF16)
        for df in range(1, n_fs):
            h_copy(df, g).start()

    for h in range(n_heads):
        lanes = slice(h * LANES, (h + 1) * LANES)

        @pl.when(has_prev)
        def _(h=h, lanes=lanes):
            st_copy(h).wait_recv()

            @pl.when(has_next)
            def _():
                st_out[h] = (st_in[h].astype(F32) * dec[h, 0:1, :] + st_loc[h]).astype(BF16)
                st_copy(h).start()

            loc[:, lanes] += dot_nt(qdec[:, lanes], st_in[h])

        raw = loc[:, lanes]
        norm = lax.rsqrt(jnp.mean(raw * raw, axis=1, keepdims=True) + norm_eps)
        heads[1, :, lanes] = (raw * norm * out_gain[...]).astype(BF16)
        for df in range(1, n_fs):
            h_copy(df, GROUPS + h).start()

    w_copies[N_PROJ].wait()
    w_copies[N_PROJ + 1].wait()

    half = out_cols // CHUNKS

    def pp_copy(df, dt, k):
        index = (df * (n_tp - 1) + dt - 1) * CHUNKS + k
        start = pl.multiple_of(tp_at(dt) * share, share)
        return pltpu.make_async_remote_copy(
            src_ref=part.at[df, k, pl.ds(start, share)], dst_ref=precv2.at[dt - 1, df, k],
            send_sem=pp_send.at[index], recv_sem=pp_recv.at[index],
            device_id={"tp": tp_at(dt)}, device_id_type=MESH,
        )

    def m_copy(df, k):
        index = (df - 1) * CHUNKS + k
        return pltpu.make_async_remote_copy(
            src_ref=mix.at[df - 1, k], dst_ref=mrecv.at[df - 1, k],
            send_sem=m_send.at[index], recv_sem=m_recv.at[index],
            device_id={"fs": fs_at(df)}, device_id_type=MESH,
        )

    def reduced(df, k):
        value = part[df, k, pl.ds(pl.multiple_of(tp * share, share), share)].astype(F32)
        for dt in range(1, n_tp):
            pp_copy(df, dt, k).wait_recv()
            value = value + precv2[dt - 1, df, k].astype(F32)
        return value.astype(BF16)

    def columns(owner, k):
        return pl.ds(pl.multiple_of(owner * out_cols + k * half, LANES), half)

    for df in range(1, n_fs):
        for g in range(GROUPS):
            h_copy(df, g).wait_recv()
        for k in range(CHUNKS):
            part_acc[df - 1, k] = dot_nn(hrecv[df - 1, 0], obuf[0, :, k * half:(k + 1) * half])
    for k in range(CHUNKS):
        cut = slice(k * half, (k + 1) * half)
        part[0, k] = (dot_nn(heads[0], obuf[0, :, cut]) + dot_nn(heads[1], obuf[1, :, cut])).astype(BF16)
        for dt in range(1, n_tp):
            pp_copy(0, dt, k).start()
    for df in range(1, n_fs):
        for h in range(n_heads):
            h_copy(df, GROUPS + h).wait_recv()
        for k in range(CHUNKS):
            cut = slice(k * half, (k + 1) * half)
            part[df, k] = (part_acc[df - 1, k] + dot_nn(hrecv[df - 1, 1], obuf[1, :, cut])).astype(BF16)
            for dt in range(1, n_tp):
                pp_copy(df, dt, k).start()
    for df in range(1, n_fs):
        for k in range(CHUNKS):
            mix[df - 1, k] = reduced(df, k)
            m_copy(df, k).start()
    for k in range(CHUNKS):
        out[:, columns(fs, k)] = reduced(0, k)
    for df in range(1, n_fs):
        source = lax.rem(fs + n_fs - df, n_fs)
        for k in range(CHUNKS):
            m_copy(df, k).wait_recv()
            out[:, columns(source, k)] = mrecv[df - 1, k]

    for df, dt in x_order:
        @pl.when(holder(fs_at(df)) == tp)
        def _(df=df, dt=dt):
            x_copy(df, dt).wait_send()
    for dt in range(1, n_tp):
        ss_copy(dt).wait_send()
        for df in range(1, n_fs):
            f_copy(df, dt).wait_send()
    for df in range(1, n_fs):
        for dt in range(n_tp):
            first_copy(df, dt).wait_send()
        for u in range(1, n_units):
            p_copy(df, u).wait_send()
        for c in range(n_head_units):
            h_copy(df, c).wait_send()
    for k in range(CHUNKS):
        for df in range(1, n_fs):
            m_copy(df, k).wait_send()
        for df in range(n_fs):
            for dt in range(1, n_tp):
                pp_copy(df, dt, k).wait_send()

    @pl.when(has_next)
    def _():
        for h in range(n_heads):
            st_copy(h).wait_send()

        def drain(slot, carry):
            for c in range(n_kv):
                kv_copy(slot, c).wait_send()
            return carry

        lax.fori_loop(0, sp + 1, drain, 0)


def body(
    tokens, mix_gain, attn_query, attn_key, attn_value, rec_query, rec_forget, rec_input,
    break_offset, forget_room, out_gain, out_attn, out_rec,
):
    n_sp, n_fs, n_tp = lax.axis_size("sp"), lax.axis_size("fs"), lax.axis_size("tp")
    rows, feat_t = tokens.shape[1], tokens.shape[2]
    feat_f, cols = attn_query.shape
    width = feat_t * n_tp
    n_heads = cols // LANES
    out_rows, out_cols = out_attn.shape
    share = rows // n_tp
    piece = out_cols // CHUNKS
    n_units = 2 * GROUPS + N_PROJ - 2
    vmem = pl.BlockSpec(memory_space=pltpu.VMEM)
    hbm = pl.BlockSpec(memory_space=pl.ANY)
    dma = pltpu.SemaphoreType.DMA
    square = (n_heads, LANES, LANES)
    result = pl.pallas_call(
        functools.partial(kernel, n_sp, n_fs, n_tp),
        out_shape=pltpu.VMEM((share, width), BF16),
        in_specs=[hbm] * 13,
        out_specs=vmem,
        scratch_shapes=[
            pltpu.VMEM((1, width), F32),
            pltpu.VMEM((1, n_heads), F32),
            pltpu.VMEM((n_heads, LANES), F32),
            pltpu.VMEM((1, LANES), F32),
            pltpu.VMEM((rows, feat_t), BF16),
            pltpu.VMEM((N_PROJ, feat_f, cols), BF16),
            pltpu.VMEM((2, out_rows, out_cols), BF16),
            pltpu.VMEM((n_fs, rows, feat_f), BF16),
            pltpu.VMEM((n_fs, rows, feat_f), BF16),
            pltpu.VMEM((n_tp, rows, LANES), F32),
            pltpu.VMEM((N_PROJ, rows, cols), F32),
            pltpu.VMEM((n_fs - 1, N_PROJ, rows, cols), BF16),
            pltpu.VMEM((n_fs - 1, N_PROJ, rows, cols), BF16),
            pltpu.VMEM((n_sp, 2 * GROUPS, rows, cols // GROUPS), BF16),
            pltpu.VMEM((rows, cols), BF16),
            pltpu.VMEM((rows, cols), BF16),
            pltpu.VMEM((rows, cols), F32),
            pltpu.VMEM((rows, cols), BF16),
            pltpu.VMEM((rows, cols), F32),
            pltpu.VMEM((n_heads, rows, LANES), F32),
            pltpu.VMEM((rows, cols), F32),
            pltpu.VMEM(square, F32),
            pltpu.VMEM((n_heads, 8, LANES), F32),
            pltpu.VMEM(square, BF16),
            pltpu.VMEM(square, BF16),
            pltpu.VMEM((2, rows, cols), BF16),
            pltpu.VMEM((n_fs - 1, 2, rows, cols), BF16),
            pltpu.VMEM((n_fs - 1, CHUNKS, rows, piece), F32),
            pltpu.VMEM((n_fs, CHUNKS, rows, piece), BF16),
            pltpu.VMEM((n_tp - 1, n_fs, CHUNKS, share, piece), BF16),
            pltpu.VMEM((n_fs - 1, CHUNKS, share, piece), BF16),
            pltpu.VMEM((n_fs - 1, CHUNKS, share, piece), BF16),
            dma((1,)), dma((4,)), dma((N_PROJ + 2,)),
            dma((n_fs * n_tp,)), dma((n_fs * n_tp,)), dma((n_fs * n_tp,)),
            dma((n_tp - 1,)), dma((n_tp,)),
            dma(((n_fs - 1) * (n_units + n_tp),)), dma(((n_fs - 1) * (n_units + n_tp),)),
            dma((n_sp * 2 * GROUPS,)), dma((n_sp * 2 * GROUPS,)),
            dma((2 * n_heads,)),
            dma(((n_fs - 1) * (GROUPS + n_heads),)), dma(((n_fs - 1) * (GROUPS + n_heads),)),
            dma((n_fs * (n_tp - 1) * CHUNKS,)), dma((n_fs * (n_tp - 1) * CHUNKS,)),
            dma(((n_fs - 1) * CHUNKS,)), dma(((n_fs - 1) * CHUNKS,)),
        ],
        compiler_params=pltpu.CompilerParams(
            collective_id=0, has_side_effects=True, vmem_limit_bytes=60 * 1024 * 1024
        ),
        name="layer",
    )(
        tokens.reshape(rows, feat_t), mix_gain.reshape(1, width),
        attn_key, attn_value, rec_forget, rec_input, attn_query, rec_query,
        break_offset.reshape(1, n_heads), forget_room, out_gain.reshape(1, LANES), out_attn, out_rec,
    )
    return result.reshape(1, share, width)


def solution(mesh):
    placed = (
        P(("grp", "fs"), "sp", "tp"),
        P(),
        P("fs", "tp"),
        P("fs", "tp"),
        P("fs", "tp"),
        P("fs", "tp"),
        P("fs", "tp"),
        P("fs", "tp"),
        P("tp"),
        P("tp", None),
        P(),
        P("tp", "fs"),
        P("tp", "fs"),
    )
    return jax.shard_map(
        body,
        mesh=mesh,
        in_specs=placed,
        out_specs=P(("grp", "fs"), ("sp", "tp"), None),
        check_vma=False,
    )
```

```python
import functools
import math

import jax
import jax.numpy as jnp
from jax import lax
from jax.experimental import pallas as pl
from jax.experimental.pallas import tpu as pltpu
from jax.sharding import PartitionSpec as P

LANES = 128
norm_eps = 1e-06
MESH = pl.DeviceIdType.MESH
F32 = jnp.float32
BF16 = jnp.bfloat16
N_PROJ = 6
KEY, VALUE, FORGET, INPUT, QUERY, READ = range(N_PROJ)
GROUPS = 2
CHUNKS = 2
X_CHUNKS = 4
N_SMALL = 4


def dot_nn(a, b):
    return lax.dot_general(a, b, (((1,), (0,)), ((), ())), preferred_element_type=F32)


def dot_nt(a, b):
    return lax.dot_general(a, b, (((1,), (1,)), ((), ())), preferred_element_type=F32)


def dot_tn(a, b):
    return lax.dot_general(a, b, (((0,), (0,)), ((), ())), preferred_element_type=F32)


def halves(x):
    high = x.astype(BF16)
    return high, (x - high.astype(F32)).astype(BF16)


def unit_list(cols):
    g_cols = cols // GROUPS
    units = [(w, 0) for w in (FORGET, INPUT)]
    for g in range(1, GROUPS):
        units += [(w, g * g_cols) for w in (KEY, VALUE, FORGET, INPUT)]
    units += [(w, g * g_cols) for w in (QUERY, READ) for g in range(GROUPS)]
    return units


def kernel(
    n_sp, n_fs, n_tp,
    tok_hbm, gain_hbm, w_k, w_v, w_f, w_i, w_q, w_r, offs_hbm, room_hbm, out_gain_hbm, o_attn, o_rec,
    out,
    gain, offs, room, out_gain,
    tok, wbuf, obuf, xt, xg, ss, acc, psend, precv, kv, qbuf, qdec, ecum, kinv, fresh, rec_i,
    att, run, loc, st_loc, dec, st_in, st_out, heads, hrecv, part_acc, mix, mrecv,
    t_sem, s_sem, w_sem, x_send, x_recv, f_send, own_send, own_recv, ss_send, ss_recv, p_send, p_recv,
    kv_send, kv_recv, st_send, st_recv, o_send, o_recv, h_send, h_recv, m_send, m_recv,
):
    sp, fs, tp = lax.axis_index("sp"), lax.axis_index("fs"), lax.axis_index("tp")
    rows, feat_t = tok.shape
    feat_f = xt.shape[2]
    width = feat_t * n_tp
    cols = wbuf.shape[2]
    n_heads = cols // LANES
    share = rows // n_tp
    out_cols = obuf.shape[3]
    g_cols = cols // GROUPS
    g_heads = n_heads // GROUPS
    n_kv = X_CHUNKS + 2 * (GROUPS - 1)
    x_rows = rows // X_CHUNKS
    relay = 0
    is_relay = tp == relay
    has_next = sp < n_sp - 1
    has_prev = sp > 0

    def fs_at(step):
        return lax.rem(fs + step, n_fs)

    def tp_at(step):
        return lax.rem(tp + step, n_tp)

    def group(g):
        return slice(g * g_cols, (g + 1) * g_cols)

    tok_copy = pltpu.make_async_copy(tok_hbm, tok, t_sem.at[0])
    tok_copy.start()
    barrier = pltpu.get_barrier_semaphore()
    for df in range(n_fs):
        for dt in range(n_tp):
            if df or dt:
                pl.semaphore_signal(
                    barrier, inc=1, device_id={"fs": fs_at(df), "tp": tp_at(dt)}, device_id_type=MESH
                )

    @pl.when(has_next)
    def _():
        pl.semaphore_signal(barrier, inc=1, device_id={"sp": sp + 1}, device_id_type=MESH)

    @pl.when(has_prev)
    def _():
        pl.semaphore_signal(barrier, inc=1, device_id={"sp": sp - 1}, device_id_type=MESH)

    small_copies = [
        pltpu.make_async_copy(source, target, s_sem.at[i])
        for i, (source, target) in enumerate(
            ((gain_hbm, gain), (offs_hbm, offs), (room_hbm, room), (out_gain_hbm, out_gain))
        )
    ]
    w_copies = [
        pltpu.make_async_copy(w, wbuf.at[i], w_sem.at[i])
        for i, w in enumerate((w_k, w_v, w_f, w_i, w_q, w_r))
    ]
    o_copies = [
        pltpu.make_async_copy(w, obuf.at[tp, i], w_sem.at[N_PROJ + i]) for i, w in enumerate((o_attn, o_rec))
    ]
    for copy in small_copies + w_copies + o_copies:
        copy.start()
    tok_copy.wait()

    next_count = jnp.where(has_next, 1, 0)
    prev_count = jnp.where(has_prev, 1, 0)
    pl.semaphore_wait(barrier, n_fs * n_tp - 1 + next_count + prev_count)

    def holder(f_index):
        return (f_index * feat_f) // feat_t

    def held(f_index):
        return pl.ds(pl.multiple_of(lax.rem(f_index * feat_f, feat_t), LANES), feat_f)

    def x_part(c):
        return pl.ds(c * x_rows, x_rows)

    def x_copy(df, c):
        return pltpu.make_async_remote_copy(
            src_ref=tok.at[x_part(c), held(fs_at(df))], dst_ref=xt.at[fs, x_part(c)],
            send_sem=x_send.at[(df - 1) * X_CHUNKS + c], recv_sem=x_recv.at[fs * X_CHUNKS + c],
            device_id={"fs": fs_at(df), "tp": relay}, device_id_type=MESH,
        )

    def f_copy(df, c, dt):
        slot = fs_at(df)
        return pltpu.make_async_remote_copy(
            src_ref=xt.at[slot, x_part(c)], dst_ref=xt.at[slot, x_part(c)],
            send_sem=f_send.at[((df - 1) * X_CHUNKS + c) * (n_tp - 1) + dt - 1],
            recv_sem=x_recv.at[slot * X_CHUNKS + c],
            device_id={"tp": tp_at(dt)}, device_id_type=MESH,
        )

    def own_copy(dt):
        return pltpu.make_async_remote_copy(
            src_ref=tok.at[:, held(fs)], dst_ref=xt.at[fs],
            send_sem=own_send.at[dt - 1], recv_sem=own_recv.at[0],
            device_id={"tp": tp_at(dt)}, device_id_type=MESH,
        )

    for df in range(1, n_fs):
        @pl.when(holder(fs_at(df)) == tp)
        def _(df=df):
            for c in range(X_CHUNKS):
                x_copy(df, c).start()

    own_holder = holder(fs) == tp

    @pl.when(own_holder)
    def _():
        for dt in range(1, n_tp):
            own_copy(dt).start()

    squares = jnp.zeros((rows, LANES), F32)
    for c in range(feat_t // LANES):
        piece = tok[:, c * LANES:(c + 1) * LANES].astype(F32)
        squares = squares + piece * piece
    ss[tp] = squares

    def ss_copy(dt):
        return pltpu.make_async_remote_copy(
            src_ref=ss.at[tp], dst_ref=ss.at[tp],
            send_sem=ss_send.at[dt - 1], recv_sem=ss_recv.at[tp],
            device_id={"tp": tp_at(dt)}, device_id_type=MESH,
        )

    for dt in range(1, n_tp):
        ss_copy(dt).start()

    for copy in small_copies:
        copy.wait()
    gain_f = gain[:, pl.ds(pl.multiple_of(fs * feat_f, LANES), feat_f)]

    @pl.when(own_holder)
    def _():
        xg[0] = (tok[:, held(fs)].astype(F32) * gain_f).astype(BF16)

    units = unit_list(cols)
    n_units = len(units)

    def first_copy(df, c):
        index = (df - 1) * (n_units + X_CHUNKS) + n_units + c
        return pltpu.make_async_remote_copy(
            src_ref=psend.at[df - 1, pl.ds(KEY, 2), x_part(c), pl.ds(0, g_cols)],
            dst_ref=precv.at[df - 1, pl.ds(KEY, 2), x_part(c), pl.ds(0, g_cols)],
            send_sem=p_send.at[index], recv_sem=p_recv.at[index],
            device_id={"fs": fs_at(df)}, device_id_type=MESH,
        )

    def p_copy(df, u):
        w, first = units[u]
        index = (df - 1) * (n_units + X_CHUNKS) + u
        return pltpu.make_async_remote_copy(
            src_ref=psend.at[df - 1, w, :, pl.ds(first, g_cols)],
            dst_ref=precv.at[df - 1, w, :, pl.ds(first, g_cols)],
            send_sem=p_send.at[index], recv_sem=p_recv.at[index],
            device_id={"fs": fs_at(df)}, device_id_type=MESH,
        )

    @pl.when(jnp.logical_not(own_holder))
    def _():
        pltpu.make_async_remote_copy(
            src_ref=xt.at[fs], dst_ref=xt.at[fs], send_sem=own_send.at[0], recv_sem=own_recv.at[0],
            device_id={"tp": tp_at(1)}, device_id_type=MESH,
        ).wait_recv()
        xg[0] = (xt[fs].astype(F32) * gain_f).astype(BF16)

    total = ss[tp]
    for dt in range(1, n_tp):
        other = tp_at(dt)
        pltpu.make_async_remote_copy(
            src_ref=ss.at[other], dst_ref=ss.at[other],
            send_sem=ss_send.at[dt - 1], recv_sem=ss_recv.at[other],
            device_id={"tp": other}, device_id_type=MESH,
        ).wait_recv()
        total = total + ss[other]
    factor = lax.rsqrt(jnp.sum(total, axis=1, keepdims=True) / width + norm_eps)

    def own_product(w, cut):
        acc[w, :, cut] = dot_nn(xg[0], wbuf[w, :, cut])

    w_copies[KEY].wait()
    own_product(KEY, group(0))
    w_copies[VALUE].wait()
    own_product(VALUE, group(0))
    for c in range(X_CHUNKS):
        part = slice(c * x_rows, (c + 1) * x_rows)
        for df in range(1, n_fs):
            slot = fs_at(df)
            view = xt.at[slot, x_part(c)]
            pltpu.make_async_remote_copy(
                src_ref=view, dst_ref=view, send_sem=x_send.at[0], recv_sem=x_recv.at[slot * X_CHUNKS + c],
                device_id={"tp": tp_at(1)}, device_id_type=MESH,
            ).wait_recv()

            @pl.when(is_relay)
            def _(df=df, c=c):
                for dt in range(1, n_tp):
                    f_copy(df, c, dt).start()

            xg[df, part, :] = (xt[slot, part, :].astype(F32) * gain_f).astype(BF16)
            for w in (KEY, VALUE):
                psend[df - 1, w, part, 0:g_cols] = dot_nn(xg[df, part, :], wbuf[w, :, 0:g_cols]).astype(BF16)
            first_copy(df, c).start()

    def partials(w, first, count):
        cut = slice(first, first + count)
        for df in range(1, n_fs):
            psend[df - 1, w, :, cut] = dot_nn(xg[df], wbuf[w, :, cut]).astype(BF16)

    def send_unit(w, g):
        for df in range(1, n_fs):
            p_copy(df, units.index((w, g * g_cols))).start()


    def finish(w, g):
        cut = group(g)
        value = acc[w, :, cut]
        for df in range(1, n_fs):
            p_copy(df, units.index((w, g * g_cols))).wait_recv()
            value = value + precv[df - 1, w, :, cut].astype(F32)
        return (value * factor).astype(BF16)

    def kv_copy(slot, c):
        if c < X_CHUNKS:
            view = kv.at[slot, pl.ds(0, 2), x_part(c)]
        else:
            view = kv.at[slot, 2 + c - X_CHUNKS]
        return pltpu.make_async_remote_copy(
            src_ref=view, dst_ref=view,
            send_sem=kv_send.at[slot * n_kv + c], recv_sem=kv_recv.at[slot * n_kv + c],
            device_id={"sp": lax.rem(sp + 1, n_sp)}, device_id_type=MESH,
        )

    def group_kv(g):
        if g == 0:
            return range(X_CHUNKS)
        return range(X_CHUNKS + 2 * (g - 1), X_CHUNKS + 2 * g)

    def send_kv(c):
        @pl.when(has_next)
        def _():
            kv_copy(sp, c).start()

    def finish_first(c):
        part = slice(c * x_rows, (c + 1) * x_rows)
        for df in range(1, n_fs):
            first_copy(df, c).wait_recv()
        for w in (KEY, VALUE):
            value = acc[w, part, 0:g_cols]
            for df in range(1, n_fs):
                value = value + precv[df - 1, w, part, 0:g_cols].astype(F32)
            kv[sp, w, part, :] = (value * factor[part]).astype(BF16)
        send_kv(c)

    def finish_kv(w, g):
        kv[sp, 2 * g + w] = finish(w, g)
        send_kv(X_CHUNKS + 2 * (g - 1) + w)

    def hand_on(step, c):
        kv_copy(sp - step, c).wait_recv()

        @pl.when(has_next)
        def _():
            kv_copy(sp - step, c).start()

    def hand_on_if(step, c):
        if step < n_sp:
            pl.when(sp >= step)(functools.partial(hand_on, step, c))

    for w in (FORGET, INPUT):
        w_copies[w].wait()
        partials(w, 0, cols)
        send_unit(w, 0)
        finish_first(w - FORGET)
    for w in (KEY, VALUE):
        partials(w, g_cols, cols - g_cols)
        for g in range(1, GROUPS):
            send_unit(w, g)
        finish_first(2 + w)
    for c in range(4, X_CHUNKS):
        finish_first(c)
    for w in (FORGET, INPUT):
        for g in range(1, GROUPS):
            send_unit(w, g)
    for w in (QUERY, READ):
        w_copies[w].wait()
        partials(w, 0, cols)
        for g in range(GROUPS):
            send_unit(w, g)
    for w in (FORGET, INPUT):
        own_product(w, slice(0, cols))
    for w in (KEY, VALUE):
        own_product(w, slice(g_cols, cols))
    for w in (QUERY, READ):
        own_product(w, slice(0, cols))

    def o_copy(dt):
        return pltpu.make_async_remote_copy(
            src_ref=obuf.at[tp], dst_ref=obuf.at[tp], send_sem=o_send.at[dt - 1], recv_sem=o_recv.at[tp],
            device_id={"tp": tp_at(dt)}, device_id_type=MESH,
        )

    for copy in o_copies:
        copy.wait()
    for dt in range(1, n_tp):
        o_copy(dt).start()

    iota_r = lax.broadcasted_iota(jnp.int32, (rows, rows), 0)
    iota_c = lax.broadcasted_iota(jnp.int32, (rows, rows), 1)
    causal = iota_r >= iota_c
    strict = jnp.concatenate([iota_c < iota_r] * g_heads, axis=0)
    lower = jnp.where(causal, 1.0, 0.0).astype(BF16)
    lower = jnp.concatenate([lower, lower], axis=1)
    later = jnp.where(iota_r > iota_c, 1.0, 0.0).astype(BF16)
    sums = jnp.concatenate([later, jnp.ones((rows, LANES), BF16)], axis=1)
    sums = jnp.concatenate([sums, sums], axis=0)
    scale = 1.0 / math.sqrt(LANES)

    def lanes_of(h):
        return slice(h * LANES, (h + 1) * LANES)

    def heads_of(g):
        return range(g * g_heads, (g + 1) * g_heads)

    def gates(g):
        cut = group(g)
        rooms = jnp.concatenate([room[h:h + 1, :] for h in heads_of(g)], axis=1)
        key_in = rooms * jax.nn.sigmoid(-finish(FORGET, g).astype(F32))
        high, low = halves(jnp.log1p(-key_in))
        cum = dot_nn(lower, jnp.concatenate([high, low], axis=0))
        last = cum[rows - 1:rows, :]
        ecum[:, cut] = jnp.exp(cum)
        kinv[:, cut] = (key_in * jnp.exp(-cum)).astype(BF16)
        fresh[:, cut] = (key_in * jnp.exp(last - cum)).astype(BF16)
        decay = jnp.exp(last)
        for i, h in enumerate(heads_of(g)):
            dec[h] = jnp.broadcast_to(decay[:, lanes_of(i)], dec.shape[1:])

    def st_copy(h):
        return pltpu.make_async_remote_copy(
            src_ref=st_out.at[h], dst_ref=st_in.at[h], send_sem=st_send.at[h], recv_sem=st_recv.at[h],
            device_id={"sp": lax.rem(sp + 1, n_sp)}, device_id_type=MESH,
        )

    def local_state(g):
        rec_i[:, group(g)] = finish(INPUT, g)
        for h in heads_of(g):
            st_loc[h] = dot_tn(rec_i[:, lanes_of(h)], fresh[:, lanes_of(h)])

            @pl.when(jnp.logical_and(sp == 0, has_next))
            def _(h=h):
                st_out[h] = st_loc[h].astype(BF16)
                st_copy(h).start()

    def state_step(g):
        for h in heads_of(g):
            st_copy(h).wait_recv()

            @pl.when(has_next)
            def _(h=h):
                st_out[h] = (st_in[h].astype(F32) * dec[h, 0:1, :] + st_loc[h]).astype(BF16)
                st_copy(h).start()

    def state_step_if(at, g):
        if at < n_sp:
            pl.when(sp == at)(functools.partial(state_step, g))

    def read_local(g):
        cut = group(g)
        qdec[:, cut] = (finish(READ, g).astype(F32) * ecum[:, cut]).astype(BF16)
        for h in heads_of(g):
            lanes = lanes_of(h)
            scores = jnp.where(causal, dot_nt(qdec[:, lanes], kinv[:, lanes]), 0.0)
            loc[:, lanes] = dot_nn(scores.astype(BF16), rec_i[:, lanes])

    n_parts = 2 * GROUPS

    def h_copy(df, dt, kind, g):
        index = ((df * n_tp + dt) * 2 + kind) * GROUPS + g
        lands = (n_tp - dt) % n_tp
        lands_index = ((df * n_tp + lands) * 2 + kind) * GROUPS + g
        return pltpu.make_async_remote_copy(
            src_ref=heads.at[kind, pl.ds(pl.multiple_of(tp_at(dt) * share, share), share), pl.ds(g * g_cols, g_cols)],
            dst_ref=hrecv.at[df, lands, kind, :, pl.ds(g * g_cols, g_cols)],
            send_sem=h_send.at[index], recv_sem=h_recv.at[lands_index],
            device_id={"fs": fs_at(df), "tp": tp_at(dt)}, device_id_type=MESH,
        )

    h_order = [(df, dt) for df in list(range(1, n_fs)) + [0] for dt in range(n_tp) if df or dt]

    def h_wait(df, dt, kind, g):
        view = hrecv.at[df, dt, kind, :, pl.ds(g * g_cols, g_cols)]
        pltpu.make_async_remote_copy(
            src_ref=view, dst_ref=view, send_sem=h_send.at[0],
            recv_sem=h_recv.at[((df * n_tp + dt) * 2 + kind) * GROUPS + g],
            device_id={"tp": tp_at(1)}, device_id_type=MESH,
        ).wait_recv()

    def send_attn(g):
        heads[0, :, group(g)] = att[:, group(g)].astype(BF16)
        for df, dt in h_order:
            h_copy(df, dt, 0, g).start()

    def send_attn_if(condition, g):
        pl.when(condition)(functools.partial(send_attn, g))

    def send_rec(g):
        for h in heads_of(g):
            lanes = lanes_of(h)

            @pl.when(has_prev)
            def _(h=h, lanes=lanes):
                loc[:, lanes] += dot_nt(qdec[:, lanes], st_in[h])

            raw = loc[:, lanes]
            norm = lax.rsqrt(jnp.mean(raw * raw, axis=1, keepdims=True) + norm_eps)
            heads[1, :, lanes] = (raw * norm * out_gain[...]).astype(BF16)
        for df, dt in h_order:
            h_copy(df, dt, 1, g).start()

    def attend(slot, g, diagonal):
        z = jnp.concatenate(
            [
                dot_nt(qbuf[:, lanes_of(h)], kv[slot, 2 * g, :, lanes_of(i)]) * scale + offs[0:1, h:h + 1]
                for i, h in enumerate(heads_of(g))
            ],
            axis=0,
        )
        keep = -(jnp.maximum(z, 0.0) + jnp.log(1.0 + jnp.exp(-jnp.abs(z))))
        log_stick = z + keep
        if diagonal:
            keep = jnp.where(strict, keep, 0.0)
        both = dot_nn(jnp.concatenate(halves(keep), axis=1), sums)
        stick = jnp.exp(log_stick + both[:, :rows])
        if diagonal:
            stick = jnp.where(strict, stick, 0.0)
        stick = stick.astype(BF16)
        for i, h in enumerate(heads_of(g)):
            mine = slice(i * rows, (i + 1) * rows)
            value = dot_nn(stick[mine], kv[slot, 2 * g + 1, :, lanes_of(i)])
            if diagonal:
                att[:, lanes_of(h)] = value
                run[h] = both[mine, rows:]
            else:
                past = run[h]
                att[:, lanes_of(h)] += value * jnp.exp(past)
                run[h] = past + both[mine, rows:]

    def attend_if(step, g):
        if step < n_sp:
            pl.when(sp >= step)(functools.partial(attend, sp - step, g, False))

    def attend_rest(g):
        def block(step, carry):
            for c in group_kv(g):
                hand_on(step, c)
            attend(sp - step, g, False)
            return carry

        lax.fori_loop(3, sp + 1, block, 0)

    near = sp < 3
    far = sp >= 3
    for c in group_kv(0):
        hand_on_if(1, c)
    gates(0)
    local_state(0)
    for c in group_kv(0):
        hand_on_if(2, c)
    for g in range(1, GROUPS):
        for w in (KEY, VALUE):
            finish_kv(w, g)
    state_step_if(1, 0)
    for g in range(1, GROUPS):
        gates(g)
        hand_on_if(1, group_kv(g)[0])
        local_state(g)
        hand_on_if(1, group_kv(g)[1])
    state_step_if(2, 0)
    qbuf[:, group(0)] = finish(QUERY, 0)
    attend(sp, 0, True)
    attend_if(1, 0)
    attend_if(2, 0)
    attend_rest(0)
    send_attn(0)
    for g in range(1, GROUPS):
        hand_on_if(2, group_kv(g)[0])
        state_step_if(1, g)
        qbuf[:, group(g)] = finish(QUERY, g)
        attend(sp, g, True)
        hand_on_if(2, group_kv(g)[1])
    read_local(0)

    @pl.when(far)
    def _():
        state_step(0)

    send_rec(0)
    for g in range(1, GROUPS):
        attend_if(1, g)
        state_step_if(2, g)
        attend_if(2, g)

        @pl.when(near)
        def _(g=g):
            send_attn(g)

        read_local(g)

        @pl.when(near)
        def _(g=g):
            send_rec(g)

        @pl.when(far)
        def _(g=g):
            attend_rest(g)
            send_attn(g)
            state_step(g)
            send_rec(g)

    for dt in range(1, n_tp):
        other = tp_at(dt)
        pltpu.make_async_remote_copy(
            src_ref=obuf.at[other], dst_ref=obuf.at[other], send_sem=o_send.at[dt - 1], recv_sem=o_recv.at[other],
            device_id={"tp": other}, device_id_type=MESH,
        ).wait_recv()

    half = out_cols // CHUNKS

    def m_copy(df, k):
        index = (df - 1) * CHUNKS + k
        return pltpu.make_async_remote_copy(
            src_ref=mix.at[df - 1, k], dst_ref=mrecv.at[df - 1, k],
            send_sem=m_send.at[index], recv_sem=m_recv.at[index],
            device_id={"fs": fs_at(n_fs - df)}, device_id_type=MESH,
        )

    def columns(owner, k):
        return pl.ds(pl.multiple_of(owner * out_cols + k * half, LANES), half)

    def product(df, kind, g, cut):
        value = None
        for dt in range(n_tp):
            if df == 0 and dt == 0:
                left = heads[kind, pl.ds(pl.multiple_of(tp * share, share), share), group(g)]
            else:
                left = hrecv[df, dt, kind, :, group(g)]
            term = dot_nn(left, obuf[tp_at(dt), kind, group(g), cut])
            value = term if value is None else value + term
        return value

    whole = slice(0, out_cols)
    pieces = [(kind, g) for g in range(GROUPS) for kind in range(2)]
    for df in range(1, n_fs):
        for place, (kind, g) in enumerate(pieces[:-1]):
            for dt in range(n_tp):
                h_wait(df, dt, kind, g)
            if place == 0:
                part_acc[df - 1] = product(df, kind, g, whole)
            else:
                part_acc[df - 1] += product(df, kind, g, whole)
    for df in range(1, n_fs):
        kind, g = pieces[-1]
        for dt in range(n_tp):
            h_wait(df, dt, kind, g)
        for k in range(CHUNKS):
            cut = slice(k * half, (k + 1) * half)
            mix[df - 1, k] = (part_acc[df - 1, :, cut] + product(df, kind, g, cut)).astype(BF16)
            m_copy(df, k).start()
    for dt in range(1, n_tp):
        for kind in range(2):
            for g in range(GROUPS):
                h_wait(0, dt, kind, g)
    for k in range(CHUNKS):
        cut = slice(k * half, (k + 1) * half)
        value = None
        for kind in range(2):
            for g in range(GROUPS):
                term = product(0, kind, g, cut)
                value = term if value is None else value + term
        out[:, columns(fs, k)] = value.astype(BF16)

    for df in range(1, n_fs):
        @pl.when(holder(fs_at(df)) == tp)
        def _(df=df):
            for c in range(X_CHUNKS):
                x_copy(df, c).wait_send()

        @pl.when(is_relay)
        def _(df=df):
            for c in range(X_CHUNKS):
                for dt in range(1, n_tp):
                    f_copy(df, c, dt).wait_send()

        for c in range(X_CHUNKS):
            first_copy(df, c).wait_send()
        for u in range(n_units):
            p_copy(df, u).wait_send()
    for dt in range(1, n_tp):
        @pl.when(own_holder)
        def _(dt=dt):
            own_copy(dt).wait_send()

        ss_copy(dt).wait_send()
        o_copy(dt).wait_send()
    for df, dt in h_order:
        for kind in range(2):
            for g in range(GROUPS):
                h_copy(df, dt, kind, g).wait_send()

    @pl.when(has_next)
    def _():
        for h in range(n_heads):
            st_copy(h).wait_send()

        def drain(slot, carry):
            for c in range(n_kv):
                kv_copy(slot, c).wait_send()
            return carry

        lax.fori_loop(0, sp + 1, drain, 0)

    for df in range(1, n_fs):
        for k in range(CHUNKS):
            m_copy(df, k).wait_recv()
            out[:, columns(fs_at(df), k)] = mrecv[df - 1, k]
    for df in range(1, n_fs):
        for k in range(CHUNKS):
            m_copy(df, k).wait_send()


def body(
    tokens, mix_gain, attn_query, attn_key, attn_value, rec_query, rec_forget, rec_input,
    break_offset, forget_room, out_gain, out_attn, out_rec,
):
    n_sp, n_fs, n_tp = lax.axis_size("sp"), lax.axis_size("fs"), lax.axis_size("tp")
    rows, feat_t = tokens.shape[1], tokens.shape[2]
    feat_f, cols = attn_query.shape
    width = feat_t * n_tp
    n_heads = cols // LANES
    out_rows, out_cols = out_attn.shape
    share = rows // n_tp
    piece = out_cols // CHUNKS
    n_sends = len(unit_list(cols)) + X_CHUNKS
    n_kv = X_CHUNKS + 2 * (GROUPS - 1)
    hbm = pl.BlockSpec(memory_space=pl.ANY)
    vmem = pl.BlockSpec(memory_space=pltpu.VMEM)
    dma = pltpu.SemaphoreType.DMA
    square = (n_heads, LANES, LANES)
    others = n_fs - 1
    result = pl.pallas_call(
        functools.partial(kernel, n_sp, n_fs, n_tp),
        out_shape=pltpu.VMEM((share, width), BF16),
        in_specs=[hbm] * 13,
        out_specs=vmem,
        scratch_shapes=[
            pltpu.VMEM((1, width), F32),
            pltpu.VMEM((1, n_heads), F32),
            pltpu.VMEM((n_heads, LANES), F32),
            pltpu.VMEM((1, LANES), F32),
            pltpu.VMEM((rows, feat_t), BF16),
            pltpu.VMEM((N_PROJ, feat_f, cols), BF16),
            pltpu.VMEM((n_tp, 2, out_rows, out_cols), BF16),
            pltpu.VMEM((n_fs, rows, feat_f), BF16),
            pltpu.VMEM((n_fs, rows, feat_f), BF16),
            pltpu.VMEM((n_tp, rows, LANES), F32),
            pltpu.VMEM((N_PROJ, rows, cols), F32),
            pltpu.VMEM((others, N_PROJ, rows, cols), BF16),
            pltpu.VMEM((others, N_PROJ, rows, cols), BF16),
            pltpu.VMEM((n_sp, 2 * GROUPS, rows, cols // GROUPS), BF16),
            pltpu.VMEM((rows, cols), BF16),
            pltpu.VMEM((rows, cols), BF16),
            pltpu.VMEM((rows, cols), F32),
            pltpu.VMEM((rows, cols), BF16),
            pltpu.VMEM((rows, cols), BF16),
            pltpu.VMEM((rows, cols), BF16),
            pltpu.VMEM((rows, cols), F32),
            pltpu.VMEM((n_heads, rows, LANES), F32),
            pltpu.VMEM((rows, cols), F32),
            pltpu.VMEM(square, F32),
            pltpu.VMEM((n_heads, 8, LANES), F32),
            pltpu.VMEM(square, BF16),
            pltpu.VMEM(square, BF16),
            pltpu.VMEM((2, rows, cols), BF16),
            pltpu.VMEM((n_fs, n_tp, 2, share, cols), BF16),
            pltpu.VMEM((others, share, out_cols), F32),
            pltpu.VMEM((others, CHUNKS, share, piece), BF16),
            pltpu.VMEM((others, CHUNKS, share, piece), BF16),
            dma((1,)), dma((N_SMALL,)), dma((N_PROJ + 2,)),
            dma((others * X_CHUNKS,)), dma((n_fs * X_CHUNKS,)), dma((others * X_CHUNKS * (n_tp - 1),)),
            dma((n_tp - 1,)), dma((1,)), dma((n_tp - 1,)), dma((n_tp,)),
            dma((others * n_sends,)), dma((others * n_sends,)),
            dma((n_sp * n_kv,)), dma((n_sp * n_kv,)),
            dma((n_heads,)), dma((n_heads,)),
            dma((n_tp - 1,)), dma((n_tp,)),
            dma((n_fs * n_tp * 2 * GROUPS,)), dma((n_fs * n_tp * 2 * GROUPS,)),
            dma((others * CHUNKS,)), dma((others * CHUNKS,)),
        ],
        compiler_params=pltpu.CompilerParams(
            collective_id=0, has_side_effects=True, vmem_limit_bytes=60 * 1024 * 1024
        ),
        name="layer",
    )(
        tokens.reshape(rows, feat_t), mix_gain.reshape(1, width),
        attn_key, attn_value, rec_forget, rec_input, attn_query, rec_query,
        break_offset.reshape(1, n_heads), forget_room, out_gain.reshape(1, LANES), out_attn, out_rec,
    )
    return result.reshape(1, share, width)


def solution(mesh):
    placed = (
        P(("grp", "fs"), "sp", "tp"),
        P(),
        P("fs", "tp"),
        P("fs", "tp"),
        P("fs", "tp"),
        P("fs", "tp"),
        P("fs", "tp"),
        P("fs", "tp"),
        P("tp"),
        P("tp", None),
        P(),
        P("tp", "fs"),
        P("tp", "fs"),
    )
    return jax.shard_map(
        body,
        mesh=mesh,
        in_specs=placed,
        out_specs=P(("grp", "fs"), ("sp", "tp"), None),
        check_vma=False,
    )
```

```python
import functools
import math

import jax
import jax.numpy as jnp
from jax import lax
from jax.experimental import pallas as pl
from jax.experimental.pallas import tpu as pltpu
from jax.sharding import PartitionSpec as P

LANES = 128
norm_eps = 1e-06
MESH = pl.DeviceIdType.MESH
F32 = jnp.float32
BF16 = jnp.bfloat16
N_PROJ = 6
KEY, VALUE, FORGET, INPUT, QUERY, READ = range(N_PROJ)
GROUPS = 2
CHUNKS = 4
X_CHUNKS = 4
N_SMALL = 4


def dot_nn(a, b):
    return lax.dot_general(a, b, (((1,), (0,)), ((), ())), preferred_element_type=F32)


def dot_nt(a, b):
    return lax.dot_general(a, b, (((1,), (1,)), ((), ())), preferred_element_type=F32)


def dot_tn(a, b):
    return lax.dot_general(a, b, (((0,), (0,)), ((), ())), preferred_element_type=F32)


def halves(x):
    high = x.astype(BF16)
    return high, (x - high.astype(F32)).astype(BF16)


def unit_list(cols):
    g_cols = cols // GROUPS
    last = (GROUPS - 1) * g_cols
    units = [(FORGET, 0), (INPUT, 0), (QUERY, last)]
    for g in range(1, GROUPS):
        units += [(w, g * g_cols) for w in (KEY, VALUE, FORGET, INPUT)]
    units += [(QUERY, g * g_cols) for g in range(GROUPS - 1)]
    units += [(READ, g * g_cols) for g in range(GROUPS)]
    return units


def kernel(
    n_sp, n_fs, n_tp,
    tok_hbm, gain_hbm, w_k, w_v, w_f, w_i, w_q, w_r, offs_hbm, room_hbm, out_gain_hbm, o_attn, o_rec,
    out,
    gain, offs, room, out_gain,
    tok, wbuf, obuf, xt, xg, ss, acc, psend, precv, kv, qbuf, qdec, ecum, kinv, fresh, rec_i,
    att, run, q_back, v_back, v_far, loc, st_loc, dec, st_in, st_out, heads, hrecv, part_acc, mix, mrecv,
    t_sem, s_sem, w_sem, x_send, x_recv, f_send, own_send, own_recv, ss_send, ss_recv, p_send, p_recv,
    kv_send, kv_recv, st_send, st_recv, o_send, o_recv, b_sem, h_send, h_recv, m_send, m_recv,
):
    sp, fs, tp = lax.axis_index("sp"), lax.axis_index("fs"), lax.axis_index("tp")
    rows, feat_t = tok.shape
    feat_f = xt.shape[2]
    width = feat_t * n_tp
    cols = wbuf.shape[2]
    n_heads = cols // LANES
    share = rows // n_tp
    out_cols = obuf.shape[3]
    g_cols = cols // GROUPS
    g_heads = n_heads // GROUPS
    n_kv = X_CHUNKS + 2 * (GROUPS - 1)
    x_rows = rows // X_CHUNKS
    relay = 0
    is_relay = tp == relay
    has_next = sp < n_sp - 1
    has_prev = sp > 0
    back = n_sp > 3
    at_end = sp == n_sp - 1
    last = GROUPS - 1
    near = sp < 3
    far = sp >= 3

    def fs_at(step):
        return lax.rem(fs + step, n_fs)

    def tp_at(step):
        return lax.rem(tp + step, n_tp)

    def group(g):
        return slice(g * g_cols, (g + 1) * g_cols)

    tok_copy = pltpu.make_async_copy(tok_hbm, tok, t_sem.at[0])
    tok_copy.start()
    barrier = pltpu.get_barrier_semaphore()
    for df in range(n_fs):
        for dt in range(n_tp):
            if df or dt:
                pl.semaphore_signal(
                    barrier, inc=1, device_id={"fs": fs_at(df), "tp": tp_at(dt)}, device_id_type=MESH
                )

    @pl.when(has_next)
    def _():
        pl.semaphore_signal(barrier, inc=1, device_id={"sp": sp + 1}, device_id_type=MESH)

    @pl.when(has_prev)
    def _():
        pl.semaphore_signal(barrier, inc=1, device_id={"sp": sp - 1}, device_id_type=MESH)

    small_copies = [
        pltpu.make_async_copy(source, target, s_sem.at[i])
        for i, (source, target) in enumerate(
            ((gain_hbm, gain), (offs_hbm, offs), (room_hbm, room), (out_gain_hbm, out_gain))
        )
    ]
    w_copies = [
        pltpu.make_async_copy(w, wbuf.at[i], w_sem.at[i // 2])
        for i, w in enumerate((w_k, w_v, w_f, w_i, w_q, w_r))
    ]
    o_copies = [
        pltpu.make_async_copy(w, obuf.at[tp, i], w_sem.at[N_PROJ // 2]) for i, w in enumerate((o_attn, o_rec))
    ]

    def w_wait(w):
        pair = wbuf.at[pl.ds(w, 2)]
        pltpu.make_async_copy(pair, pair, w_sem.at[w // 2]).wait()

    def land(view, sem, wait_send=False):
        copy = pltpu.make_async_remote_copy(
            src_ref=view, dst_ref=view, send_sem=sem, recv_sem=sem,
            device_id={"tp": tp_at(1)}, device_id_type=MESH,
        )
        if wait_send:
            copy.wait_send()
        else:
            copy.wait_recv()

    for copy in small_copies + w_copies + o_copies:
        copy.start()
    tok_copy.wait()

    next_count = jnp.where(has_next, 1, 0)
    prev_count = jnp.where(has_prev, 1, 0)
    pl.semaphore_wait(barrier, n_fs * n_tp - 1 + next_count + prev_count)

    def holder(f_index):
        return (f_index * feat_f) // feat_t

    def held(f_index):
        return pl.ds(pl.multiple_of(lax.rem(f_index * feat_f, feat_t), LANES), feat_f)

    def x_part(c):
        return pl.ds(c * x_rows, x_rows)

    def x_copy(df, c):
        return pltpu.make_async_remote_copy(
            src_ref=tok.at[x_part(c), held(fs_at(df))], dst_ref=xt.at[fs, x_part(c)],
            send_sem=x_send.at[df - 1], recv_sem=x_recv.at[(n_fs - df - 1) * X_CHUNKS + c],
            device_id={"fs": fs_at(df), "tp": relay}, device_id_type=MESH,
        )

    def f_copy(df, c, dt):
        slot = fs_at(df)
        return pltpu.make_async_remote_copy(
            src_ref=xt.at[slot, x_part(c)], dst_ref=xt.at[slot, x_part(c)],
            send_sem=f_send.at[(df - 1) * (n_tp - 1) + dt - 1],
            recv_sem=x_recv.at[(df - 1) * X_CHUNKS + c],
            device_id={"tp": tp_at(dt)}, device_id_type=MESH,
        )

    def own_copy(dt):
        return pltpu.make_async_remote_copy(
            src_ref=tok.at[:, held(fs)], dst_ref=xt.at[fs],
            send_sem=own_send.at[dt - 1], recv_sem=own_recv.at[0],
            device_id={"tp": tp_at(dt)}, device_id_type=MESH,
        )

    for df in range(1, n_fs):
        @pl.when(holder(fs_at(df)) == tp)
        def _(df=df):
            for c in range(X_CHUNKS):
                x_copy(df, c).start()

    own_holder = holder(fs) == tp

    @pl.when(own_holder)
    def _():
        for dt in range(1, n_tp):
            own_copy(dt).start()

    squares = jnp.zeros((rows, LANES), F32)
    for c in range(feat_t // LANES):
        piece = tok[:, c * LANES:(c + 1) * LANES].astype(F32)
        squares = squares + piece * piece
    ss[tp] = squares

    def ss_copy(dt):
        return pltpu.make_async_remote_copy(
            src_ref=ss.at[tp], dst_ref=ss.at[tp],
            send_sem=ss_send.at[dt - 1], recv_sem=ss_recv.at[n_tp - dt - 1],
            device_id={"tp": tp_at(dt)}, device_id_type=MESH,
        )

    for dt in range(1, n_tp):
        ss_copy(dt).start()

    for copy in small_copies:
        copy.wait()
    gain_f = gain[:, pl.ds(pl.multiple_of(fs * feat_f, LANES), feat_f)]

    @pl.when(own_holder)
    def _():
        xg[0] = (tok[:, held(fs)].astype(F32) * gain_f).astype(BF16)

    units = unit_list(cols)
    n_units = len(units)

    def first_copy(df, c):
        index = (df - 1) * (n_units + X_CHUNKS) + n_units + c
        return pltpu.make_async_remote_copy(
            src_ref=psend.at[df - 1, pl.ds(KEY, 2), x_part(c), pl.ds(0, g_cols)],
            dst_ref=precv.at[df - 1, pl.ds(KEY, 2), x_part(c), pl.ds(0, g_cols)],
            send_sem=p_send.at[df - 1], recv_sem=p_recv.at[index],
            device_id={"fs": fs_at(df)}, device_id_type=MESH,
        )

    def p_copy(df, u):
        w, first = units[u]
        index = (df - 1) * (n_units + X_CHUNKS) + u
        return pltpu.make_async_remote_copy(
            src_ref=psend.at[df - 1, w, :, pl.ds(first, g_cols)],
            dst_ref=precv.at[df - 1, w, :, pl.ds(first, g_cols)],
            send_sem=p_send.at[df - 1], recv_sem=p_recv.at[index],
            device_id={"fs": fs_at(df)}, device_id_type=MESH,
        )

    @pl.when(jnp.logical_not(own_holder))
    def _():
        land(xt.at[fs], own_recv.at[0])
        xg[0] = (xt[fs].astype(F32) * gain_f).astype(BF16)

    total = ss[tp]
    for dt in range(1, n_tp):
        other = tp_at(dt)
        land(ss.at[other], ss_recv.at[dt - 1])
        total = total + ss[other]
    factor = lax.rsqrt(jnp.sum(total, axis=1, keepdims=True) / width + norm_eps)

    def own_product(w, cut):
        acc[w, :, cut] = dot_nn(xg[0], wbuf[w, :, cut])

    w_wait(KEY)
    own_product(KEY, group(0))
    own_product(VALUE, group(0))
    for c in range(X_CHUNKS):
        part = slice(c * x_rows, (c + 1) * x_rows)
        for df in range(1, n_fs):
            slot = fs_at(df)
            land(xt.at[slot, x_part(c)], x_recv.at[(df - 1) * X_CHUNKS + c])

            @pl.when(is_relay)
            def _(df=df, c=c):
                for dt in range(1, n_tp):
                    f_copy(df, c, dt).start()

            xg[df, part, :] = (xt[slot, part, :].astype(F32) * gain_f).astype(BF16)
            for w in (KEY, VALUE):
                psend[df - 1, w, part, 0:g_cols] = dot_nn(xg[df, part, :], wbuf[w, :, 0:g_cols]).astype(BF16)
            first_copy(df, c).start()

    def partials(w, first, count):
        cut = slice(first, first + count)
        for df in range(1, n_fs):
            psend[df - 1, w, :, cut] = dot_nn(xg[df], wbuf[w, :, cut]).astype(BF16)

    def send_unit(w, g):
        for df in range(1, n_fs):
            p_copy(df, units.index((w, g * g_cols))).start()


    def finish(w, g):
        cut = group(g)
        value = acc[w, :, cut]
        for df in range(1, n_fs):
            p_copy(df, units.index((w, g * g_cols))).wait_recv()
            value = value + precv[df - 1, w, :, cut].astype(F32)
        return (value * factor).astype(BF16)

    def kv_copy(slot, c):
        if c < X_CHUNKS:
            view = kv.at[slot, pl.ds(0, 2), x_part(c)]
        else:
            view = kv.at[slot, 2 + c - X_CHUNKS]
        return pltpu.make_async_remote_copy(
            src_ref=view, dst_ref=view,
            send_sem=kv_send.at[slot], recv_sem=kv_recv.at[slot * n_kv + c],
            device_id={"sp": lax.rem(sp + 1, n_sp)}, device_id_type=MESH,
        )

    def group_kv(g):
        if g == 0:
            return range(X_CHUNKS)
        return range(X_CHUNKS + 2 * (g - 1), X_CHUNKS + 2 * g)

    def send_kv(c):
        @pl.when(has_next)
        def _():
            kv_copy(sp, c).start()

    def finish_first(c):
        part = slice(c * x_rows, (c + 1) * x_rows)
        for df in range(1, n_fs):
            first_copy(df, c).wait_recv()
        for w in (KEY, VALUE):
            value = acc[w, part, 0:g_cols]
            for df in range(1, n_fs):
                value = value + precv[df - 1, w, part, 0:g_cols].astype(F32)
            kv[sp, w, part, :] = (value * factor[part]).astype(BF16)
        send_kv(c)

    def finish_kv(w, g):
        kv[sp, 2 * g + w] = finish(w, g)
        send_kv(X_CHUNKS + 2 * (g - 1) + w)

    def hand_on(step, c):
        kv_copy(sp - step, c).wait_recv()
        goes_on = has_next
        if back and c in group_kv(last):
            goes_on = jnp.logical_and(has_next, jnp.logical_or(step < sp, sp < n_sp - 2))

        @pl.when(goes_on)
        def _():
            kv_copy(sp - step, c).start()

    def hand_on_if(step, c):
        if step < n_sp:
            pl.when(sp >= step)(functools.partial(hand_on, step, c))

    w_wait(FORGET)
    quarter = X_CHUNKS // 4
    for w in (FORGET, INPUT):
        partials(w, 0, cols)
        send_unit(w, 0)
        for c in range(quarter):
            finish_first((w - FORGET) * quarter + c)
    w_wait(QUERY)
    partials(QUERY, 0, cols)
    send_unit(QUERY, last)
    for w in (KEY, VALUE):
        partials(w, g_cols, cols - g_cols)
        for g in range(1, GROUPS):
            send_unit(w, g)
        for c in range(quarter):
            finish_first((2 + w) * quarter + c)
    for w in (FORGET, INPUT):
        for g in range(1, GROUPS):
            send_unit(w, g)
    for g in range(last):
        send_unit(QUERY, g)
    partials(READ, 0, cols)
    for g in range(GROUPS):
        send_unit(READ, g)
    for w in (FORGET, INPUT):
        own_product(w, slice(0, cols))
    for w in (KEY, VALUE):
        own_product(w, slice(g_cols, cols))
    for w in (QUERY, READ):
        own_product(w, slice(0, cols))

    def o_copy(dt):
        return pltpu.make_async_remote_copy(
            src_ref=obuf.at[tp], dst_ref=obuf.at[tp], send_sem=o_send.at[dt - 1], recv_sem=o_recv.at[n_tp - dt - 1],
            device_id={"tp": tp_at(dt)}, device_id_type=MESH,
        )

    pltpu.make_async_copy(obuf.at[tp], obuf.at[tp], w_sem.at[N_PROJ // 2]).wait()
    for dt in range(1, n_tp):
        o_copy(dt).start()

    iota_r = lax.broadcasted_iota(jnp.int32, (rows, rows), 0)
    iota_c = lax.broadcasted_iota(jnp.int32, (rows, rows), 1)
    causal = iota_r >= iota_c
    strict = jnp.concatenate([iota_c < iota_r] * g_heads, axis=0)
    lower = jnp.where(causal, 1.0, 0.0).astype(BF16)
    lower = jnp.concatenate([lower, lower], axis=1)
    later = jnp.where(iota_r > iota_c, 1.0, 0.0).astype(BF16)
    sums = jnp.concatenate([later, jnp.ones((rows, LANES), BF16)], axis=1)
    sums = jnp.concatenate([sums, sums], axis=0)
    scale = 1.0 / math.sqrt(LANES)

    def lanes_of(h):
        return slice(h * LANES, (h + 1) * LANES)

    def heads_of(g):
        return range(g * g_heads, (g + 1) * g_heads)

    def gates(g):
        cut = group(g)
        rooms = jnp.concatenate([room[h:h + 1, :] for h in heads_of(g)], axis=1)
        key_in = rooms * jax.nn.sigmoid(-finish(FORGET, g).astype(F32))
        high, low = halves(jnp.log1p(-key_in))
        cum = dot_nn(lower, jnp.concatenate([high, low], axis=0))
        last = cum[rows - 1:rows, :]
        ecum[:, cut] = jnp.exp(cum)
        kinv[:, cut] = (key_in * jnp.exp(-cum)).astype(BF16)
        fresh[:, cut] = (key_in * jnp.exp(last - cum)).astype(BF16)
        decay = jnp.exp(last)
        for i, h in enumerate(heads_of(g)):
            dec[h] = jnp.broadcast_to(decay[:, lanes_of(i)], dec.shape[1:])

    def st_copy(h):
        return pltpu.make_async_remote_copy(
            src_ref=st_out.at[h], dst_ref=st_in.at[h], send_sem=st_send.at[0], recv_sem=st_recv.at[h],
            device_id={"sp": lax.rem(sp + 1, n_sp)}, device_id_type=MESH,
        )

    def local_state(g):
        rec_i[:, group(g)] = finish(INPUT, g)
        for h in heads_of(g):
            st_loc[h] = dot_tn(rec_i[:, lanes_of(h)], fresh[:, lanes_of(h)])

            @pl.when(jnp.logical_and(sp == 0, has_next))
            def _(h=h):
                st_out[h] = st_loc[h].astype(BF16)
                st_copy(h).start()

    def state_step(h):
        st_copy(h).wait_recv()

        @pl.when(has_next)
        def _():
            st_out[h] = (st_in[h].astype(F32) * dec[h, 0:1, :] + st_loc[h]).astype(BF16)
            st_copy(h).start()

    def state_steps(g):
        for h in heads_of(g):
            state_step(h)

    def state_step_if(at, g):
        if at < n_sp:
            pl.when(sp == at)(functools.partial(state_steps, g))

    def read_local(g):
        cut = group(g)
        qdec[:, cut] = (finish(READ, g).astype(F32) * ecum[:, cut]).astype(BF16)
        for h in heads_of(g):
            lanes = lanes_of(h)
            scores = jnp.where(causal, dot_nt(qdec[:, lanes], kinv[:, lanes]), 0.0)
            loc[:, lanes] = dot_nn(scores.astype(BF16), rec_i[:, lanes])

    n_land = 2 + g_heads
    early = pl.ds(0, last * g_cols)

    def h_sem(df, dt, mark):
        return h_recv.at[dt if df == 0 else n_tp + ((df - 1) * n_tp + dt) * n_land + mark]

    def h_copy(df, dt, kind, first, count, mark):
        lands = (n_tp - dt) % n_tp
        lanes = pl.ds(first, count)
        return pltpu.make_async_remote_copy(
            src_ref=heads.at[kind, pl.ds(pl.multiple_of(tp_at(dt) * share, share), share), lanes],
            dst_ref=hrecv.at[df, lands, kind, :, lanes],
            send_sem=h_send.at[df * n_tp + dt], recv_sem=h_sem(df, lands, mark),
            device_id={"fs": fs_at(df), "tp": tp_at(dt)}, device_id_type=MESH,
        )

    h_order = [(df, dt) for df in list(range(1, n_fs)) + [0] for dt in range(n_tp) if df or dt]

    def send_heads(kind, first, count, mark):
        for df, dt in h_order:
            h_copy(df, dt, kind, first, count, mark).start()

    def send_attn(g):
        heads[0, :, group(g)] = att[:, group(g)].astype(BF16)
        send_heads(0, g * g_cols, g_cols, 1 if g == last else 0)

    def finish_rec(h):
        lanes = lanes_of(h)

        @pl.when(has_prev)
        def _():
            loc[:, lanes] += dot_nt(qdec[:, lanes], st_in[h])

        raw = loc[:, lanes]
        norm = lax.rsqrt(jnp.mean(raw * raw, axis=1, keepdims=True) + norm_eps)
        heads[1, :, lanes] = (raw * norm * out_gain[...]).astype(BF16)

    def send_rec(g):
        for i, h in enumerate(heads_of(g)):
            if g == last:
                pl.when(far)(functools.partial(state_step, h))
            finish_rec(h)
            if g == last:
                send_heads(1, h * LANES, LANES, 2 + i)
        if g < last:
            send_heads(1, g * g_cols, g_cols, 0)

    def sticks(queries, slot, g, diagonal):
        z = jnp.concatenate(
            [
                dot_nt(queries[:, lanes_of(i)], kv[slot, 2 * g, :, lanes_of(i)]) * scale + offs[0:1, h:h + 1]
                for i, h in enumerate(heads_of(g))
            ],
            axis=0,
        )
        keep = -(jnp.maximum(z, 0.0) + jnp.log(1.0 + jnp.exp(-jnp.abs(z))))
        log_stick = z + keep
        if diagonal:
            keep = jnp.where(strict, keep, 0.0)
        both = dot_nn(jnp.concatenate(halves(keep), axis=1), sums)
        stick = jnp.exp(log_stick + both[:, :rows])
        if diagonal:
            stick = jnp.where(strict, stick, 0.0)
        return stick.astype(BF16), both

    def attend(slot, g, diagonal):
        stick, both = sticks(qbuf.at[:, group(g)], slot, g, diagonal)
        for i, h in enumerate(heads_of(g)):
            mine = slice(i * rows, (i + 1) * rows)
            value = dot_nn(stick[mine], kv[slot, 2 * g + 1, :, lanes_of(i)])
            if diagonal:
                att[:, lanes_of(h)] = value
                run[h] = both[mine, rows:]
            else:
                past = run[h]
                att[:, lanes_of(h)] += value * jnp.exp(past)
                run[h] = past + both[mine, rows:]

    def attend_if(step, g):
        if step < n_sp:
            pl.when(sp >= step)(functools.partial(attend, sp - step, g, False))

    def attend_rest(g):
        def block(step, carry):
            for c in group_kv(g):
                hand_on(step, c)
            attend(sp - step, g, False)
            return carry

        end = sp + 1
        if back and g == last:
            end = jnp.where(at_end, sp, sp + 1)
        lax.fori_loop(3, end, block, 0)

    def q_copy():
        return pltpu.make_async_remote_copy(
            src_ref=qbuf.at[:, pl.ds(last * g_cols, g_cols)], dst_ref=q_back,
            send_sem=b_sem.at[0], recv_sem=b_sem.at[0], device_id={"sp": 0}, device_id_type=MESH,
        )

    def v_copy():
        return pltpu.make_async_remote_copy(
            src_ref=v_back, dst_ref=v_far,
            send_sem=b_sem.at[1], recv_sem=b_sem.at[1], device_id={"sp": n_sp - 1}, device_id_type=MESH,
        )

    def ask_back():
        q_copy().start()

    def answer():
        q_copy().wait_recv()
        stick, _ = sticks(q_back, 0, last, False)
        for i in range(g_heads):
            value = dot_nn(stick[i * rows:(i + 1) * rows], kv[0, 2 * last + 1, :, lanes_of(i)])
            v_back[:, lanes_of(i)] = value.astype(BF16)
        v_copy().start()

    def take_answer():
        v_copy().wait_recv()
        for i, h in enumerate(heads_of(last)):
            att[:, lanes_of(h)] += v_far[:, lanes_of(i)].astype(F32) * jnp.exp(run[h])

    for c in group_kv(0):
        hand_on_if(1, c)
    gates(0)
    local_state(0)
    qbuf[:, group(last)] = finish(QUERY, last)
    for c in group_kv(0):
        hand_on_if(2, c)
        if back and c == 0:
            pl.when(at_end)(ask_back)
    for g in range(1, GROUPS):
        for w in (KEY, VALUE):
            finish_kv(w, g)
    state_step_if(1, 0)
    for g in range(1, GROUPS):
        gates(g)
        hand_on_if(1, group_kv(g)[0])
        local_state(g)
        hand_on_if(1, group_kv(g)[1])
    state_step_if(2, 0)
    for g in range(last):
        qbuf[:, group(g)] = finish(QUERY, g)
        attend(sp, g, True)
        attend_if(1, g)
        attend_if(2, g)
        attend_rest(g)
        send_attn(g)
    for g in range(1, GROUPS):
        state_step_if(1, g)
        attend(sp, g, True)
        attend_if(1, g)

        @pl.when(sp < 2)
        def _(g=g):
            send_attn(g)

    if back:
        pl.when(sp == 0)(answer)
    read_local(0)

    @pl.when(near)
    def _():
        send_rec(0)

    for g in range(1, GROUPS):
        hand_on_if(2, group_kv(g)[0])
        read_local(g)
        state_step_if(2, g)
        hand_on_if(2, group_kv(g)[1])
        attend_if(2, g)

        @pl.when(far)
        def _(g=g):
            attend_rest(g)
            if back and g == last:
                pl.when(at_end)(take_answer)

        @pl.when(sp >= 2)
        def _(g=g):
            send_attn(g)

        @pl.when(far)
        def _(g=g):
            state_steps(g - 1)
            send_rec(g - 1)

        send_rec(g)

    for dt in range(1, n_tp):
        other = tp_at(dt)
        land(obuf.at[other], o_recv.at[dt - 1])

    half = out_cols // CHUNKS

    def m_copy(df, k):
        index = (df - 1) * CHUNKS + k
        return pltpu.make_async_remote_copy(
            src_ref=mix.at[df - 1, k], dst_ref=mrecv.at[df - 1, k],
            send_sem=m_send.at[df - 1], recv_sem=m_recv.at[index],
            device_id={"fs": fs_at(n_fs - df)}, device_id_type=MESH,
        )

    def columns(owner, k):
        return pl.ds(pl.multiple_of(owner * out_cols + k * half, LANES), half)

    def product(df, kind, lanes, cut):
        value = None
        for dt in range(n_tp):
            if df == 0 and dt == 0:
                left = heads[kind, pl.ds(pl.multiple_of(tp * share, share), share), lanes]
            else:
                left = hrecv[df, dt, kind, :, lanes]
            term = dot_nn(left, obuf[tp_at(dt), kind, lanes, cut])
            value = term if value is None else value + term
        return value

    whole = slice(0, out_cols)
    final = lanes_of(n_heads - 1)
    for df in range(1, n_fs):
        for dt in range(n_tp):
            land(hrecv.at[df, dt, :, :, early], h_sem(df, dt, 0))
        for kind in range(2):
            for g in range(last):
                if kind == 0 and g == 0:
                    part_acc[df - 1] = product(df, kind, group(g), whole)
                else:
                    part_acc[df - 1] += product(df, kind, group(g), whole)
        marks = [(0, group(last))] + [(1, lanes_of(h)) for h in heads_of(last)]
        for mark, (kind, lanes) in enumerate(marks):
            for dt in range(n_tp):
                land(hrecv.at[df, dt, kind, :, lanes], h_sem(df, dt, 1 + mark))
            if mark < len(marks) - 1:
                part_acc[df - 1] += product(df, kind, lanes, whole)
        for k in range(CHUNKS):
            cut = slice(k * half, (k + 1) * half)
            mix[df - 1, k] = (part_acc[df - 1, :, cut] + product(df, 1, final, cut)).astype(BF16)
            m_copy(df, k).start()
    for dt in range(1, n_tp):
        land(hrecv.at[0, dt], h_sem(0, dt, 0))
    for k in range(CHUNKS):
        cut = slice(k * half, (k + 1) * half)
        value = product(0, 0, slice(0, cols), cut) + product(0, 1, slice(0, cols), cut)
        out[:, columns(fs, k)] = value.astype(BF16)

    for df in range(1, n_fs):
        @pl.when(holder(fs_at(df)) == tp)
        def _(df=df):
            land(xt.at[0], x_send.at[df - 1], True)

        @pl.when(is_relay)
        def _(df=df):
            for dt in range(1, n_tp):
                land(xt.at[0], f_send.at[(df - 1) * (n_tp - 1) + dt - 1], True)

        land(psend.at[df - 1], p_send.at[df - 1], True)
    for dt in range(1, n_tp):
        @pl.when(own_holder)
        def _(dt=dt):
            own_copy(dt).wait_send()

        ss_copy(dt).wait_send()
        o_copy(dt).wait_send()
    for df, dt in h_order:
        land(hrecv.at[df, dt], h_send.at[df * n_tp + dt], True)

    @pl.when(has_next)
    def _():
        land(st_out, st_send.at[0], True)

        def drain(slot, carry):
            land(kv.at[slot], kv_send.at[slot], True)
            return carry

        if back:
            shorter = sp == n_sp - 2

            @pl.when(shorter)
            def _():
                land(kv.at[0, pl.ds(0, 2 * last)], kv_send.at[0], True)

            lax.fori_loop(jnp.where(shorter, 1, 0), sp + 1, drain, 0)
        else:
            lax.fori_loop(0, sp + 1, drain, 0)

    if back:
        @pl.when(at_end)
        def _():
            q_copy().wait_send()

        @pl.when(sp == 0)
        def _():
            v_copy().wait_send()

    for df in range(1, n_fs):
        for k in range(CHUNKS):
            m_copy(df, k).wait_recv()
            out[:, columns(fs_at(df), k)] = mrecv[df - 1, k]
    for df in range(1, n_fs):
        land(mix.at[df - 1], m_send.at[df - 1], True)


def body(
    tokens, mix_gain, attn_query, attn_key, attn_value, rec_query, rec_forget, rec_input,
    break_offset, forget_room, out_gain, out_attn, out_rec,
):
    n_sp, n_fs, n_tp = lax.axis_size("sp"), lax.axis_size("fs"), lax.axis_size("tp")
    rows, feat_t = tokens.shape[1], tokens.shape[2]
    feat_f, cols = attn_query.shape
    width = feat_t * n_tp
    n_heads = cols // LANES
    out_rows, out_cols = out_attn.shape
    share = rows // n_tp
    piece = out_cols // CHUNKS
    n_sends = len(unit_list(cols)) + X_CHUNKS
    n_kv = X_CHUNKS + 2 * (GROUPS - 1)
    hbm = pl.BlockSpec(memory_space=pl.ANY)
    vmem = pl.BlockSpec(memory_space=pltpu.VMEM)
    dma = pltpu.SemaphoreType.DMA
    square = (n_heads, LANES, LANES)
    others = n_fs - 1
    result = pl.pallas_call(
        functools.partial(kernel, n_sp, n_fs, n_tp),
        out_shape=pltpu.VMEM((share, width), BF16),
        in_specs=[hbm] * 13,
        out_specs=vmem,
        scratch_shapes=[
            pltpu.VMEM((1, width), F32),
            pltpu.VMEM((1, n_heads), F32),
            pltpu.VMEM((n_heads, LANES), F32),
            pltpu.VMEM((1, LANES), F32),
            pltpu.VMEM((rows, feat_t), BF16),
            pltpu.VMEM((N_PROJ, feat_f, cols), BF16),
            pltpu.VMEM((n_tp, 2, out_rows, out_cols), BF16),
            pltpu.VMEM((n_fs, rows, feat_f), BF16),
            pltpu.VMEM((n_fs, rows, feat_f), BF16),
            pltpu.VMEM((n_tp, rows, LANES), F32),
            pltpu.VMEM((N_PROJ, rows, cols), F32),
            pltpu.VMEM((others, N_PROJ, rows, cols), BF16),
            pltpu.VMEM((others, N_PROJ, rows, cols), BF16),
            pltpu.VMEM((n_sp, 2 * GROUPS, rows, cols // GROUPS), BF16),
            pltpu.VMEM((rows, cols), BF16),
            pltpu.VMEM((rows, cols), BF16),
            pltpu.VMEM((rows, cols), F32),
            pltpu.VMEM((rows, cols), BF16),
            pltpu.VMEM((rows, cols), BF16),
            pltpu.VMEM((rows, cols), BF16),
            pltpu.VMEM((rows, cols), F32),
            pltpu.VMEM((n_heads, rows, LANES), F32),
            pltpu.VMEM((rows, cols // GROUPS), BF16),
            pltpu.VMEM((rows, cols // GROUPS), BF16),
            pltpu.VMEM((rows, cols // GROUPS), BF16),
            pltpu.VMEM((rows, cols), F32),
            pltpu.VMEM(square, F32),
            pltpu.VMEM((n_heads, 8, LANES), F32),
            pltpu.VMEM(square, BF16),
            pltpu.VMEM(square, BF16),
            pltpu.VMEM((2, rows, cols), BF16),
            pltpu.VMEM((n_fs, n_tp, 2, share, cols), BF16),
            pltpu.VMEM((others, share, out_cols), F32),
            pltpu.VMEM((others, CHUNKS, share, piece), BF16),
            pltpu.VMEM((others, CHUNKS, share, piece), BF16),
            dma((1,)), dma((N_SMALL,)), dma((N_PROJ // 2 + 1,)),
            dma((others,)), dma((others * X_CHUNKS,)), dma((others * (n_tp - 1),)),
            dma((n_tp - 1,)), dma((1,)), dma((n_tp - 1,)), dma((n_tp - 1,)),
            dma((others,)), dma((others * n_sends,)),
            dma((n_sp,)), dma(((n_sp - 1) * n_kv,)),
            dma((1,)), dma((n_heads,)),
            dma((n_tp - 1,)), dma((n_tp - 1,)), dma((2,)),
            dma((n_fs * n_tp,)), dma((n_tp + others * n_tp * (2 + n_heads // GROUPS),)),
            dma((others,)), dma((others * CHUNKS,)),
        ],
        compiler_params=pltpu.CompilerParams(
            collective_id=0, has_side_effects=True, vmem_limit_bytes=60 * 1024 * 1024
        ),
        name="layer",
    )(
        tokens.reshape(rows, feat_t), mix_gain.reshape(1, width),
        attn_key, attn_value, rec_forget, rec_input, attn_query, rec_query,
        break_offset.reshape(1, n_heads), forget_room, out_gain.reshape(1, LANES), out_attn, out_rec,
    )
    return result.reshape(1, share, width)


def solution(mesh):
    placed = (
        P(("grp", "fs"), "sp", "tp"),
        P(),
        P("fs", "tp"),
        P("fs", "tp"),
        P("fs", "tp"),
        P("fs", "tp"),
        P("fs", "tp"),
        P("fs", "tp"),
        P("tp"),
        P("tp", None),
        P(),
        P("tp", "fs"),
        P("tp", "fs"),
    )
    return jax.shard_map(
        body,
        mesh=mesh,
        in_specs=placed,
        out_specs=P(("grp", "fs"), ("sp", "tp"), None),
        check_vma=False,
    )
```

```python
import functools
import math

import jax
import jax.numpy as jnp
from jax import lax
from jax.experimental import pallas as pl
from jax.experimental.pallas import tpu as pltpu
from jax.sharding import PartitionSpec as P

LANES = 128
norm_eps = 1e-06
MESH = pl.DeviceIdType.MESH
F32 = jnp.float32
BF16 = jnp.bfloat16
N_PROJ = 6
KEY, VALUE, FORGET, INPUT, QUERY, READ = range(N_PROJ)
GROUPS = 2
CHUNKS = 4
X_CHUNKS = 4
N_SMALL = 4
N_ASK = 2


def dot_nn(a, b):
    return lax.dot_general(a, b, (((1,), (0,)), ((), ())), preferred_element_type=F32)


def dot_nt(a, b):
    return lax.dot_general(a, b, (((1,), (1,)), ((), ())), preferred_element_type=F32)


def dot_tn(a, b):
    return lax.dot_general(a, b, (((0,), (0,)), ((), ())), preferred_element_type=F32)


def halves(x):
    high = x.astype(BF16)
    return high, (x - high.astype(F32)).astype(BF16)


def unit_list(cols):
    g_cols = cols // GROUPS
    last = (GROUPS - 1) * g_cols
    units = [(FORGET, 0), (INPUT, 0), (QUERY, last)]
    for g in range(1, GROUPS):
        units += [(w, g * g_cols) for w in (KEY, VALUE, FORGET, INPUT)]
    units += [(QUERY, g * g_cols) for g in range(GROUPS - 1)]
    units += [(READ, g * g_cols) for g in range(GROUPS)]
    return units


def kernel(
    n_sp, n_fs, n_tp,
    tok_hbm, gain_hbm, w_k, w_v, w_f, w_i, w_q, w_r, offs_hbm, room_hbm, out_gain_hbm, o_attn, o_rec,
    out,
    gain, offs, room, out_gain,
    tok, wbuf, obuf, xt, xg, ss, acc, psend, precv, kv, qbuf, qdec, ecum, kinv, fresh, rec_i,
    att, run, q_back, v_back, v_far, loc, st_loc, dec, st_in, st_out, heads, hrecv, part_acc, mix,
    t_sem, s_sem, w_sem, x_send, x_recv, f_send, own_send, own_recv, ss_send, ss_recv, p_send, p_recv,
    kv_send, kv_recv, st_send, st_recv, o_send, o_recv, b_sem, h_send, h_recv, m_send, m_recv, ready,
):
    sp, fs, tp = lax.axis_index("sp"), lax.axis_index("fs"), lax.axis_index("tp")
    rows, feat_t = tok.shape
    feat_f = xt.shape[2]
    width = feat_t * n_tp
    cols = wbuf.shape[2]
    n_heads = cols // LANES
    share = rows // n_tp
    out_cols = obuf.shape[3]
    g_cols = cols // GROUPS
    g_heads = n_heads // GROUPS
    n_kv = X_CHUNKS + 2 * (GROUPS - 1)
    x_rows = rows // X_CHUNKS
    relay = 0
    is_relay = tp == relay
    has_next = sp < n_sp - 1
    has_prev = sp > 0
    n_ask = min(N_ASK, n_sp - 2)
    first_ask = n_sp - n_ask
    asks = sp >= first_ask
    last = GROUPS - 1
    near = sp < 3
    far = sp >= 3

    def fs_at(step):
        return lax.rem(fs + step, n_fs)

    def tp_at(step):
        return lax.rem(tp + step, n_tp)

    def group(g):
        return slice(g * g_cols, (g + 1) * g_cols)

    tok_copy = pltpu.make_async_copy(tok_hbm, tok, t_sem.at[0])
    tok_copy.start()
    barrier = pltpu.get_barrier_semaphore()
    for df in range(n_fs):
        for dt in range(n_tp):
            if df or dt:
                pl.semaphore_signal(
                    barrier, inc=1, device_id={"fs": fs_at(df), "tp": tp_at(dt)}, device_id_type=MESH
                )

    @pl.when(has_next)
    def _():
        pl.semaphore_signal(barrier, inc=1, device_id={"sp": sp + 1}, device_id_type=MESH)


    small_copies = [
        pltpu.make_async_copy(source, target, s_sem.at[i])
        for i, (source, target) in enumerate(
            ((gain_hbm, gain), (offs_hbm, offs), (room_hbm, room), (out_gain_hbm, out_gain))
        )
    ]
    w_copies = [
        pltpu.make_async_copy(w, wbuf.at[i], w_sem.at[i // 2])
        for i, w in enumerate((w_k, w_v, w_f, w_i, w_q, w_r))
    ]
    o_copies = [
        pltpu.make_async_copy(w, obuf.at[tp, i], w_sem.at[N_PROJ // 2]) for i, w in enumerate((o_attn, o_rec))
    ]

    def w_wait(w):
        pair = wbuf.at[pl.ds(w, 2)]
        pltpu.make_async_copy(pair, pair, w_sem.at[w // 2]).wait()

    def land(view, sem, wait_send=False):
        copy = pltpu.make_async_remote_copy(
            src_ref=view, dst_ref=view, send_sem=sem, recv_sem=sem,
            device_id={"tp": tp_at(1)}, device_id_type=MESH,
        )
        if wait_send:
            copy.wait_send()
        else:
            copy.wait_recv()

    for copy in small_copies + w_copies + o_copies:
        copy.start()
    tok_copy.wait()

    pl.semaphore_wait(barrier, n_fs * n_tp - 1 + jnp.where(has_prev, 1, 0))

    @pl.when(has_prev)
    def _():
        pl.semaphore_signal(ready, inc=1, device_id={"sp": sp - 1}, device_id_type=MESH)

    def holder(f_index):
        return (f_index * feat_f) // feat_t

    def held(f_index):
        return pl.ds(pl.multiple_of(lax.rem(f_index * feat_f, feat_t), LANES), feat_f)

    def x_part(c):
        return pl.ds(c * x_rows, x_rows)

    def x_copy(df, c):
        return pltpu.make_async_remote_copy(
            src_ref=tok.at[x_part(c), held(fs_at(df))], dst_ref=xt.at[fs, x_part(c)],
            send_sem=x_send.at[df - 1], recv_sem=x_recv.at[(n_fs - df - 1) * X_CHUNKS + c],
            device_id={"fs": fs_at(df), "tp": relay}, device_id_type=MESH,
        )

    def f_copy(df, c, dt):
        slot = fs_at(df)
        return pltpu.make_async_remote_copy(
            src_ref=xt.at[slot, x_part(c)], dst_ref=xt.at[slot, x_part(c)],
            send_sem=f_send.at[(df - 1) * (n_tp - 1) + dt - 1],
            recv_sem=x_recv.at[(df - 1) * X_CHUNKS + c],
            device_id={"tp": tp_at(dt)}, device_id_type=MESH,
        )

    def own_copy(dt):
        return pltpu.make_async_remote_copy(
            src_ref=tok.at[:, held(fs)], dst_ref=xt.at[fs],
            send_sem=own_send.at[dt - 1], recv_sem=own_recv.at[0],
            device_id={"tp": tp_at(dt)}, device_id_type=MESH,
        )

    for df in range(1, n_fs):
        @pl.when(holder(fs_at(df)) == tp)
        def _(df=df):
            for c in range(X_CHUNKS):
                x_copy(df, c).start()

    own_holder = holder(fs) == tp

    @pl.when(own_holder)
    def _():
        for dt in range(1, n_tp):
            own_copy(dt).start()

    squares = jnp.zeros((rows, LANES), F32)
    for c in range(feat_t // LANES):
        piece = tok[:, c * LANES:(c + 1) * LANES].astype(F32)
        squares = squares + piece * piece
    ss[tp] = squares

    def ss_copy(dt):
        return pltpu.make_async_remote_copy(
            src_ref=ss.at[tp], dst_ref=ss.at[tp],
            send_sem=ss_send.at[dt - 1], recv_sem=ss_recv.at[n_tp - dt - 1],
            device_id={"tp": tp_at(dt)}, device_id_type=MESH,
        )

    for dt in range(1, n_tp):
        ss_copy(dt).start()

    for copy in small_copies:
        copy.wait()
    gain_f = gain[:, pl.ds(pl.multiple_of(fs * feat_f, LANES), feat_f)]

    @pl.when(own_holder)
    def _():
        xg[0] = (tok[:, held(fs)].astype(F32) * gain_f).astype(BF16)

    units = unit_list(cols)
    n_units = len(units)

    def first_copy(df, c):
        index = (df - 1) * (n_units + X_CHUNKS) + n_units + c
        return pltpu.make_async_remote_copy(
            src_ref=psend.at[df - 1, pl.ds(KEY, 2), x_part(c), pl.ds(0, g_cols)],
            dst_ref=precv.at[df - 1, pl.ds(KEY, 2), x_part(c), pl.ds(0, g_cols)],
            send_sem=p_send.at[df - 1], recv_sem=p_recv.at[index],
            device_id={"fs": fs_at(df)}, device_id_type=MESH,
        )

    def p_copy(df, u):
        w, first = units[u]
        index = (df - 1) * (n_units + X_CHUNKS) + u
        return pltpu.make_async_remote_copy(
            src_ref=psend.at[df - 1, w, :, pl.ds(first, g_cols)],
            dst_ref=precv.at[df - 1, w, :, pl.ds(first, g_cols)],
            send_sem=p_send.at[df - 1], recv_sem=p_recv.at[index],
            device_id={"fs": fs_at(df)}, device_id_type=MESH,
        )

    @pl.when(jnp.logical_not(own_holder))
    def _():
        land(xt.at[fs], own_recv.at[0])
        xg[0] = (xt[fs].astype(F32) * gain_f).astype(BF16)

    total = ss[tp]
    for dt in range(1, n_tp):
        other = tp_at(dt)
        land(ss.at[other], ss_recv.at[dt - 1])
        total = total + ss[other]
    factor = lax.rsqrt(jnp.sum(total, axis=1, keepdims=True) / width + norm_eps)

    def own_product(w, cut):
        acc[w, :, cut] = dot_nn(xg[0], wbuf[w, :, cut])

    w_wait(KEY)
    own_product(KEY, group(0))
    own_product(VALUE, group(0))
    for c in range(X_CHUNKS):
        part = slice(c * x_rows, (c + 1) * x_rows)
        for df in range(1, n_fs):
            slot = fs_at(df)
            land(xt.at[slot, x_part(c)], x_recv.at[(df - 1) * X_CHUNKS + c])

            @pl.when(is_relay)
            def _(df=df, c=c):
                for dt in range(1, n_tp):
                    f_copy(df, c, dt).start()

            xg[df, part, :] = (xt[slot, part, :].astype(F32) * gain_f).astype(BF16)
            for w in (KEY, VALUE):
                psend[df - 1, w, part, 0:g_cols] = dot_nn(xg[df, part, :], wbuf[w, :, 0:g_cols]).astype(BF16)
            first_copy(df, c).start()

    def partials(w, first, count):
        cut = slice(first, first + count)
        for df in range(1, n_fs):
            psend[df - 1, w, :, cut] = dot_nn(xg[df], wbuf[w, :, cut]).astype(BF16)

    def send_unit(w, g):
        for df in range(1, n_fs):
            p_copy(df, units.index((w, g * g_cols))).start()


    def finish(w, g):
        cut = group(g)
        value = acc[w, :, cut]
        for df in range(1, n_fs):
            p_copy(df, units.index((w, g * g_cols))).wait_recv()
            value = value + precv[df - 1, w, :, cut].astype(F32)
        return (value * factor).astype(BF16)

    def kv_copy(slot, c):
        if c < X_CHUNKS:
            view = kv.at[slot, pl.ds(0, 2), x_part(c)]
        else:
            view = kv.at[slot, 2 + c - X_CHUNKS]
        return pltpu.make_async_remote_copy(
            src_ref=view, dst_ref=view,
            send_sem=kv_send.at[slot], recv_sem=kv_recv.at[slot * n_kv + c],
            device_id={"sp": lax.rem(sp + 1, n_sp)}, device_id_type=MESH,
        )

    def group_kv(g):
        if g == 0:
            return range(X_CHUNKS)
        return range(X_CHUNKS + 2 * (g - 1), X_CHUNKS + 2 * g)

    def send_kv(c):
        @pl.when(has_next)
        def _():
            kv_copy(sp, c).start()

    def finish_first(c):
        part = slice(c * x_rows, (c + 1) * x_rows)
        for df in range(1, n_fs):
            first_copy(df, c).wait_recv()
        for w in (KEY, VALUE):
            value = acc[w, part, 0:g_cols]
            for df in range(1, n_fs):
                value = value + precv[df - 1, w, part, 0:g_cols].astype(F32)
            kv[sp, w, part, :] = (value * factor[part]).astype(BF16)
        send_kv(c)

    def finish_kv(w, g):
        kv[sp, 2 * g + w] = finish(w, g)
        send_kv(X_CHUNKS + 2 * (g - 1) + w)

    def hand_on(step, c):
        kv_copy(sp - step, c).wait_recv()
        goes_on = has_next
        if c in group_kv(last):
            goes_on = jnp.logical_and(has_next, jnp.logical_or(step < sp, sp + 1 < first_ask))

        @pl.when(goes_on)
        def _():
            kv_copy(sp - step, c).start()

    def from_step(step, g):
        return step + 1 if g == last and step >= first_ask else step

    def hand_on_if(step, c):
        if step < n_sp:
            g = last if c in group_kv(last) else 0
            pl.when(sp >= from_step(step, g))(functools.partial(hand_on, step, c))

    @pl.when(has_next)
    def _():
        pl.semaphore_wait(ready, 1)

    w_wait(FORGET)
    quarter = X_CHUNKS // 4
    for w in (FORGET, INPUT):
        partials(w, 0, cols)
        send_unit(w, 0)
        for c in range(quarter):
            finish_first((w - FORGET) * quarter + c)
    w_wait(QUERY)
    partials(QUERY, 0, cols)
    pl.when(has_prev)(functools.partial(send_unit, QUERY, last))
    for w in (KEY, VALUE):
        partials(w, g_cols, cols - g_cols)
        for g in range(1, GROUPS):
            send_unit(w, g)
        for c in range(quarter):
            finish_first((2 + w) * quarter + c)
    for w in (FORGET, INPUT):
        for g in range(1, GROUPS):
            send_unit(w, g)
    pl.when(sp == 0)(functools.partial(send_unit, QUERY, last))
    for g in range(last):
        send_unit(QUERY, g)
    partials(READ, 0, cols)
    for g in range(GROUPS):
        send_unit(READ, g)
    for w in (FORGET, INPUT):
        own_product(w, slice(0, cols))
    for w in (KEY, VALUE):
        own_product(w, slice(g_cols, cols))
    for w in (QUERY, READ):
        own_product(w, slice(0, cols))

    def o_copy(dt):
        return pltpu.make_async_remote_copy(
            src_ref=obuf.at[tp], dst_ref=obuf.at[tp], send_sem=o_send.at[dt - 1], recv_sem=o_recv.at[n_tp - dt - 1],
            device_id={"tp": tp_at(dt)}, device_id_type=MESH,
        )

    pltpu.make_async_copy(obuf.at[tp], obuf.at[tp], w_sem.at[N_PROJ // 2]).wait()
    for dt in range(1, n_tp):
        o_copy(dt).start()

    iota_r = lax.broadcasted_iota(jnp.int32, (rows, rows), 0)
    iota_c = lax.broadcasted_iota(jnp.int32, (rows, rows), 1)
    causal = iota_r >= iota_c
    strict = jnp.concatenate([iota_c < iota_r] * g_heads, axis=0)
    lower = jnp.where(causal, 1.0, 0.0).astype(BF16)
    lower = jnp.concatenate([lower, lower], axis=1)
    later = jnp.where(iota_r > iota_c, 1.0, 0.0).astype(BF16)
    sums = jnp.concatenate([later, jnp.ones((rows, LANES), BF16)], axis=1)
    sums = jnp.concatenate([sums, sums], axis=0)
    scale = 1.0 / math.sqrt(LANES)

    def lanes_of(h):
        return slice(h * LANES, (h + 1) * LANES)

    def heads_of(g):
        return range(g * g_heads, (g + 1) * g_heads)

    def gates(g):
        cut = group(g)
        rooms = jnp.concatenate([room[h:h + 1, :] for h in heads_of(g)], axis=1)
        key_in = rooms * jax.nn.sigmoid(-finish(FORGET, g).astype(F32))
        high, low = halves(jnp.log1p(-key_in))
        cum = dot_nn(lower, jnp.concatenate([high, low], axis=0))
        last = cum[rows - 1:rows, :]
        ecum[:, cut] = jnp.exp(cum)
        kinv[:, cut] = (key_in * jnp.exp(-cum)).astype(BF16)
        fresh[:, cut] = (key_in * jnp.exp(last - cum)).astype(BF16)
        decay = jnp.exp(last)
        for i, h in enumerate(heads_of(g)):
            dec[h] = jnp.broadcast_to(decay[:, lanes_of(i)], dec.shape[1:])

    def st_copy(h):
        return pltpu.make_async_remote_copy(
            src_ref=st_out.at[h], dst_ref=st_in.at[h], send_sem=st_send.at[0], recv_sem=st_recv.at[h],
            device_id={"sp": lax.rem(sp + 1, n_sp)}, device_id_type=MESH,
        )

    def local_state(g):
        rec_i[:, group(g)] = finish(INPUT, g)
        for h in heads_of(g):
            st_loc[h] = dot_tn(rec_i[:, lanes_of(h)], fresh[:, lanes_of(h)])

            @pl.when(jnp.logical_and(sp == 0, has_next))
            def _(h=h):
                st_out[h] = st_loc[h].astype(BF16)
                st_copy(h).start()

    def state_step(h):
        st_copy(h).wait_recv()

        @pl.when(has_next)
        def _():
            st_out[h] = (st_in[h].astype(F32) * dec[h, 0:1, :] + st_loc[h]).astype(BF16)
            st_copy(h).start()

    def state_steps(g, half=None):
        mine = heads_of(g)
        if half is not None:
            mine = mine[:1] if half == 0 else mine[1:]
        for h in mine:
            state_step(h)

    def state_step_if(at, g, half=None):
        if at < n_sp:
            pl.when(sp == at)(functools.partial(state_steps, g, half))

    def read_local(g):
        cut = group(g)
        qdec[:, cut] = (finish(READ, g).astype(F32) * ecum[:, cut]).astype(BF16)
        for h in heads_of(g):
            lanes = lanes_of(h)
            scores = jnp.where(causal, dot_nt(qdec[:, lanes], kinv[:, lanes]), 0.0)
            loc[:, lanes] = dot_nn(scores.astype(BF16), rec_i[:, lanes])

    n_land = 2 + g_heads
    early = pl.ds(0, last * g_cols)

    def h_sem(df, dt, mark):
        return h_recv.at[dt if df == 0 else n_tp + ((df - 1) * n_tp + dt) * n_land + mark]

    def h_copy(df, dt, kind, first, count, mark):
        lands = (n_tp - dt) % n_tp
        lanes = pl.ds(first, count)
        return pltpu.make_async_remote_copy(
            src_ref=heads.at[kind, pl.ds(pl.multiple_of(tp_at(dt) * share, share), share), lanes],
            dst_ref=hrecv.at[df, lands, kind, :, lanes],
            send_sem=h_send.at[df * n_tp + dt], recv_sem=h_sem(df, lands, mark),
            device_id={"fs": fs_at(df), "tp": tp_at(dt)}, device_id_type=MESH,
        )

    h_order = [(df, dt) for df in list(range(1, n_fs)) + [0] for dt in range(n_tp) if df or dt]

    def send_heads(kind, first, count, mark):
        for df, dt in h_order:
            h_copy(df, dt, kind, first, count, mark).start()

    def send_attn(g):
        heads[0, :, group(g)] = att[:, group(g)].astype(BF16)
        send_heads(0, g * g_cols, g_cols, 1 if g == last else 0)

    def finish_rec(h):
        lanes = lanes_of(h)

        @pl.when(has_prev)
        def _():
            loc[:, lanes] += dot_nt(qdec[:, lanes], st_in[h])

        raw = loc[:, lanes]
        norm = lax.rsqrt(jnp.mean(raw * raw, axis=1, keepdims=True) + norm_eps)
        heads[1, :, lanes] = (raw * norm * out_gain[...]).astype(BF16)

    def send_rec(g):
        for i, h in enumerate(heads_of(g)):
            if g == last:
                pl.when(far)(functools.partial(state_step, h))
            finish_rec(h)
            if g == last:
                send_heads(1, h * LANES, LANES, 2 + i)
        if g < last:
            send_heads(1, g * g_cols, g_cols, 0)

    def sticks(queries, slot, g, diagonal):
        z = jnp.concatenate(
            [
                dot_nt(queries[:, lanes_of(i)], kv[slot, 2 * g, :, lanes_of(i)]) * scale + offs[0:1, h:h + 1]
                for i, h in enumerate(heads_of(g))
            ],
            axis=0,
        )
        keep = -(jnp.maximum(z, 0.0) + jnp.log(1.0 + jnp.exp(-jnp.abs(z))))
        log_stick = z + keep
        if diagonal:
            keep = jnp.where(strict, keep, 0.0)
        both = dot_nn(jnp.concatenate(halves(keep), axis=1), sums)
        stick = jnp.exp(log_stick + both[:, :rows])
        if diagonal:
            stick = jnp.where(strict, stick, 0.0)
        return stick.astype(BF16), both

    def attend(slot, g, diagonal):
        stick, both = sticks(qbuf.at[:, group(g)], slot, g, diagonal)
        for i, h in enumerate(heads_of(g)):
            mine = slice(i * rows, (i + 1) * rows)
            value = dot_nn(stick[mine], kv[slot, 2 * g + 1, :, lanes_of(i)])
            if diagonal:
                att[:, lanes_of(h)] = value
                run[h] = both[mine, rows:]
            else:
                past = run[h]
                att[:, lanes_of(h)] += value * jnp.exp(past)
                run[h] = past + both[mine, rows:]

    def attend_if(step, g):
        if step < n_sp:
            pl.when(sp >= from_step(step, g))(functools.partial(attend, sp - step, g, False))

    def attend_rest(g):
        def block(step, carry):
            for c in group_kv(g):
                hand_on(step, c)
            attend(sp - step, g, False)
            return carry

        end = jnp.where(asks, sp, sp + 1) if g == last else sp + 1
        lax.fori_loop(3, end, block, 0)

    def q_copy(asker):
        return pltpu.make_async_remote_copy(
            src_ref=qbuf.at[:, pl.ds(last * g_cols, g_cols)], dst_ref=q_back.at[asker],
            send_sem=b_sem.at[asker], recv_sem=b_sem.at[asker], device_id={"sp": 0}, device_id_type=MESH,
        )

    def v_copy(asker):
        return pltpu.make_async_remote_copy(
            src_ref=v_back.at[asker], dst_ref=v_far,
            send_sem=b_sem.at[n_ask + asker], recv_sem=b_sem.at[n_ask + asker],
            device_id={"sp": first_ask + asker}, device_id_type=MESH,
        )

    def ask_back():
        for asker in range(n_ask):
            @pl.when(sp == first_ask + asker)
            def _(asker=asker):
                q_copy(asker).start()

    def answer():
        for asker in reversed(range(n_ask)):
            q_copy(asker).wait_recv()
            stick, _ = sticks(q_back.at[asker], 0, last, False)
            for i in range(g_heads):
                value = dot_nn(stick[i * rows:(i + 1) * rows], kv[0, 2 * last + 1, :, lanes_of(i)])
                v_back[asker, :, lanes_of(i)] = value.astype(BF16)
            v_copy(asker).start()

    def take_answer():
        for asker in range(n_ask):
            @pl.when(sp == first_ask + asker)
            def _(asker=asker):
                v_copy(asker).wait_recv()

        for i, h in enumerate(heads_of(last)):
            att[:, lanes_of(h)] += v_far[:, lanes_of(i)].astype(F32) * jnp.exp(run[h])

    for c in group_kv(0):
        hand_on_if(1, c)
    gates(0)
    local_state(0)

    def last_queries():
        qbuf[:, group(last)] = finish(QUERY, last)

    pl.when(has_prev)(last_queries)
    for c in group_kv(0):
        hand_on_if(2, c)
        if c == 0 and n_sp <= 4:
            ask_back()
    for g in range(1, GROUPS):
        for w in (KEY, VALUE):
            finish_kv(w, g)
    state_step_if(1, 0)
    for g in range(1, GROUPS):
        gates(g)
        hand_on_if(1, group_kv(g)[0])
        local_state(g)
        hand_on_if(1, group_kv(g)[1])
    state_step_if(2, 0)
    pl.when(sp == 0)(last_queries)
    for g in range(1, GROUPS):
        state_step_if(1, g)
    for g in range(last):
        qbuf[:, group(g)] = finish(QUERY, g)
        attend(sp, g, True)
        attend_if(1, g)
        attend_if(2, g)
        attend_rest(g)
        send_attn(g)
    if n_sp > 4:
        ask_back()
    if n_ask:
        pl.when(sp == 0)(answer)
    for g in range(1, GROUPS):
        attend(sp, g, True)
        attend_if(1, g)

        @pl.when(sp < 2)
        def _(g=g):
            send_attn(g)

    state_step_if(2, last, 0)
    read_local(0)

    @pl.when(near)
    def _():
        send_rec(0)

    for g in range(1, GROUPS):
        read_local(g)
        if g == last:
            state_step_if(2, g, 1)
        hand_on_if(2, group_kv(g)[0])
        hand_on_if(2, group_kv(g)[1])
        attend_if(2, g)

        @pl.when(far)
        def _(g=g):
            attend_rest(g)

        if g == last:
            pl.when(asks)(take_answer)

        @pl.when(sp >= 2)
        def _(g=g):
            send_attn(g)

        @pl.when(far)
        def _(g=g):
            state_steps(g - 1)
            send_rec(g - 1)

        send_rec(g)

    for dt in range(1, n_tp):
        other = tp_at(dt)
        land(obuf.at[other], o_recv.at[dt - 1])

    half = out_cols // CHUNKS

    def columns(owner, k):
        return pl.ds(pl.multiple_of(owner * out_cols + k * half, LANES), half)

    def m_copy(df, k):
        return pltpu.make_async_remote_copy(
            src_ref=mix.at[df - 1, k], dst_ref=out.at[:, columns(fs, k)],
            send_sem=m_send.at[df - 1], recv_sem=m_recv.at[df - 1],
            device_id={"fs": fs_at(n_fs - df)}, device_id_type=MESH,
        )

    def product(df, kind, lanes, cut):
        value = None
        for dt in range(n_tp):
            if df == 0 and dt == 0:
                left = heads[kind, pl.ds(pl.multiple_of(tp * share, share), share), lanes]
            else:
                left = hrecv[df, dt, kind, :, lanes]
            term = dot_nn(left, obuf[tp_at(dt), kind, lanes, cut])
            value = term if value is None else value + term
        return value

    whole = slice(0, out_cols)
    final = lanes_of(n_heads - 1)
    for df in range(1, n_fs):
        for dt in range(n_tp):
            land(hrecv.at[df, dt, :, :, early], h_sem(df, dt, 0))
        for kind in range(2):
            for g in range(last):
                if kind == 0 and g == 0:
                    part_acc[df - 1] = product(df, kind, group(g), whole)
                else:
                    part_acc[df - 1] += product(df, kind, group(g), whole)
        marks = [(0, group(last))] + [(1, lanes_of(h)) for h in heads_of(last)]
        for mark, (kind, lanes) in enumerate(marks):
            for dt in range(n_tp):
                land(hrecv.at[df, dt, kind, :, lanes], h_sem(df, dt, 1 + mark))
            if mark < len(marks) - 1:
                part_acc[df - 1] += product(df, kind, lanes, whole)
        for k in range(CHUNKS):
            cut = slice(k * half, (k + 1) * half)
            mix[df - 1, k] = (part_acc[df - 1, :, cut] + product(df, 1, final, cut)).astype(BF16)
            m_copy(df, k).start()
    for dt in range(1, n_tp):
        land(hrecv.at[0, dt], h_sem(0, dt, 0))
    for k in range(CHUNKS):
        cut = slice(k * half, (k + 1) * half)
        value = product(0, 0, slice(0, cols), cut) + product(0, 1, slice(0, cols), cut)
        out[:, columns(fs, k)] = value.astype(BF16)

    for df in range(1, n_fs):
        @pl.when(holder(fs_at(df)) == tp)
        def _(df=df):
            land(xt.at[0], x_send.at[df - 1], True)

        @pl.when(is_relay)
        def _(df=df):
            for dt in range(1, n_tp):
                land(xt.at[0], f_send.at[(df - 1) * (n_tp - 1) + dt - 1], True)

        land(psend.at[df - 1], p_send.at[df - 1], True)
    for dt in range(1, n_tp):
        @pl.when(own_holder)
        def _(dt=dt):
            own_copy(dt).wait_send()

        ss_copy(dt).wait_send()
        o_copy(dt).wait_send()
    for df, dt in h_order:
        land(hrecv.at[df, dt], h_send.at[df * n_tp + dt], True)

    @pl.when(has_next)
    def _():
        land(st_out, st_send.at[0], True)

        def drain(slot, carry):
            land(kv.at[slot], kv_send.at[slot], True)
            return carry

        shorter = sp + 1 >= first_ask

        @pl.when(shorter)
        def _():
            land(kv.at[0, pl.ds(0, 2 * last)], kv_send.at[0], True)

        lax.fori_loop(jnp.where(shorter, 1, 0), sp + 1, drain, 0)

    for asker in range(n_ask):
        @pl.when(sp == first_ask + asker)
        def _(asker=asker):
            q_copy(asker).wait_send()

        @pl.when(sp == 0)
        def _(asker=asker):
            v_copy(asker).wait_send()

    for df in range(1, n_fs):
        land(mix.at[df - 1], m_recv.at[df - 1])
        land(mix.at[df - 1], m_send.at[df - 1], True)


def body(
    tokens, mix_gain, attn_query, attn_key, attn_value, rec_query, rec_forget, rec_input,
    break_offset, forget_room, out_gain, out_attn, out_rec,
):
    n_sp, n_fs, n_tp = lax.axis_size("sp"), lax.axis_size("fs"), lax.axis_size("tp")
    rows, feat_t = tokens.shape[1], tokens.shape[2]
    feat_f, cols = attn_query.shape
    width = feat_t * n_tp
    n_heads = cols // LANES
    out_rows, out_cols = out_attn.shape
    share = rows // n_tp
    piece = out_cols // CHUNKS
    n_sends = len(unit_list(cols)) + X_CHUNKS
    n_kv = X_CHUNKS + 2 * (GROUPS - 1)
    n_ask = min(N_ASK, n_sp - 2)
    hbm = pl.BlockSpec(memory_space=pl.ANY)
    vmem = pl.BlockSpec(memory_space=pltpu.VMEM)
    dma = pltpu.SemaphoreType.DMA
    square = (n_heads, LANES, LANES)
    others = n_fs - 1
    result = pl.pallas_call(
        functools.partial(kernel, n_sp, n_fs, n_tp),
        out_shape=pltpu.VMEM((share, width), BF16),
        in_specs=[hbm] * 13,
        out_specs=vmem,
        scratch_shapes=[
            pltpu.VMEM((1, width), F32),
            pltpu.VMEM((1, n_heads), F32),
            pltpu.VMEM((n_heads, LANES), F32),
            pltpu.VMEM((1, LANES), F32),
            pltpu.VMEM((rows, feat_t), BF16),
            pltpu.VMEM((N_PROJ, feat_f, cols), BF16),
            pltpu.VMEM((n_tp, 2, out_rows, out_cols), BF16),
            pltpu.VMEM((n_fs, rows, feat_f), BF16),
            pltpu.VMEM((n_fs, rows, feat_f), BF16),
            pltpu.VMEM((n_tp, rows, LANES), F32),
            pltpu.VMEM((N_PROJ, rows, cols), F32),
            pltpu.VMEM((others, N_PROJ, rows, cols), BF16),
            pltpu.VMEM((others, N_PROJ, rows, cols), BF16),
            pltpu.VMEM((n_sp, 2 * GROUPS, rows, cols // GROUPS), BF16),
            pltpu.VMEM((rows, cols), BF16),
            pltpu.VMEM((rows, cols), BF16),
            pltpu.VMEM((rows, cols), F32),
            pltpu.VMEM((rows, cols), BF16),
            pltpu.VMEM((rows, cols), BF16),
            pltpu.VMEM((rows, cols), BF16),
            pltpu.VMEM((rows, cols), F32),
            pltpu.VMEM((n_heads, rows, LANES), F32),
            pltpu.VMEM((max(n_ask, 1), rows, cols // GROUPS), BF16),
            pltpu.VMEM((max(n_ask, 1), rows, cols // GROUPS), BF16),
            pltpu.VMEM((rows, cols // GROUPS), BF16),
            pltpu.VMEM((rows, cols), F32),
            pltpu.VMEM(square, F32),
            pltpu.VMEM((n_heads, 8, LANES), F32),
            pltpu.VMEM(square, BF16),
            pltpu.VMEM(square, BF16),
            pltpu.VMEM((2, rows, cols), BF16),
            pltpu.VMEM((n_fs, n_tp, 2, share, cols), BF16),
            pltpu.VMEM((others, share, out_cols), F32),
            pltpu.VMEM((others, CHUNKS, share, piece), BF16),
            dma((1,)), dma((N_SMALL,)), dma((N_PROJ // 2 + 1,)),
            dma((others,)), dma((others * X_CHUNKS,)), dma((others * (n_tp - 1),)),
            dma((n_tp - 1,)), dma((1,)), dma((n_tp - 1,)), dma((n_tp - 1,)),
            dma((others,)), dma((others * n_sends,)),
            dma((n_sp,)), dma(((n_sp - 1) * n_kv,)),
            dma((1,)), dma((n_heads,)),
            dma((n_tp - 1,)), dma((n_tp - 1,)), dma((max(2 * n_ask, 1),)),
            dma((n_fs * n_tp,)), dma((n_tp + others * n_tp * (2 + n_heads // GROUPS),)),
            dma((others,)), dma((others,)),
            pltpu.SemaphoreType.REGULAR,
        ],
        compiler_params=pltpu.CompilerParams(
            collective_id=0, has_side_effects=True, vmem_limit_bytes=60 * 1024 * 1024
        ),
        name="layer",
    )(
        tokens.reshape(rows, feat_t), mix_gain.reshape(1, width),
        attn_key, attn_value, rec_forget, rec_input, attn_query, rec_query,
        break_offset.reshape(1, n_heads), forget_room, out_gain.reshape(1, LANES), out_attn, out_rec,
    )
    return result.reshape(1, share, width)


def solution(mesh):
    placed = (
        P(("grp", "fs"), "sp", "tp"),
        P(),
        P("fs", "tp"),
        P("fs", "tp"),
        P("fs", "tp"),
        P("fs", "tp"),
        P("fs", "tp"),
        P("fs", "tp"),
        P("tp"),
        P("tp", None),
        P(),
        P("tp", "fs"),
        P("tp", "fs"),
    )
    return jax.shard_map(
        body,
        mesh=mesh,
        in_specs=placed,
        out_specs=P(("grp", "fs"), ("sp", "tp"), None),
        check_vma=False,
    )
```

```python
import functools
import math

import jax
import jax.numpy as jnp
from jax import lax
from jax.experimental import pallas as pl
from jax.experimental.pallas import tpu as pltpu
from jax.sharding import PartitionSpec as P

LANES = 128
norm_eps = 1e-06
MESH = pl.DeviceIdType.MESH
F32 = jnp.float32
BF16 = jnp.bfloat16
N_PROJ = 6
KEY, VALUE, FORGET, INPUT, QUERY, READ = range(N_PROJ)
GROUPS = 2
CHUNKS = 4
X_SPLIT = (1,2,2,3)
X_CHUNKS = len(X_SPLIT)
N_SMALL = 4
N_ASK = 2
SUM_ROWS = 16


def dot_nn(a, b):
    return lax.dot_general(a, b, (((1,), (0,)), ((), ())), preferred_element_type=F32)


def dot_nt(a, b):
    return lax.dot_general(a, b, (((1,), (1,)), ((), ())), preferred_element_type=F32)


def dot_tn(a, b):
    return lax.dot_general(a, b, (((0,), (0,)), ((), ())), preferred_element_type=F32)


def halves(x):
    high = x.astype(BF16)
    return high, (x - high.astype(F32)).astype(BF16)


def unit_list(cols):
    g_cols = cols // GROUPS
    last = (GROUPS - 1) * g_cols
    units = [(FORGET, 0), (INPUT, 0), (QUERY, last)]
    for g in range(1, GROUPS):
        units += [(w, g * g_cols) for w in (KEY, VALUE, FORGET, INPUT)]
    units += [(QUERY, g * g_cols) for g in range(GROUPS - 1)]
    units += [(READ, g * g_cols) for g in range(GROUPS)]
    return units


def ask_list(n_sp):
    first = n_sp - min(N_ASK, n_sp - 2)
    pairs = [(asker, 0) for asker in range(first, n_sp)]
    if n_sp > 2:
        pairs.append((n_sp - 1, n_sp - 2))
    return pairs


def kernel(
    n_sp, n_fs, n_tp,
    tok_hbm, gain_hbm, w_k, w_v, w_f, w_i, w_q, w_r, offs_hbm, room_hbm, out_gain_hbm, o_attn, o_rec,
    out,
    gain, offs, room, out_gain,
    tok, wbuf, obuf, xt, xg, ss, acc, psend, precv, kv, qbuf, qdec, ecum, kinv, fresh, rec_i,
    att, run, q_back, v_back, v_far, loc, st_loc, dec, st_in, st_out, heads, hrecv, part_acc, mix,
    t_sem, s_sem, w_sem, x_send, x_recv, f_send, own_send, own_recv, ss_send, ss_recv, p_send, p_recv,
    kv_send, kv_recv, st_send, st_recv, o_send, o_recv, b_sem, h_send, h_recv, m_send, m_recv, ready,
):
    sp, fs, tp = lax.axis_index("sp"), lax.axis_index("fs"), lax.axis_index("tp")
    rows, feat_t = tok.shape
    feat_f = xt.shape[2]
    width = feat_t * n_tp
    cols = wbuf.shape[2]
    n_heads = cols // LANES
    share = rows // n_tp
    out_cols = obuf.shape[3]
    g_cols = cols // GROUPS
    g_heads = n_heads // GROUPS
    n_kv = X_CHUNKS + 2 * (GROUPS - 1)
    x_edges = [rows * sum(X_SPLIT[:c]) // sum(X_SPLIT) for c in range(X_CHUNKS + 1)]
    relay = 0
    is_relay = tp == relay
    has_next = sp < n_sp - 1
    has_prev = sp > 0
    n_ask = min(N_ASK, n_sp - 2)
    first_ask = n_sp - n_ask
    asks = sp >= first_ask
    asked = ask_list(n_sp)
    near_owner = n_sp - 2 if n_sp > 2 else -1
    last = GROUPS - 1
    near = sp < 3
    far = sp >= 3

    def fs_at(step):
        return lax.rem(fs + step, n_fs)

    def tp_at(step):
        return lax.rem(tp + step, n_tp)

    def group(g):
        return slice(g * g_cols, (g + 1) * g_cols)

    tok_copy = pltpu.make_async_copy(tok_hbm, tok, t_sem.at[0])
    tok_copy.start()
    barrier = pltpu.get_barrier_semaphore()
    for df in range(n_fs):
        for dt in range(n_tp):
            if df or dt:
                pl.semaphore_signal(
                    barrier, inc=1, device_id={"fs": fs_at(df), "tp": tp_at(dt)}, device_id_type=MESH
                )

    @pl.when(has_next)
    def _():
        pl.semaphore_signal(barrier, inc=1, device_id={"sp": sp + 1}, device_id_type=MESH)


    small_copies = [
        pltpu.make_async_copy(source, target, s_sem.at[i])
        for i, (source, target) in enumerate(
            ((gain_hbm, gain), (offs_hbm, offs), (room_hbm, room), (out_gain_hbm, out_gain))
        )
    ]
    w_copies = [
        pltpu.make_async_copy(w, wbuf.at[i], w_sem.at[i // 2])
        for i, w in enumerate((w_k, w_v, w_f, w_i, w_q, w_r))
    ]
    o_copies = [
        pltpu.make_async_copy(w, obuf.at[tp, i], w_sem.at[N_PROJ // 2]) for i, w in enumerate((o_attn, o_rec))
    ]

    def w_wait(w):
        pair = wbuf.at[pl.ds(w, 2)]
        pltpu.make_async_copy(pair, pair, w_sem.at[w // 2]).wait()

    def land(view, sem, wait_send=False):
        copy = pltpu.make_async_remote_copy(
            src_ref=view, dst_ref=view, send_sem=sem, recv_sem=sem,
            device_id={"tp": tp_at(1)}, device_id_type=MESH,
        )
        if wait_send:
            copy.wait_send()
        else:
            copy.wait_recv()

    for copy in small_copies + w_copies + o_copies:
        copy.start()
    tok_copy.wait()

    pl.semaphore_wait(barrier, n_fs * n_tp - 1 + jnp.where(has_prev, 1, 0))

    @pl.when(has_prev)
    def _():
        pl.semaphore_signal(ready, inc=1, device_id={"sp": sp - 1}, device_id_type=MESH)

    def holder(f_index):
        return (f_index * feat_f) // feat_t

    def held(f_index):
        return pl.ds(pl.multiple_of(lax.rem(f_index * feat_f, feat_t), LANES), feat_f)

    def x_part(c):
        return pl.ds(x_edges[c], x_edges[c + 1] - x_edges[c])

    def x_copy(df, c):
        return pltpu.make_async_remote_copy(
            src_ref=tok.at[x_part(c), held(fs_at(df))], dst_ref=xt.at[fs, x_part(c)],
            send_sem=x_send.at[df - 1], recv_sem=x_recv.at[(n_fs - df - 1) * X_CHUNKS + c],
            device_id={"fs": fs_at(df), "tp": relay}, device_id_type=MESH,
        )

    def f_copy(df, c, dt):
        slot = fs_at(df)
        return pltpu.make_async_remote_copy(
            src_ref=xt.at[slot, x_part(c)], dst_ref=xt.at[slot, x_part(c)],
            send_sem=f_send.at[(df - 1) * (n_tp - 1) + dt - 1],
            recv_sem=x_recv.at[(df - 1) * X_CHUNKS + c],
            device_id={"tp": tp_at(dt)}, device_id_type=MESH,
        )

    def own_copy(dt):
        return pltpu.make_async_remote_copy(
            src_ref=tok.at[:, held(fs)], dst_ref=xt.at[fs],
            send_sem=own_send.at[dt - 1], recv_sem=own_recv.at[0],
            device_id={"tp": tp_at(dt)}, device_id_type=MESH,
        )

    for df in range(1, n_fs):
        @pl.when(holder(fs_at(df)) == tp)
        def _(df=df):
            for c in range(X_CHUNKS):
                x_copy(df, c).start()

    own_holder = holder(fs) == tp

    @pl.when(own_holder)
    def _():
        for dt in range(1, n_tp):
            own_copy(dt).start()

    squares = jnp.zeros((rows, LANES), F32)
    for c in range(feat_t // LANES):
        piece = tok[:, c * LANES:(c + 1) * LANES].astype(F32)
        squares = squares + piece * piece
    ss[tp] = squares

    def ss_copy(dt):
        return pltpu.make_async_remote_copy(
            src_ref=ss.at[tp], dst_ref=ss.at[tp],
            send_sem=ss_send.at[dt - 1], recv_sem=ss_recv.at[n_tp - dt - 1],
            device_id={"tp": tp_at(dt)}, device_id_type=MESH,
        )

    for dt in range(1, n_tp):
        ss_copy(dt).start()

    for copy in small_copies:
        copy.wait()
    gain_f = gain[:, pl.ds(pl.multiple_of(fs * feat_f, LANES), feat_f)]

    @pl.when(own_holder)
    def _():
        xg[0] = (tok[:, held(fs)].astype(F32) * gain_f).astype(BF16)

    units = unit_list(cols)
    n_units = len(units)

    def first_copy(df, c):
        index = (df - 1) * (n_units + X_CHUNKS) + n_units + c
        return pltpu.make_async_remote_copy(
            src_ref=psend.at[df - 1, pl.ds(KEY, 2), x_part(c), pl.ds(0, g_cols)],
            dst_ref=precv.at[df - 1, pl.ds(KEY, 2), x_part(c), pl.ds(0, g_cols)],
            send_sem=p_send.at[df - 1], recv_sem=p_recv.at[index],
            device_id={"fs": fs_at(df)}, device_id_type=MESH,
        )

    def p_copy(df, u):
        w, first = units[u]
        index = (df - 1) * (n_units + X_CHUNKS) + u
        return pltpu.make_async_remote_copy(
            src_ref=psend.at[df - 1, w, :, pl.ds(first, g_cols)],
            dst_ref=precv.at[df - 1, w, :, pl.ds(first, g_cols)],
            send_sem=p_send.at[df - 1], recv_sem=p_recv.at[index],
            device_id={"fs": fs_at(df)}, device_id_type=MESH,
        )

    @pl.when(jnp.logical_not(own_holder))
    def _():
        land(xt.at[fs], own_recv.at[0])
        xg[0] = (xt[fs].astype(F32) * gain_f).astype(BF16)

    total = ss[tp]
    for dt in range(1, n_tp):
        other = tp_at(dt)
        land(ss.at[other], ss_recv.at[dt - 1])
        total = total + ss[other]
    factor = lax.rsqrt(jnp.sum(total, axis=1, keepdims=True) / width + norm_eps)

    def own_product(w, cut):
        acc[w, :, cut] = dot_nn(xg[0], wbuf[w, :, cut])

    @pl.when(sp == 0)
    def _():
        st_in[...] = jnp.zeros_like(st_in)

    w_wait(KEY)
    own_product(KEY, group(0))
    own_product(VALUE, group(0))
    for c in range(X_CHUNKS):
        part = slice(x_edges[c], x_edges[c + 1])
        for df in range(1, n_fs):
            slot = fs_at(df)
            land(xt.at[slot, x_part(c)], x_recv.at[(df - 1) * X_CHUNKS + c])

            @pl.when(is_relay)
            def _(df=df, c=c):
                for dt in range(1, n_tp):
                    f_copy(df, c, dt).start()

            xg[df, part, :] = (xt[slot, part, :].astype(F32) * gain_f).astype(BF16)
            for w in (KEY, VALUE):
                psend[df - 1, w, part, 0:g_cols] = dot_nn(xg[df, part, :], wbuf[w, :, 0:g_cols]).astype(BF16)
            first_copy(df, c).start()

    def partials(w, first, count):
        cut = slice(first, first + count)
        for df in range(1, n_fs):
            psend[df - 1, w, :, cut] = dot_nn(xg[df], wbuf[w, :, cut]).astype(BF16)

    def send_unit(w, g):
        for df in range(1, n_fs):
            p_copy(df, units.index((w, g * g_cols))).start()


    def finish(w, g):
        cut = group(g)
        value = acc[w, :, cut]
        for df in range(1, n_fs):
            p_copy(df, units.index((w, g * g_cols))).wait_recv()
            value = value + precv[df - 1, w, :, cut].astype(F32)
        return (value * factor).astype(BF16)

    def kv_copy(slot, c):
        if c < X_CHUNKS:
            view = kv.at[slot, pl.ds(0, 2), x_part(c)]
        else:
            view = kv.at[slot, 2 + c - X_CHUNKS]
        return pltpu.make_async_remote_copy(
            src_ref=view, dst_ref=view,
            send_sem=kv_send.at[slot], recv_sem=kv_recv.at[slot * n_kv + c],
            device_id={"sp": lax.rem(sp + 1, n_sp)}, device_id_type=MESH,
        )

    def group_kv(g):
        if g == 0:
            return range(X_CHUNKS)
        return range(X_CHUNKS + 2 * (g - 1), X_CHUNKS + 2 * g)

    def send_kv(c):
        @pl.when(has_next)
        def _():
            kv_copy(sp, c).start()

    def finish_first(c):
        part = slice(x_edges[c], x_edges[c + 1])
        for df in range(1, n_fs):
            first_copy(df, c).wait_recv()
        for w in (KEY, VALUE):
            value = acc[w, part, 0:g_cols]
            for df in range(1, n_fs):
                value = value + precv[df - 1, w, part, 0:g_cols].astype(F32)
            kv[sp, w, part, :] = (value * factor[part]).astype(BF16)
        send_kv(c)

    def finish_kv(w, g):
        kv[sp, 2 * g + w] = finish(w, g)
        goes_on = jnp.logical_and(has_next, sp != near_owner) if g == last else has_next

        @pl.when(goes_on)
        def _():
            kv_copy(sp, X_CHUNKS + 2 * (g - 1) + w).start()

    def hand_on(step, c):
        kv_copy(sp - step, c).wait_recv()
        goes_on = has_next
        if c in group_kv(last):
            goes_on = jnp.logical_and(has_next, jnp.logical_or(step < sp, sp + 1 < first_ask))

        @pl.when(goes_on)
        def _():
            kv_copy(sp - step, c).start()

    def arrives(step, g):
        here = sp >= step
        if g == last:
            unasked = jnp.logical_or(sp < first_ask, sp > step)
            here = jnp.logical_and(here, unasked if step > 1 else sp != near_owner + 1)
        return here

    def hand_on_if(step, c):
        if step < n_sp:
            g = last if c in group_kv(last) else 0
            pl.when(arrives(step, g))(functools.partial(hand_on, step, c))

    @pl.when(has_next)
    def _():
        pl.semaphore_wait(ready, 1)

    def send_if(condition, w, g):
        pl.when(condition)(functools.partial(send_unit, w, g))

    first = sp == 0
    w_wait(QUERY)
    partials(QUERY, 0, cols)
    send_if(asks, QUERY, last)
    finish_first(0)
    for w in (KEY, VALUE):
        partials(w, g_cols, cols - g_cols)
        for g in range(1, GROUPS):
            send_if(has_prev, w, g)
    finish_first(1)
    w_wait(FORGET)
    for w in (FORGET, INPUT):
        partials(w, 0, cols)
        send_unit(w, 0)
        finish_first(w)
    for c in range(INPUT + 1, X_CHUNKS):
        finish_first(c)
    for w in (FORGET, INPUT):
        for g in range(1, GROUPS):
            send_unit(w, g)
    for w in (KEY, VALUE):
        for g in range(1, GROUPS):
            send_if(first, w, g)
    send_if(jnp.logical_not(asks), QUERY, last)
    for g in range(last):
        send_unit(QUERY, g)
    partials(READ, 0, cols)
    for g in range(GROUPS):
        send_unit(READ, g)
    for w in (KEY, VALUE):
        own_product(w, slice(g_cols, cols))
    for w in (QUERY, FORGET, INPUT, READ):
        own_product(w, slice(0, cols))

    def o_copy(dt):
        return pltpu.make_async_remote_copy(
            src_ref=obuf.at[tp], dst_ref=obuf.at[tp], send_sem=o_send.at[dt - 1], recv_sem=o_recv.at[n_tp - dt - 1],
            device_id={"tp": tp_at(dt)}, device_id_type=MESH,
        )

    pltpu.make_async_copy(obuf.at[tp], obuf.at[tp], w_sem.at[N_PROJ // 2]).wait()
    for dt in range(1, n_tp):
        o_copy(dt).start()

    iota_r = lax.broadcasted_iota(jnp.int32, (rows, rows), 0)
    iota_c = lax.broadcasted_iota(jnp.int32, (rows, rows), 1)
    causal = iota_r >= iota_c
    strict = jnp.concatenate([iota_c < iota_r] * g_heads, axis=0)
    lower = jnp.where(causal, 1.0, 0.0).astype(BF16)
    lower = jnp.concatenate([lower, lower], axis=1)
    later = jnp.where(iota_r > iota_c, 1.0, 0.0).astype(BF16)
    sums = jnp.concatenate([later, jnp.ones((rows, LANES), BF16)], axis=1)
    sums = jnp.concatenate([sums, sums], axis=0)
    scale = 1.0 / math.sqrt(LANES)

    def lanes_of(h):
        return slice(h * LANES, (h + 1) * LANES)

    def heads_of(g):
        return range(g * g_heads, (g + 1) * g_heads)

    def gates(g):
        cut = group(g)
        rooms = jnp.concatenate([room[h:h + 1, :] for h in heads_of(g)], axis=1)
        key_in = rooms * jax.nn.sigmoid(-finish(FORGET, g).astype(F32))
        high, low = halves(jnp.log1p(-key_in))
        cum = dot_nn(lower, jnp.concatenate([high, low], axis=0))
        last = cum[rows - 1:rows, :]
        ecum[:, cut] = jnp.exp(cum)
        kinv[:, cut] = (key_in * jnp.exp(-cum)).astype(BF16)
        fresh[:, cut] = (key_in * jnp.exp(last - cum)).astype(BF16)
        decay = jnp.exp(last)
        for i, h in enumerate(heads_of(g)):
            dec[h] = jnp.broadcast_to(decay[:, lanes_of(i)], dec.shape[1:])

    def st_copy(h):
        return pltpu.make_async_remote_copy(
            src_ref=st_out.at[h], dst_ref=st_in.at[h], send_sem=st_send.at[0], recv_sem=st_recv.at[h],
            device_id={"sp": lax.rem(sp + 1, n_sp)}, device_id_type=MESH,
        )

    def local_state(g):
        rec_i[:, group(g)] = finish(INPUT, g)
        for h in heads_of(g):
            st_loc[h] = dot_tn(rec_i[:, lanes_of(h)], fresh[:, lanes_of(h)])

            @pl.when(jnp.logical_and(sp == 0, has_next))
            def _(h=h):
                st_out[h] = st_loc[h].astype(BF16)
                st_copy(h).start()

    def state_step(h):
        st_copy(h).wait_recv()

        @pl.when(has_next)
        def _():
            st_out[h] = (st_in[h].astype(F32) * dec[h, 0:1, :] + st_loc[h]).astype(BF16)
            st_copy(h).start()

    def state_steps(g, half=None):
        mine = heads_of(g)
        if half is not None:
            mine = mine[:1] if half == 0 else mine[1:]
        for h in mine:
            state_step(h)

    def state_step_if(at, g, half=None):
        if at < n_sp:
            pl.when(sp == at)(functools.partial(state_steps, g, half))

    def read_local(g):
        cut = group(g)
        qdec[:, cut] = (finish(READ, g).astype(F32) * ecum[:, cut]).astype(BF16)
        for h in heads_of(g):
            lanes = lanes_of(h)
            scores = jnp.where(causal, dot_nt(qdec[:, lanes], kinv[:, lanes]), 0.0)
            loc[:, lanes] = dot_nn(scores.astype(BF16), rec_i[:, lanes])

    n_land = 2 + g_heads
    early = pl.ds(0, last * g_cols)

    def h_sem(df, dt, mark):
        return h_recv.at[dt - 1 if df == 0 else n_tp - 1 + ((df - 1) * n_tp + dt) * n_land + mark]

    def h_copy(df, dt, kind, first, count, mark):
        lands = (n_tp - dt) % n_tp
        lanes = pl.ds(first, count)
        return pltpu.make_async_remote_copy(
            src_ref=heads.at[kind, pl.ds(pl.multiple_of(tp_at(dt) * share, share), share), lanes],
            dst_ref=hrecv.at[df * n_tp + lands, kind, :, lanes],
            send_sem=h_send.at[0], recv_sem=h_sem(df, lands, mark),
            device_id={"fs": fs_at(df), "tp": tp_at(dt)}, device_id_type=MESH,
        )

    h_order = [(df, dt) for df in list(range(1, n_fs)) + [0] for dt in range(n_tp) if df or dt]

    def send_heads(kind, first, count, mark):
        for df, dt in h_order:
            h_copy(df, dt, kind, first, count, mark).start()

    def send_attn(g):
        heads[0, :, group(g)] = att[:, group(g)].astype(BF16)
        send_heads(0, g * g_cols, g_cols, 1 if g == last else 0)

    def finish_rec(h):
        lanes = lanes_of(h)

        raw = loc[:, lanes] + dot_nt(qdec[:, lanes], st_in[h])
        norm = lax.rsqrt(jnp.mean(raw * raw, axis=1, keepdims=True) + norm_eps)
        heads[1, :, lanes] = (raw * norm * out_gain[...]).astype(BF16)

    def send_rec(g):
        for i, h in enumerate(heads_of(g)):
            if g == last:
                pl.when(far)(functools.partial(state_step, h))
            finish_rec(h)
            if g == last:
                send_heads(1, h * LANES, LANES, 2 + i)
        if g < last:
            send_heads(1, g * g_cols, g_cols, 0)

    def sticks(queries, slot, g, diagonal):
        z = jnp.concatenate(
            [
                dot_nt(queries[:, lanes_of(i)], kv[slot, 2 * g, :, lanes_of(i)]) * scale + offs[0:1, h:h + 1]
                for i, h in enumerate(heads_of(g))
            ],
            axis=0,
        )
        keep = -(jnp.maximum(z, 0.0) + jnp.log(1.0 + jnp.exp(-jnp.abs(z))))
        log_stick = z + keep
        if diagonal:
            keep = jnp.where(strict, keep, 0.0)
        keeps = jnp.concatenate(halves(keep), axis=1)
        both = dot_nn(keeps, sums)
        stick = jnp.exp(log_stick + both[:, :rows])
        if diagonal:
            stick = jnp.where(strict, stick, 0.0)
        return stick.astype(BF16), both, keeps

    def attend(slot, g, diagonal):
        stick, both, _ = sticks(qbuf.at[:, group(g)], slot, g, diagonal)
        for i, h in enumerate(heads_of(g)):
            mine = slice(i * rows, (i + 1) * rows)
            value = dot_nn(stick[mine], kv[slot, 2 * g + 1, :, lanes_of(i)])
            if diagonal:
                att[:, lanes_of(h)] = value
                run[h] = both[mine, rows:]
            else:
                past = run[h]
                att[:, lanes_of(h)] += value * jnp.exp(past)
                run[h] = past + both[mine, rows:]

    def attend_if(step, g):
        if step < n_sp:
            pl.when(arrives(step, g))(functools.partial(attend, sp - step, g, False))

    def attend_rest(g):
        def block(step, carry):
            for c in group_kv(g):
                hand_on(step, c)
            attend(sp - step, g, False)
            return carry

        end = jnp.where(asks, sp, sp + 1) if g == last else sp + 1
        lax.fori_loop(3, end, block, 0)

    def place(pair):
        asker, owner = asked[pair]
        return asker - first_ask if owner == 0 else 0

    def q_copy(pair):
        return pltpu.make_async_remote_copy(
            src_ref=qbuf.at[:, pl.ds(last * g_cols, g_cols)], dst_ref=q_back.at[place(pair)],
            send_sem=b_sem.at[pair], recv_sem=b_sem.at[pair],
            device_id={"sp": asked[pair][1]}, device_id_type=MESH,
        )

    def v_copy(pair):
        asker, owner = asked[pair]
        sem = b_sem.at[len(asked) + pair]
        count = pl.ds(0, rows if owner == 0 else rows + SUM_ROWS)
        return pltpu.make_async_remote_copy(
            src_ref=v_back.at[place(pair), count], dst_ref=v_far.at[0 if owner == 0 else 1, count],
            send_sem=sem, recv_sem=sem, device_id={"sp": asker}, device_id_type=MESH,
        )

    def ask_back():
        for pair in reversed(range(len(asked))):
            @pl.when(sp == asked[pair][0])
            def _(pair=pair):
                q_copy(pair).start()

    def answer(pair):
        owner, mine = asked[pair][1], place(pair)
        q_copy(pair).wait_recv()
        stick, _, keeps = sticks(q_back.at[mine], owner, last, False)
        for i in range(g_heads):
            part = slice(i * rows, (i + 1) * rows)
            value = dot_nn(stick[part], kv[owner, 2 * last + 1, :, lanes_of(i)])
            v_back[mine, 0:rows, lanes_of(i)] = value.astype(BF16)
            if owner > 0:
                sums_t = dot_nt(jnp.ones((SUM_ROWS // 2, keeps.shape[1]), BF16), keeps[part])
                high = sums_t.astype(BF16).astype(F32)
                pieces = jnp.concatenate([high, sums_t - high], axis=0)
                v_back[mine, rows:rows + SUM_ROWS, lanes_of(i)] = pieces.astype(BF16)
        v_copy(pair).start()

    def answers(near_ones):
        for pair in reversed(range(len(asked))):
            owner = asked[pair][1]
            if (owner > 0) == near_ones:
                pl.when(sp == owner)(functools.partial(answer, pair))

    def take(pair):
        slot = 0 if asked[pair][1] == 0 else 1
        v_copy(pair).wait_recv()
        for i, h in enumerate(heads_of(last)):
            past = run[h]
            value = v_far[slot, 0:rows, lanes_of(i)].astype(F32)
            att[:, lanes_of(h)] += value * jnp.exp(past)
            if slot > 0:
                spread = jnp.full((SUM_ROWS, LANES), 2.0 / SUM_ROWS, BF16)
                run[h] = past + dot_tn(v_far[slot, rows:rows + SUM_ROWS, lanes_of(i)], spread)

    def take_answers(near_ones):
        for pair, (asker, owner) in enumerate(asked):
            if (owner > 0) == near_ones:
                pl.when(sp == asker)(functools.partial(take, pair))

    def last_queries():
        qbuf[:, group(last)] = finish(QUERY, last)

    def late_keys():
        for g in range(1, GROUPS):
            for w in (KEY, VALUE):
                finish_kv(w, g)

    def last_hop():
        for g in range(1, GROUPS):
            for c in group_kv(g):
                hand_on(1, c)

    pl.when(asks)(last_queries)
    for c in group_kv(0):
        hand_on_if(1, c)
    pl.when(has_prev)(late_keys)
    for c in group_kv(0):
        hand_on_if(2, c)
        if c == 0 and n_sp <= 4:
            ask_back()
    gates(0)
    local_state(0)
    state_step_if(1, 0)
    pl.when(jnp.logical_and(sp > 1, sp != near_owner + 1))(last_hop)
    for g in range(1, GROUPS):
        gates(g)
        state_step_if(2, g - 1)
        if n_sp <= 4:
            answers(True)
        local_state(g)
        state_step_if(1, g)
    pl.when(first)(late_keys)
    pl.when(jnp.logical_not(asks))(last_queries)
    state_step_if(2, last)
    attend(sp, last, True)

    @pl.when(first)
    def _():
        send_attn(last)

    if n_sp <= 4:
        answers(False)
    for g in range(last):
        qbuf[:, group(g)] = finish(QUERY, g)
        attend(sp, g, True)
        attend_if(1, g)
        attend_if(2, g)
        attend_rest(g)
        send_attn(g)
    if n_sp > 4:
        ask_back()
        answers(True)
        answers(False)
    pl.when(sp == 1)(last_hop)
    attend_if(1, last)

    @pl.when(sp == 1)
    def _():
        send_attn(last)

    read_local(0)
    pl.when(far)(functools.partial(state_steps, 0))
    send_rec(0)
    read_local(last)
    take_answers(True)
    for c in group_kv(last):
        hand_on_if(2, c)
    attend_if(2, last)

    @pl.when(far)
    def _():
        attend_rest(last)

    take_answers(False)

    @pl.when(sp >= 2)
    def _():
        send_attn(last)

    send_rec(last)

    for dt in range(1, n_tp):
        other = tp_at(dt)
        land(obuf.at[other], o_recv.at[dt - 1])

    half = out_cols // CHUNKS

    def columns(owner, k):
        return pl.ds(pl.multiple_of(owner * out_cols + k * half, LANES), half)

    def m_copy(df, k):
        return pltpu.make_async_remote_copy(
            src_ref=mix.at[df - 1, k], dst_ref=out.at[:, columns(fs, k)],
            send_sem=m_send.at[df - 1], recv_sem=m_recv.at[df - 1],
            device_id={"fs": fs_at(n_fs - df)}, device_id_type=MESH,
        )

    def product(df, kind, lanes, cut):
        value = None
        for dt in range(n_tp):
            if df == 0 and dt == 0:
                left = heads[kind, pl.ds(pl.multiple_of(tp * share, share), share), lanes]
            else:
                left = hrecv[df * n_tp + dt, kind, :, lanes]
            term = dot_nn(left, obuf[tp_at(dt), kind, lanes, cut])
            value = term if value is None else value + term
        return value

    whole = slice(0, out_cols)
    final = lanes_of(n_heads - 1)
    for df in range(1, n_fs):
        for dt in range(n_tp):
            land(hrecv.at[df * n_tp + dt, :, :, early], h_sem(df, dt, 0))
        for kind in range(2):
            for g in range(last):
                if kind == 0 and g == 0:
                    part_acc[df - 1] = product(df, kind, group(g), whole)
                else:
                    part_acc[df - 1] += product(df, kind, group(g), whole)
        marks = [(0, group(last))] + [(1, lanes_of(h)) for h in heads_of(last)]
        for mark, (kind, lanes) in enumerate(marks):
            for dt in range(n_tp):
                land(hrecv.at[df * n_tp + dt, kind, :, lanes], h_sem(df, dt, 1 + mark))
            if mark < len(marks) - 1:
                part_acc[df - 1] += product(df, kind, lanes, whole)
        for k in range(CHUNKS):
            cut = slice(k * half, (k + 1) * half)
            mix[df - 1, k] = (part_acc[df - 1, :, cut] + product(df, 1, final, cut)).astype(BF16)
            m_copy(df, k).start()
    for dt in range(1, n_tp):
        land(hrecv.at[dt], h_sem(0, dt, 0))
    for k in range(CHUNKS):
        cut = slice(k * half, (k + 1) * half)
        value = product(0, 0, slice(0, cols), cut) + product(0, 1, slice(0, cols), cut)
        out[:, columns(fs, k)] = value.astype(BF16)

    for df in range(1, n_fs):
        @pl.when(holder(fs_at(df)) == tp)
        def _(df=df):
            land(xt.at[0], x_send.at[df - 1], True)

        @pl.when(is_relay)
        def _(df=df):
            for dt in range(1, n_tp):
                land(xt.at[0], f_send.at[(df - 1) * (n_tp - 1) + dt - 1], True)

        land(psend.at[df - 1], p_send.at[df - 1], True)
    for dt in range(1, n_tp):
        @pl.when(own_holder)
        def _(dt=dt):
            own_copy(dt).wait_send()

        ss_copy(dt).wait_send()
        o_copy(dt).wait_send()
    land(hrecv.at[pl.ds(1, n_fs * n_tp - 1)], h_send.at[0], True)

    @pl.when(has_next)
    def _():
        land(st_out, st_send.at[0], True)

        def drain(slot, carry):
            handed = jnp.logical_and(slot == 0, sp + 1 >= first_ask)
            own = jnp.logical_and(slot == sp, sp == near_owner)
            short = jnp.logical_or(handed, own)

            @pl.when(short)
            def _():
                land(kv.at[slot, pl.ds(0, 2 * last)], kv_send.at[slot], True)

            @pl.when(jnp.logical_not(short))
            def _():
                land(kv.at[slot], kv_send.at[slot], True)

            return carry

        lax.fori_loop(0, sp + 1, drain, 0)

    for pair, (asker, owner) in enumerate(asked):
        @pl.when(sp == asker)
        def _(pair=pair):
            q_copy(pair).wait_send()

        @pl.when(sp == owner)
        def _(pair=pair):
            v_copy(pair).wait_send()

    for df in range(1, n_fs):
        land(mix.at[df - 1], m_recv.at[df - 1])
        land(mix.at[df - 1], m_send.at[df - 1], True)


def body(
    tokens, mix_gain, attn_query, attn_key, attn_value, rec_query, rec_forget, rec_input,
    break_offset, forget_room, out_gain, out_attn, out_rec,
):
    n_sp, n_fs, n_tp = lax.axis_size("sp"), lax.axis_size("fs"), lax.axis_size("tp")
    rows, feat_t = tokens.shape[1], tokens.shape[2]
    feat_f, cols = attn_query.shape
    width = feat_t * n_tp
    n_heads = cols // LANES
    out_rows, out_cols = out_attn.shape
    share = rows // n_tp
    piece = out_cols // CHUNKS
    n_sends = len(unit_list(cols)) + X_CHUNKS
    n_kv = X_CHUNKS + 2 * (GROUPS - 1)
    n_ask = min(N_ASK, n_sp - 2)
    hbm = pl.BlockSpec(memory_space=pl.ANY)
    vmem = pl.BlockSpec(memory_space=pltpu.VMEM)
    dma = pltpu.SemaphoreType.DMA
    square = (n_heads, LANES, LANES)
    others = n_fs - 1
    result = pl.pallas_call(
        functools.partial(kernel, n_sp, n_fs, n_tp),
        out_shape=pltpu.VMEM((share, width), BF16),
        in_specs=[hbm] * 13,
        out_specs=vmem,
        scratch_shapes=[
            pltpu.VMEM((1, width), F32),
            pltpu.VMEM((1, n_heads), F32),
            pltpu.VMEM((n_heads, LANES), F32),
            pltpu.VMEM((1, LANES), F32),
            pltpu.VMEM((rows, feat_t), BF16),
            pltpu.VMEM((N_PROJ, feat_f, cols), BF16),
            pltpu.VMEM((n_tp, 2, out_rows, out_cols), BF16),
            pltpu.VMEM((n_fs, rows, feat_f), BF16),
            pltpu.VMEM((n_fs, rows, feat_f), BF16),
            pltpu.VMEM((n_tp, rows, LANES), F32),
            pltpu.VMEM((N_PROJ, rows, cols), F32),
            pltpu.VMEM((others, N_PROJ, rows, cols), BF16),
            pltpu.VMEM((others, N_PROJ, rows, cols), BF16),
            pltpu.VMEM((n_sp, 2 * GROUPS, rows, cols // GROUPS), BF16),
            pltpu.VMEM((rows, cols), BF16),
            pltpu.VMEM((rows, cols), BF16),
            pltpu.VMEM((rows, cols), F32),
            pltpu.VMEM((rows, cols), BF16),
            pltpu.VMEM((rows, cols), BF16),
            pltpu.VMEM((rows, cols), BF16),
            pltpu.VMEM((rows, cols), F32),
            pltpu.VMEM((n_heads, rows, LANES), F32),
            pltpu.VMEM((max(n_ask, 1), rows, cols // GROUPS), BF16),
            pltpu.VMEM((max(n_ask, 1), rows + SUM_ROWS, cols // GROUPS), BF16),
            pltpu.VMEM((2, rows + SUM_ROWS, cols // GROUPS), BF16),
            pltpu.VMEM((rows, cols), F32),
            pltpu.VMEM(square, F32),
            pltpu.VMEM((n_heads, 8, LANES), F32),
            pltpu.VMEM(square, BF16),
            pltpu.VMEM(square, BF16),
            pltpu.VMEM((2, rows, cols), BF16),
            pltpu.VMEM((n_fs * n_tp, 2, share, cols), BF16),
            pltpu.VMEM((others, share, out_cols), F32),
            pltpu.VMEM((others, CHUNKS, share, piece), BF16),
            dma((1,)), dma((N_SMALL,)), dma((N_PROJ // 2 + 1,)),
            dma((others,)), dma((others * X_CHUNKS,)), dma((others * (n_tp - 1),)),
            dma((n_tp - 1,)), dma((1,)), dma((n_tp - 1,)), dma((n_tp - 1,)),
            dma((others,)), dma((others * n_sends,)),
            dma((n_sp,)), dma(((n_sp - 1) * n_kv,)),
            dma((1,)), dma((n_heads,)),
            dma((n_tp - 1,)), dma((n_tp - 1,)), dma((max(2 * len(ask_list(n_sp)), 1),)),
            dma((1,)), dma((n_tp - 1 + others * n_tp * (2 + n_heads // GROUPS),)),
            dma((others,)), dma((others,)),
            pltpu.SemaphoreType.REGULAR,
        ],
        compiler_params=pltpu.CompilerParams(
            collective_id=0, has_side_effects=True, vmem_limit_bytes=60 * 1024 * 1024
        ),
        name="layer",
    )(
        tokens.reshape(rows, feat_t), mix_gain.reshape(1, width),
        attn_key, attn_value, rec_forget, rec_input, attn_query, rec_query,
        break_offset.reshape(1, n_heads), forget_room, out_gain.reshape(1, LANES), out_attn, out_rec,
    )
    return result.reshape(1, share, width)


def solution(mesh):
    placed = (
        P(("grp", "fs"), "sp", "tp"),
        P(),
        P("fs", "tp"),
        P("fs", "tp"),
        P("fs", "tp"),
        P("fs", "tp"),
        P("fs", "tp"),
        P("fs", "tp"),
        P("tp"),
        P("tp", None),
        P(),
        P("tp", "fs"),
        P("tp", "fs"),
    )
    return jax.shard_map(
        body,
        mesh=mesh,
        in_specs=placed,
        out_specs=P(("grp", "fs"), ("sp", "tp"), None),
        check_vma=False,
    )
```

```python
import functools
import math

import jax
import jax.numpy as jnp
from jax import lax
from jax.experimental import pallas as pl
from jax.experimental.pallas import tpu as pltpu
from jax.sharding import PartitionSpec as P

LANES = 128
norm_eps = 1e-06
MESH = pl.DeviceIdType.MESH
F32 = jnp.float32
BF16 = jnp.bfloat16
N_PROJ = 6
KEY, VALUE, FORGET, INPUT, QUERY, READ = range(N_PROJ)
GROUPS = 2
CHUNKS = 4
X_SPLIT = (1,2,2,3)
X_CHUNKS = len(X_SPLIT)
N_SMALL = 4
N_ASK = 2
SUM_ROWS = 16


def dot_nn(a, b):
    return lax.dot_general(a, b, (((1,), (0,)), ((), ())), preferred_element_type=F32)


def dot_nt(a, b):
    return lax.dot_general(a, b, (((1,), (1,)), ((), ())), preferred_element_type=F32)


def dot_tn(a, b):
    return lax.dot_general(a, b, (((0,), (0,)), ((), ())), preferred_element_type=F32)


def halves(x):
    high = x.astype(BF16)
    return high, (x - high.astype(F32)).astype(BF16)


def unit_list(cols):
    g_cols = cols // GROUPS
    last = (GROUPS - 1) * g_cols
    units = [(FORGET, 0), (INPUT, 0), (QUERY, last)]
    for g in range(1, GROUPS):
        units += [(w, g * g_cols) for w in (KEY, VALUE, FORGET, INPUT)]
    units += [(QUERY, g * g_cols) for g in range(GROUPS - 1)]
    units += [(READ, g * g_cols) for g in range(GROUPS)]
    return units


def ask_list(n_sp):
    first = n_sp - min(N_ASK, n_sp - 2)
    pairs = [(asker, 0) for asker in range(first, n_sp)]
    if n_sp > 2:
        pairs.append((n_sp - 1, n_sp - 2))
    return pairs


def kernel(
    n_sp, n_fs, n_tp,
    tok_hbm, gain_hbm, w_k, w_v, w_f, w_i, w_q, w_r, offs_hbm, room_hbm, out_gain_hbm, o_attn, o_rec,
    out,
    gain, offs, room, out_gain,
    tok, wbuf, obuf, xt, xg, ss, acc, psend, precv, kv, qbuf, qdec, ecum, kinv, fresh, rec_i,
    att, run, q_back, v_back, v_far, loc, st_loc, dec, st_in, st_out, heads, hrecv, part_acc, mix,
    t_sem, s_sem, w_sem, x_send, x_recv, f_send, own_send, own_recv, ss_send, ss_recv, p_send, p_recv,
    kv_send, kv_recv, st_send, st_recv, o_send, o_recv, b_sem, h_send, h_recv, m_send, m_recv, ready,
):
    sp, fs, tp = lax.axis_index("sp"), lax.axis_index("fs"), lax.axis_index("tp")
    rows, feat_t = tok.shape
    feat_f = xt.shape[2]
    width = feat_t * n_tp
    cols = wbuf.shape[2]
    n_heads = cols // LANES
    share = rows // n_tp
    out_cols = obuf.shape[3]
    g_cols = cols // GROUPS
    g_heads = n_heads // GROUPS
    n_kv = X_CHUNKS + 2 * (GROUPS - 1)
    x_edges = [rows * sum(X_SPLIT[:c]) // sum(X_SPLIT) for c in range(X_CHUNKS + 1)]
    relay = 0
    is_relay = tp == relay
    has_next = sp < n_sp - 1
    has_prev = sp > 0
    n_ask = min(N_ASK, n_sp - 2)
    first_ask = n_sp - n_ask
    asks = sp >= first_ask
    asked = ask_list(n_sp)
    near_owner = n_sp - 2 if n_sp > 2 else -1
    last = GROUPS - 1
    near = sp < 3
    far = sp >= 3

    def fs_at(step):
        return lax.rem(fs + step, n_fs)

    def tp_at(step):
        return lax.rem(tp + step, n_tp)

    def group(g):
        return slice(g * g_cols, (g + 1) * g_cols)

    tok_copy = pltpu.make_async_copy(tok_hbm, tok, t_sem.at[0])
    tok_copy.start()
    barrier = pltpu.get_barrier_semaphore()
    for df in range(n_fs):
        for dt in range(n_tp):
            if df or dt:
                pl.semaphore_signal(
                    barrier, inc=1, device_id={"fs": fs_at(df), "tp": tp_at(dt)}, device_id_type=MESH
                )

    @pl.when(has_next)
    def _():
        pl.semaphore_signal(barrier, inc=1, device_id={"sp": sp + 1}, device_id_type=MESH)


    small_copies = [
        pltpu.make_async_copy(source, target, s_sem.at[i])
        for i, (source, target) in enumerate(
            ((gain_hbm, gain), (offs_hbm, offs), (room_hbm, room), (out_gain_hbm, out_gain))
        )
    ]
    w_copies = [
        pltpu.make_async_copy(w, wbuf.at[i], w_sem.at[i // 2])
        for i, w in enumerate((w_k, w_v, w_f, w_i, w_q, w_r))
    ]
    o_copies = [
        pltpu.make_async_copy(w, obuf.at[tp, i], w_sem.at[N_PROJ // 2]) for i, w in enumerate((o_attn, o_rec))
    ]

    def w_wait(w):
        pair = wbuf.at[pl.ds(w, 2)]
        pltpu.make_async_copy(pair, pair, w_sem.at[w // 2]).wait()

    def land(view, sem, wait_send=False):
        copy = pltpu.make_async_remote_copy(
            src_ref=view, dst_ref=view, send_sem=sem, recv_sem=sem,
            device_id={"tp": tp_at(1)}, device_id_type=MESH,
        )
        if wait_send:
            copy.wait_send()
        else:
            copy.wait_recv()

    for copy in small_copies + w_copies + o_copies:
        copy.start()
    tok_copy.wait()

    pl.semaphore_wait(barrier, n_fs * n_tp - 1 + jnp.where(has_prev, 1, 0))

    @pl.when(has_prev)
    def _():
        pl.semaphore_signal(ready, inc=1, device_id={"sp": sp - 1}, device_id_type=MESH)

    def holder(f_index):
        return (f_index * feat_f) // feat_t

    def held(f_index):
        return pl.ds(pl.multiple_of(lax.rem(f_index * feat_f, feat_t), LANES), feat_f)

    def x_part(c):
        return pl.ds(x_edges[c], x_edges[c + 1] - x_edges[c])

    def x_copy(df, c):
        return pltpu.make_async_remote_copy(
            src_ref=tok.at[x_part(c), held(fs_at(df))], dst_ref=xt.at[fs, x_part(c)],
            send_sem=x_send.at[df - 1], recv_sem=x_recv.at[(n_fs - df - 1) * X_CHUNKS + c],
            device_id={"fs": fs_at(df), "tp": relay}, device_id_type=MESH,
        )

    def f_copy(df, c, dt):
        slot = fs_at(df)
        return pltpu.make_async_remote_copy(
            src_ref=xt.at[slot, x_part(c)], dst_ref=xt.at[slot, x_part(c)],
            send_sem=f_send.at[(df - 1) * (n_tp - 1) + dt - 1],
            recv_sem=x_recv.at[(df - 1) * X_CHUNKS + c],
            device_id={"tp": tp_at(dt)}, device_id_type=MESH,
        )

    def own_copy(dt):
        return pltpu.make_async_remote_copy(
            src_ref=tok.at[:, held(fs)], dst_ref=xt.at[fs],
            send_sem=own_send.at[dt - 1], recv_sem=own_recv.at[0],
            device_id={"tp": tp_at(dt)}, device_id_type=MESH,
        )

    for df in range(1, n_fs):
        @pl.when(holder(fs_at(df)) == tp)
        def _(df=df):
            for c in range(X_CHUNKS):
                x_copy(df, c).start()

    own_holder = holder(fs) == tp

    @pl.when(own_holder)
    def _():
        for dt in range(1, n_tp):
            own_copy(dt).start()

    squares = jnp.zeros((rows, LANES), F32)
    for c in range(feat_t // LANES):
        piece = tok[:, c * LANES:(c + 1) * LANES].astype(F32)
        squares = squares + piece * piece
    ss[tp] = squares

    def ss_copy(dt):
        return pltpu.make_async_remote_copy(
            src_ref=ss.at[tp], dst_ref=ss.at[tp],
            send_sem=ss_send.at[dt - 1], recv_sem=ss_recv.at[n_tp - dt - 1],
            device_id={"tp": tp_at(dt)}, device_id_type=MESH,
        )

    for dt in range(1, n_tp):
        ss_copy(dt).start()

    for copy in small_copies:
        copy.wait()
    gain_f = gain[:, pl.ds(pl.multiple_of(fs * feat_f, LANES), feat_f)]

    @pl.when(own_holder)
    def _():
        xg[0] = (tok[:, held(fs)].astype(F32) * gain_f).astype(BF16)

    units = unit_list(cols)
    n_units = len(units)

    def first_copy(df, c):
        index = (df - 1) * (n_units + X_CHUNKS) + n_units + c
        return pltpu.make_async_remote_copy(
            src_ref=psend.at[df - 1, pl.ds(KEY, 2), x_part(c), pl.ds(0, g_cols)],
            dst_ref=precv.at[df - 1, pl.ds(KEY, 2), x_part(c), pl.ds(0, g_cols)],
            send_sem=p_send.at[df - 1], recv_sem=p_recv.at[index],
            device_id={"fs": fs_at(df)}, device_id_type=MESH,
        )

    def p_copy(df, u):
        w, first = units[u]
        index = (df - 1) * (n_units + X_CHUNKS) + u
        return pltpu.make_async_remote_copy(
            src_ref=psend.at[df - 1, w, :, pl.ds(first, g_cols)],
            dst_ref=precv.at[df - 1, w, :, pl.ds(first, g_cols)],
            send_sem=p_send.at[df - 1], recv_sem=p_recv.at[index],
            device_id={"fs": fs_at(df)}, device_id_type=MESH,
        )

    @pl.when(jnp.logical_not(own_holder))
    def _():
        land(xt.at[fs], own_recv.at[0])
        xg[0] = (xt[fs].astype(F32) * gain_f).astype(BF16)

    total = ss[tp]
    for dt in range(1, n_tp):
        other = tp_at(dt)
        land(ss.at[other], ss_recv.at[dt - 1])
        total = total + ss[other]
    factor = lax.rsqrt(jnp.sum(total, axis=1, keepdims=True) / width + norm_eps)

    def own_product(w, cut):
        acc[w, :, cut] = dot_nn(xg[0], wbuf[w, :, cut])

    @pl.when(sp == 0)
    def _():
        st_in[...] = jnp.zeros_like(st_in)

    w_wait(KEY)
    own_product(KEY, group(0))
    own_product(VALUE, group(0))
    for c in range(X_CHUNKS):
        part = slice(x_edges[c], x_edges[c + 1])
        for df in range(1, n_fs):
            slot = fs_at(df)
            land(xt.at[slot, x_part(c)], x_recv.at[(df - 1) * X_CHUNKS + c])

            @pl.when(is_relay)
            def _(df=df, c=c):
                for dt in range(1, n_tp):
                    f_copy(df, c, dt).start()

            xg[df, part, :] = (xt[slot, part, :].astype(F32) * gain_f).astype(BF16)
            for w in (KEY, VALUE):
                psend[df - 1, w, part, 0:g_cols] = dot_nn(xg[df, part, :], wbuf[w, :, 0:g_cols]).astype(BF16)
            first_copy(df, c).start()

    def partials(w, first, count):
        cut = slice(first, first + count)
        for df in range(1, n_fs):
            psend[df - 1, w, :, cut] = dot_nn(xg[df], wbuf[w, :, cut]).astype(BF16)

    def send_unit(w, g):
        for df in range(1, n_fs):
            p_copy(df, units.index((w, g * g_cols))).start()


    def finish(w, g):
        cut = group(g)
        value = acc[w, :, cut]
        for df in range(1, n_fs):
            p_copy(df, units.index((w, g * g_cols))).wait_recv()
            value = value + precv[df - 1, w, :, cut].astype(F32)
        return (value * factor).astype(BF16)

    def kv_copy(slot, c):
        if c < X_CHUNKS:
            view = kv.at[slot, pl.ds(0, 2), x_part(c)]
        else:
            view = kv.at[slot, 2 + c - X_CHUNKS]
        return pltpu.make_async_remote_copy(
            src_ref=view, dst_ref=view,
            send_sem=kv_send.at[slot], recv_sem=kv_recv.at[slot * n_kv + c],
            device_id={"sp": lax.rem(sp + 1, n_sp)}, device_id_type=MESH,
        )

    def group_kv(g):
        if g == 0:
            return range(X_CHUNKS)
        return range(X_CHUNKS + 2 * (g - 1), X_CHUNKS + 2 * g)

    def send_kv(c):
        @pl.when(has_next)
        def _():
            kv_copy(sp, c).start()

    def finish_first(c):
        part = slice(x_edges[c], x_edges[c + 1])
        for df in range(1, n_fs):
            first_copy(df, c).wait_recv()
        for w in (KEY, VALUE):
            value = acc[w, part, 0:g_cols]
            for df in range(1, n_fs):
                value = value + precv[df - 1, w, part, 0:g_cols].astype(F32)
            kv[sp, w, part, :] = (value * factor[part]).astype(BF16)
        send_kv(c)

    def finish_kv(w, g):
        kv[sp, 2 * g + w] = finish(w, g)
        goes_on = jnp.logical_and(has_next, sp != near_owner) if g == last else has_next

        @pl.when(goes_on)
        def _():
            kv_copy(sp, X_CHUNKS + 2 * (g - 1) + w).start()

    def hand_on(step, c):
        kv_copy(sp - step, c).wait_recv()
        goes_on = has_next
        if c in group_kv(last):
            goes_on = jnp.logical_and(has_next, jnp.logical_or(step < sp, sp + 1 < first_ask))

        @pl.when(goes_on)
        def _():
            kv_copy(sp - step, c).start()

    def arrives(step, g):
        here = sp >= step
        if g == last:
            unasked = jnp.logical_or(sp < first_ask, sp > step)
            here = jnp.logical_and(here, unasked if step > 1 else sp != near_owner + 1)
        return here

    def hand_on_if(step, c):
        if step < n_sp:
            g = last if c in group_kv(last) else 0
            pl.when(arrives(step, g))(functools.partial(hand_on, step, c))

    @pl.when(has_next)
    def _():
        pl.semaphore_wait(ready, 1)

    def send_if(condition, w, g):
        pl.when(condition)(functools.partial(send_unit, w, g))

    first = sp == 0
    w_wait(QUERY)
    partials(QUERY, 0, cols)
    send_if(asks, QUERY, last)
    finish_first(0)
    for w in (KEY, VALUE):
        partials(w, g_cols, cols - g_cols)
        for g in range(1, GROUPS):
            send_if(has_prev, w, g)
    finish_first(1)
    w_wait(FORGET)
    for w in (FORGET, INPUT):
        partials(w, 0, cols)
        send_unit(w, 0)
        finish_first(w)
    for c in range(INPUT + 1, X_CHUNKS):
        finish_first(c)
    for w in (FORGET, INPUT):
        for g in range(1, GROUPS):
            send_unit(w, g)
    for w in (KEY, VALUE):
        for g in range(1, GROUPS):
            send_if(first, w, g)
    send_if(jnp.logical_not(asks), QUERY, last)
    for g in range(last):
        send_unit(QUERY, g)
    partials(READ, 0, cols)
    for g in range(GROUPS):
        send_unit(READ, g)
    for w in (KEY, VALUE):
        own_product(w, slice(g_cols, cols))
    for w in (QUERY, FORGET, INPUT, READ):
        own_product(w, slice(0, cols))

    def o_copy(dt):
        return pltpu.make_async_remote_copy(
            src_ref=obuf.at[tp], dst_ref=obuf.at[tp], send_sem=o_send.at[dt - 1], recv_sem=o_recv.at[n_tp - dt - 1],
            device_id={"tp": tp_at(dt)}, device_id_type=MESH,
        )

    pltpu.make_async_copy(obuf.at[tp], obuf.at[tp], w_sem.at[N_PROJ // 2]).wait()
    for dt in range(1, n_tp):
        o_copy(dt).start()

    iota_r = lax.broadcasted_iota(jnp.int32, (rows, rows), 0)
    iota_c = lax.broadcasted_iota(jnp.int32, (rows, rows), 1)
    causal = iota_r >= iota_c
    strict = jnp.concatenate([iota_c < iota_r] * g_heads, axis=0)
    lower = jnp.where(causal, 1.0, 0.0).astype(BF16)
    lower = jnp.concatenate([lower, lower], axis=1)
    later = jnp.where(iota_r > iota_c, 1.0, 0.0).astype(BF16)
    sums = jnp.concatenate([later, jnp.ones((rows, LANES), BF16)], axis=1)
    sums = jnp.concatenate([sums, sums], axis=0)
    scale = 1.0 / math.sqrt(LANES)

    def lanes_of(h):
        return slice(h * LANES, (h + 1) * LANES)

    def heads_of(g):
        return range(g * g_heads, (g + 1) * g_heads)

    def gates(g):
        cut = group(g)
        rooms = jnp.concatenate([room[h:h + 1, :] for h in heads_of(g)], axis=1)
        key_in = rooms * jax.nn.sigmoid(-finish(FORGET, g).astype(F32))
        high, low = halves(jnp.log1p(-key_in))
        cum = dot_nn(lower, jnp.concatenate([high, low], axis=0))
        last = cum[rows - 1:rows, :]
        ecum[:, cut] = jnp.exp(cum)
        kinv[:, cut] = (key_in * jnp.exp(-cum)).astype(BF16)
        fresh[:, cut] = (key_in * jnp.exp(last - cum)).astype(BF16)
        decay = jnp.exp(last)
        for i, h in enumerate(heads_of(g)):
            dec[h] = jnp.broadcast_to(decay[:, lanes_of(i)], dec.shape[1:])

    def st_copy(h):
        return pltpu.make_async_remote_copy(
            src_ref=st_out.at[h], dst_ref=st_in.at[h], send_sem=st_send.at[0], recv_sem=st_recv.at[h],
            device_id={"sp": lax.rem(sp + 1, n_sp)}, device_id_type=MESH,
        )

    def local_state(g):
        rec_i[:, group(g)] = finish(INPUT, g)
        for h in heads_of(g):
            st_loc[h] = dot_tn(rec_i[:, lanes_of(h)], fresh[:, lanes_of(h)])

            @pl.when(jnp.logical_and(sp == 0, has_next))
            def _(h=h):
                st_out[h] = st_loc[h].astype(BF16)
                st_copy(h).start()

    def state_step(h):
        st_copy(h).wait_recv()

        @pl.when(has_next)
        def _():
            st_out[h] = (st_in[h].astype(F32) * dec[h, 0:1, :] + st_loc[h]).astype(BF16)
            st_copy(h).start()

    def state_steps(g, half=None):
        mine = heads_of(g)
        if half is not None:
            mine = mine[:1] if half == 0 else mine[1:]
        for h in mine:
            state_step(h)

    def state_step_if(at, g, half=None):
        if at < n_sp:
            pl.when(sp == at)(functools.partial(state_steps, g, half))

    def read_local(g):
        cut = group(g)
        qdec[:, cut] = (finish(READ, g).astype(F32) * ecum[:, cut]).astype(BF16)
        for h in heads_of(g):
            lanes = lanes_of(h)
            scores = jnp.where(causal, dot_nt(qdec[:, lanes], kinv[:, lanes]), 0.0)
            loc[:, lanes] = dot_nn(scores.astype(BF16), rec_i[:, lanes])

    n_land = 2 + g_heads
    early = pl.ds(0, last * g_cols)

    def h_sem(df, dt, mark):
        return h_recv.at[dt - 1 if df == 0 else n_tp - 1 + ((df - 1) * n_tp + dt) * n_land + mark]

    def h_copy(df, dt, kind, first, count, mark):
        lands = (n_tp - dt) % n_tp
        lanes = pl.ds(first, count)
        return pltpu.make_async_remote_copy(
            src_ref=heads.at[kind, pl.ds(pl.multiple_of(tp_at(dt) * share, share), share), lanes],
            dst_ref=hrecv.at[df * n_tp + lands, kind, :, lanes],
            send_sem=h_send.at[0], recv_sem=h_sem(df, lands, mark),
            device_id={"fs": fs_at(df), "tp": tp_at(dt)}, device_id_type=MESH,
        )

    h_order = [(df, dt) for df in list(range(1, n_fs)) + [0] for dt in range(n_tp) if df or dt]

    def send_heads(kind, first, count, mark):
        for df, dt in h_order:
            h_copy(df, dt, kind, first, count, mark).start()

    def send_attn(g):
        heads[0, :, group(g)] = att[:, group(g)].astype(BF16)
        send_heads(0, g * g_cols, g_cols, 1 if g == last else 0)

    def finish_rec(h):
        lanes = lanes_of(h)

        raw = loc[:, lanes] + dot_nt(qdec[:, lanes], st_in[h])
        norm = lax.rsqrt(jnp.mean(raw * raw, axis=1, keepdims=True) + norm_eps)
        heads[1, :, lanes] = (raw * norm * out_gain[...]).astype(BF16)

    def send_rec(g):
        for i, h in enumerate(heads_of(g)):
            if g == last:
                pl.when(far)(functools.partial(state_step, h))
            finish_rec(h)
            if g == last:
                send_heads(1, h * LANES, LANES, 2 + i)
        if g < last:
            send_heads(1, g * g_cols, g_cols, 0)

    def sticks(queries, slot, g, diagonal):
        z = jnp.concatenate(
            [
                dot_nt(queries[:, lanes_of(i)], kv[slot, 2 * g, :, lanes_of(i)]) * scale + offs[0:1, h:h + 1]
                for i, h in enumerate(heads_of(g))
            ],
            axis=0,
        )
        keep = -(jnp.maximum(z, 0.0) + jnp.log(1.0 + jnp.exp(-jnp.abs(z))))
        log_stick = z + keep
        if diagonal:
            keep = jnp.where(strict, keep, 0.0)
        keeps = jnp.concatenate(halves(keep), axis=1)
        both = dot_nn(keeps, sums)
        stick = jnp.exp(log_stick + both[:, :rows])
        if diagonal:
            stick = jnp.where(strict, stick, 0.0)
        return stick.astype(BF16), both, keeps

    def attend(slot, g, diagonal):
        stick, both, _ = sticks(qbuf.at[:, group(g)], slot, g, diagonal)
        for i, h in enumerate(heads_of(g)):
            mine = slice(i * rows, (i + 1) * rows)
            value = dot_nn(stick[mine], kv[slot, 2 * g + 1, :, lanes_of(i)])
            if diagonal:
                att[:, lanes_of(h)] = value
                run[h] = both[mine, rows:]
            else:
                past = run[h]
                att[:, lanes_of(h)] += value * jnp.exp(past)
                run[h] = past + both[mine, rows:]

    def attend_if(step, g):
        if step < n_sp:
            pl.when(arrives(step, g))(functools.partial(attend, sp - step, g, False))

    def attend_rest(g):
        def block(step, carry):
            for c in group_kv(g):
                hand_on(step, c)
            attend(sp - step, g, False)
            return carry

        end = jnp.where(asks, sp, sp + 1) if g == last else sp + 1
        lax.fori_loop(3, end, block, 0)

    def place(pair):
        asker, owner = asked[pair]
        return asker - first_ask if owner == 0 else 0

    def q_copy(pair):
        return pltpu.make_async_remote_copy(
            src_ref=qbuf.at[:, pl.ds(last * g_cols, g_cols)], dst_ref=q_back.at[place(pair)],
            send_sem=b_sem.at[pair], recv_sem=b_sem.at[pair],
            device_id={"sp": asked[pair][1]}, device_id_type=MESH,
        )

    def v_copy(pair):
        asker, owner = asked[pair]
        sem = b_sem.at[len(asked) + pair]
        count = pl.ds(0, rows if owner == 0 else rows + SUM_ROWS)
        return pltpu.make_async_remote_copy(
            src_ref=v_back.at[place(pair), count], dst_ref=v_far.at[0 if owner == 0 else 1, count],
            send_sem=sem, recv_sem=sem, device_id={"sp": asker}, device_id_type=MESH,
        )

    def ask_back():
        for pair in reversed(range(len(asked))):
            @pl.when(sp == asked[pair][0])
            def _(pair=pair):
                q_copy(pair).start()

    def answer(pair):
        owner, mine = asked[pair][1], place(pair)
        q_copy(pair).wait_recv()
        stick, _, keeps = sticks(q_back.at[mine], owner, last, False)
        for i in range(g_heads):
            part = slice(i * rows, (i + 1) * rows)
            value = dot_nn(stick[part], kv[owner, 2 * last + 1, :, lanes_of(i)])
            v_back[mine, 0:rows, lanes_of(i)] = value.astype(BF16)
            if owner > 0:
                sums_t = dot_nt(jnp.ones((SUM_ROWS // 2, keeps.shape[1]), BF16), keeps[part])
                high = sums_t.astype(BF16).astype(F32)
                pieces = jnp.concatenate([high, sums_t - high], axis=0)
                v_back[mine, rows:rows + SUM_ROWS, lanes_of(i)] = pieces.astype(BF16)
        v_copy(pair).start()

    def answers(near_ones, ends=(False, True)):
        for pair in reversed(range(len(asked))):
            asker, owner = asked[pair]
            if (owner > 0) == near_ones and (asker == n_sp - 1) in ends:
                pl.when(sp == owner)(functools.partial(answer, pair))

    def take(pair):
        slot = 0 if asked[pair][1] == 0 else 1
        v_copy(pair).wait_recv()
        for i, h in enumerate(heads_of(last)):
            past = run[h]
            value = v_far[slot, 0:rows, lanes_of(i)].astype(F32)
            att[:, lanes_of(h)] += value * jnp.exp(past)
            if slot > 0:
                spread = jnp.full((SUM_ROWS, LANES), 2.0 / SUM_ROWS, BF16)
                run[h] = past + dot_tn(v_far[slot, rows:rows + SUM_ROWS, lanes_of(i)], spread)

    def take_answers(near_ones):
        for pair, (asker, owner) in enumerate(asked):
            if (owner > 0) == near_ones:
                pl.when(sp == asker)(functools.partial(take, pair))

    def last_queries():
        qbuf[:, group(last)] = finish(QUERY, last)

    def late_keys():
        for g in range(1, GROUPS):
            for w in (KEY, VALUE):
                finish_kv(w, g)

    def last_hop():
        for g in range(1, GROUPS):
            for c in group_kv(g):
                hand_on(1, c)

    pl.when(asks)(last_queries)
    for c in group_kv(0):
        hand_on_if(1, c)
    pl.when(has_prev)(late_keys)
    for c in group_kv(0):
        hand_on_if(2, c)
        if c == 0 and n_sp <= 4:
            ask_back()
    gates(0)
    local_state(0)
    state_step_if(1, 0)
    pl.when(jnp.logical_and(sp > 1, sp != near_owner + 1))(last_hop)
    for g in range(1, GROUPS):
        gates(g)
        state_step_if(2, g - 1)
        if n_sp <= 4:
            answers(True)
        local_state(g)
        state_step_if(1, g)
    pl.when(first)(late_keys)
    pl.when(jnp.logical_not(asks))(last_queries)
    attend(sp, last, True)

    @pl.when(first)
    def _():
        send_attn(last)

    if n_sp <= 4:
        answers(False, (False,))
    for g in range(last):
        qbuf[:, group(g)] = finish(QUERY, g)
        attend(sp, g, True)
        attend_if(1, g)
        attend_if(2, g)
        attend_rest(g)
        send_attn(g)
    if n_sp > 4:
        ask_back()
        answers(True)
        answers(False)
    else:
        answers(False, (True,))
    state_step_if(2, last)
    pl.when(sp == 1)(last_hop)
    attend_if(1, last)

    @pl.when(sp == 1)
    def _():
        send_attn(last)

    read_local(0)
    pl.when(far)(functools.partial(state_steps, 0))
    send_rec(0)
    read_local(last)
    pl.when(near)(functools.partial(send_rec, last))
    take_answers(True)
    for c in group_kv(last):
        hand_on_if(2, c)
    attend_if(2, last)

    @pl.when(far)
    def _():
        attend_rest(last)

    take_answers(False)

    @pl.when(sp >= 2)
    def _():
        send_attn(last)

    pl.when(far)(functools.partial(send_rec, last))

    for dt in range(1, n_tp):
        other = tp_at(dt)
        land(obuf.at[other], o_recv.at[dt - 1])

    half = out_cols // CHUNKS

    def columns(owner, k):
        return pl.ds(pl.multiple_of(owner * out_cols + k * half, LANES), half)

    def m_copy(df, k):
        return pltpu.make_async_remote_copy(
            src_ref=mix.at[df - 1, k], dst_ref=out.at[:, columns(fs, k)],
            send_sem=m_send.at[df - 1], recv_sem=m_recv.at[df - 1],
            device_id={"fs": fs_at(n_fs - df)}, device_id_type=MESH,
        )

    def product(df, kind, lanes, cut):
        value = None
        for dt in range(n_tp):
            if df == 0 and dt == 0:
                left = heads[kind, pl.ds(pl.multiple_of(tp * share, share), share), lanes]
            else:
                left = hrecv[df * n_tp + dt, kind, :, lanes]
            term = dot_nn(left, obuf[tp_at(dt), kind, lanes, cut])
            value = term if value is None else value + term
        return value

    whole = slice(0, out_cols)
    final = lanes_of(n_heads - 1)
    for df in range(1, n_fs):
        for dt in range(n_tp):
            land(hrecv.at[df * n_tp + dt, :, :, early], h_sem(df, dt, 0))
        for kind in range(2):
            for g in range(last):
                if kind == 0 and g == 0:
                    part_acc[df - 1] = product(df, kind, group(g), whole)
                else:
                    part_acc[df - 1] += product(df, kind, group(g), whole)
        marks = [(0, group(last))] + [(1, lanes_of(h)) for h in heads_of(last)]
        for mark, (kind, lanes) in enumerate(marks):
            for dt in range(n_tp):
                land(hrecv.at[df * n_tp + dt, kind, :, lanes], h_sem(df, dt, 1 + mark))
            if mark < len(marks) - 1:
                part_acc[df - 1] += product(df, kind, lanes, whole)
        for k in range(CHUNKS):
            cut = slice(k * half, (k + 1) * half)
            mix[df - 1, k] = (part_acc[df - 1, :, cut] + product(df, 1, final, cut)).astype(BF16)
            m_copy(df, k).start()
    for dt in range(1, n_tp):
        land(hrecv.at[dt], h_sem(0, dt, 0))
    for k in range(CHUNKS):
        cut = slice(k * half, (k + 1) * half)
        value = product(0, 0, slice(0, cols), cut) + product(0, 1, slice(0, cols), cut)
        out[:, columns(fs, k)] = value.astype(BF16)

    for df in range(1, n_fs):
        @pl.when(holder(fs_at(df)) == tp)
        def _(df=df):
            land(xt.at[0], x_send.at[df - 1], True)

        @pl.when(is_relay)
        def _(df=df):
            for dt in range(1, n_tp):
                land(xt.at[0], f_send.at[(df - 1) * (n_tp - 1) + dt - 1], True)

        land(psend.at[df - 1], p_send.at[df - 1], True)
    for dt in range(1, n_tp):
        @pl.when(own_holder)
        def _(dt=dt):
            own_copy(dt).wait_send()

        ss_copy(dt).wait_send()
        o_copy(dt).wait_send()
    land(hrecv.at[pl.ds(1, n_fs * n_tp - 1)], h_send.at[0], True)

    @pl.when(has_next)
    def _():
        land(st_out, st_send.at[0], True)

        def drain(slot, carry):
            handed = jnp.logical_and(slot == 0, sp + 1 >= first_ask)
            own = jnp.logical_and(slot == sp, sp == near_owner)
            short = jnp.logical_or(handed, own)

            @pl.when(short)
            def _():
                land(kv.at[slot, pl.ds(0, 2 * last)], kv_send.at[slot], True)

            @pl.when(jnp.logical_not(short))
            def _():
                land(kv.at[slot], kv_send.at[slot], True)

            return carry

        lax.fori_loop(0, sp + 1, drain, 0)

    for pair, (asker, owner) in enumerate(asked):
        @pl.when(sp == asker)
        def _(pair=pair):
            q_copy(pair).wait_send()

        @pl.when(sp == owner)
        def _(pair=pair):
            v_copy(pair).wait_send()

    for df in range(1, n_fs):
        land(mix.at[df - 1], m_recv.at[df - 1])
        land(mix.at[df - 1], m_send.at[df - 1], True)


def body(
    tokens, mix_gain, attn_query, attn_key, attn_value, rec_query, rec_forget, rec_input,
    break_offset, forget_room, out_gain, out_attn, out_rec,
):
    n_sp, n_fs, n_tp = lax.axis_size("sp"), lax.axis_size("fs"), lax.axis_size("tp")
    rows, feat_t = tokens.shape[1], tokens.shape[2]
    feat_f, cols = attn_query.shape
    width = feat_t * n_tp
    n_heads = cols // LANES
    out_rows, out_cols = out_attn.shape
    share = rows // n_tp
    piece = out_cols // CHUNKS
    n_sends = len(unit_list(cols)) + X_CHUNKS
    n_kv = X_CHUNKS + 2 * (GROUPS - 1)
    n_ask = min(N_ASK, n_sp - 2)
    hbm = pl.BlockSpec(memory_space=pl.ANY)
    vmem = pl.BlockSpec(memory_space=pltpu.VMEM)
    dma = pltpu.SemaphoreType.DMA
    square = (n_heads, LANES, LANES)
    others = n_fs - 1
    result = pl.pallas_call(
        functools.partial(kernel, n_sp, n_fs, n_tp),
        out_shape=pltpu.VMEM((share, width), BF16),
        in_specs=[hbm] * 13,
        out_specs=vmem,
        scratch_shapes=[
            pltpu.VMEM((1, width), F32),
            pltpu.VMEM((1, n_heads), F32),
            pltpu.VMEM((n_heads, LANES), F32),
            pltpu.VMEM((1, LANES), F32),
            pltpu.VMEM((rows, feat_t), BF16),
            pltpu.VMEM((N_PROJ, feat_f, cols), BF16),
            pltpu.VMEM((n_tp, 2, out_rows, out_cols), BF16),
            pltpu.VMEM((n_fs, rows, feat_f), BF16),
            pltpu.VMEM((n_fs, rows, feat_f), BF16),
            pltpu.VMEM((n_tp, rows, LANES), F32),
            pltpu.VMEM((N_PROJ, rows, cols), F32),
            pltpu.VMEM((others, N_PROJ, rows, cols), BF16),
            pltpu.VMEM((others, N_PROJ, rows, cols), BF16),
            pltpu.VMEM((n_sp, 2 * GROUPS, rows, cols // GROUPS), BF16),
            pltpu.VMEM((rows, cols), BF16),
            pltpu.VMEM((rows, cols), BF16),
            pltpu.VMEM((rows, cols), F32),
            pltpu.VMEM((rows, cols), BF16),
            pltpu.VMEM((rows, cols), BF16),
            pltpu.VMEM((rows, cols), BF16),
            pltpu.VMEM((rows, cols), F32),
            pltpu.VMEM((n_heads, rows, LANES), F32),
            pltpu.VMEM((max(n_ask, 1), rows, cols // GROUPS), BF16),
            pltpu.VMEM((max(n_ask, 1), rows + SUM_ROWS, cols // GROUPS), BF16),
            pltpu.VMEM((2, rows + SUM_ROWS, cols // GROUPS), BF16),
            pltpu.VMEM((rows, cols), F32),
            pltpu.VMEM(square, F32),
            pltpu.VMEM((n_heads, 8, LANES), F32),
            pltpu.VMEM(square, BF16),
            pltpu.VMEM(square, BF16),
            pltpu.VMEM((2, rows, cols), BF16),
            pltpu.VMEM((n_fs * n_tp, 2, share, cols), BF16),
            pltpu.VMEM((others, share, out_cols), F32),
            pltpu.VMEM((others, CHUNKS, share, piece), BF16),
            dma((1,)), dma((N_SMALL,)), dma((N_PROJ // 2 + 1,)),
            dma((others,)), dma((others * X_CHUNKS,)), dma((others * (n_tp - 1),)),
            dma((n_tp - 1,)), dma((1,)), dma((n_tp - 1,)), dma((n_tp - 1,)),
            dma((others,)), dma((others * n_sends,)),
            dma((n_sp,)), dma(((n_sp - 1) * n_kv,)),
            dma((1,)), dma((n_heads,)),
            dma((n_tp - 1,)), dma((n_tp - 1,)), dma((max(2 * len(ask_list(n_sp)), 1),)),
            dma((1,)), dma((n_tp - 1 + others * n_tp * (2 + n_heads // GROUPS),)),
            dma((others,)), dma((others,)),
            pltpu.SemaphoreType.REGULAR,
        ],
        compiler_params=pltpu.CompilerParams(
            collective_id=0, has_side_effects=True, vmem_limit_bytes=60 * 1024 * 1024
        ),
        name="layer",
    )(
        tokens.reshape(rows, feat_t), mix_gain.reshape(1, width),
        attn_key, attn_value, rec_forget, rec_input, attn_query, rec_query,
        break_offset.reshape(1, n_heads), forget_room, out_gain.reshape(1, LANES), out_attn, out_rec,
    )
    return result.reshape(1, share, width)


def solution(mesh):
    placed = (
        P(("grp", "fs"), "sp", "tp"),
        P(),
        P("fs", "tp"),
        P("fs", "tp"),
        P("fs", "tp"),
        P("fs", "tp"),
        P("fs", "tp"),
        P("fs", "tp"),
        P("tp"),
        P("tp", None),
        P(),
        P("tp", "fs"),
        P("tp", "fs"),
    )
    return jax.shard_map(
        body,
        mesh=mesh,
        in_specs=placed,
        out_specs=P(("grp", "fs"), ("sp", "tp"), None),
        check_vma=False,
    )
```
